32 devices in a mesh: ep: 16 (over z, y, x), tp: 2 (over core).
Axes of the slice: x: 2, y: 2, z: 4, core: 2. Of those that a mesh axis runs over, the one named last changes fastest.
Arguments:
- hidden: bfloat16 [256, 2048], P('ep'), may hold values from -6 to 6
- attn_gain: bfloat16 [2048], replicated, may hold values from 0.099609375 to 1.8984375
- query_weight: bfloat16 [2048, 2048], P(None, 'tp'), may hold values from -0.125 to 0.125
- key_weight: bfloat16 [2048, 128], P(None, 'tp'), may hold values from -0.125 to 0.125
- value_weight: bfloat16 [2048, 128], P(None, 'tp'), may hold values from -0.125 to 0.125
- forget_weight: bfloat16 [2048, 32], P(None, 'tp'), may hold values from -0.125 to 0.125
- forget_bias: float32 [32], P('tp'), may hold values from -1 to 4
- cache_keys: bfloat16 [256, 2, 64, 1024], P('ep', 'tp'), may hold values from -64 to 64
- cache_values: bfloat16 [256, 2, 64, 1024], P('ep', 'tp'), may hold values from -6 to 6
- cache_logsum: float32 [256, 32, 1024], P('ep', 'tp'), may hold values from -144 to 0, as said below
- lengths: int32 [256], P('ep'), may hold values from 2 to 1023, as said below
- out_weight: bfloat16 [2048, 2048], P('ep'), may hold values from -0.125 to 0.125
- ffn_gain: bfloat16 [2048], replicated, may hold values from 0.099609375 to 1.8984375
- expert_ids: int32 [256, 6], P('ep'), may hold values from 0 to 15, all different within a row; in each aligned block of 16 rows (0 to 15, 16 to 31, ...) at most 12 rows name the same one
- expert_scores: float32 [256, 6], P('ep'), may hold values from 0.1 to 1
- gate_weights: bfloat16 [16, 2048, 512], P('ep', None, 'tp'), may hold values from -0.125 to 0.125
- up_weights: bfloat16 [16, 2048, 512], P('ep', None, 'tp'), may hold values from -0.125 to 0.125
- down_weights: bfloat16 [16, 512, 2048], P('ep', 'tp'), may hold values from -0.25 to 0.25
Outputs:
- updated: bfloat16 [256, 2048], P('ep')
- new_key: bfloat16 [256, 2, 64], P('ep', 'tp')
- new_value: bfloat16 [256, 2, 64], P('ep', 'tp')
- new_logsum: float32 [256, 32], P('ep', 'tp')
The draws below stay inside these ranges and needn't reach their ends.
Inputs may be any that keep to these rules, and one draw needn't show every extreme that they name: `cache_logsum`: non-increasing along the positions. The new token stands at position lengths; some sequence has 1023 cached positions. `expert_ids`: each row names 6 different experts; the rows of one index of ep name one expert at most 12 times.
All inputs are finite; a program needn't handle non-finite values.
Results may differ from the reference program's by a relative error of at most 0.006.
Values may be sent and summed in bfloat16 or wider, within the bound.
A program may use at most 64 MiB of HBM per device.

```python
import math
import jax
import jax.numpy as jnp
import numpy as np
from jax import lax

D = 2048
HEADS = 32
HD = 64
KV_HEADS = 2
DEXP = 512
TOP_K = 6
CACHE_POSITIONS = 1024
SEQ_DEV = 16
BATCH_SEQUENCES = 256
EXPERTS = 16
CAP = 12
N_EP = 16
N_TP = 2


def draw_cache_keys(key, part):
    random_subkeys = jax.random.split(key, 1)
    values_drawn = jnp.clip(jax.random.normal(random_subkeys[0], (BATCH_SEQUENCES, KV_HEADS, HD, CACHE_POSITIONS), jnp.float32), -6.0, 6.0)
    return values_drawn.astype(jnp.bfloat16)


def draw_cache_logsum(key, part):
    random_subkeys = jax.random.split(key, 7)
    head_order = jax.random.permutation(random_subkeys[0], HEADS)
    is_sluggish = head_order < HEADS // 2
    is_sluggish = is_sluggish.astype(jnp.float32)[None, :, None]
    slow_rate = jax.random.uniform(random_subkeys[1], (1, HEADS, 1), jnp.float32, 0.2, 0.8) / CACHE_POSITIONS
    fast_rate = 1.0 / jax.random.uniform(random_subkeys[2], (1, HEADS, 1), jnp.float32, 30.0, 100.0)
    decay_rate = is_sluggish * slow_rate + (1.0 - is_sluggish) * fast_rate
    sequence_factor = jnp.exp(jax.random.uniform(random_subkeys[3], (BATCH_SEQUENCES, 1, 1), jnp.float32, math.log(0.5), math.log(2.0)))
    random_wobble = jax.random.uniform(random_subkeys[4], (BATCH_SEQUENCES, HEADS, CACHE_POSITIONS), jnp.float32, 0.4, 1.6)
    spike_mask = (jax.random.uniform(random_subkeys[5], (BATCH_SEQUENCES, 1, CACHE_POSITIONS)) < 3.0 / CACHE_POSITIONS).astype(jnp.float32)
    shift_amount = jax.random.uniform(random_subkeys[6], (BATCH_SEQUENCES, HEADS, CACHE_POSITIONS), jnp.float32, 0.22, 0.69)
    step_logarithm = -(decay_rate * sequence_factor * random_wobble) - spike_mask * shift_amount * is_sluggish
    return jnp.cumsum(step_logarithm, axis=-1).astype(jnp.float32)


def draw_lengths(key, part):
    random_subkeys = jax.random.split(key, 2)
    groups = BATCH_SEQUENCES // SEQ_DEV
    device_top = jax.random.randint(random_subkeys[0], (groups, 1), CACHE_POSITIONS // 8, CACHE_POSITIONS - 1)
    raw_bits = jax.random.randint(random_subkeys[1], (groups, SEQ_DEV), 0, 1 << 20)
    lengths_drawn = 2 + raw_bits % (device_top - 1)
    lengths_drawn = lengths_drawn.reshape(BATCH_SEQUENCES).at[0].set(CACHE_POSITIONS - 1)
    return lengths_drawn.astype(jnp.int32)


def levels(own_key, dims, pieces, smallest, high):
    level, own = 1.0, jax.random.fold_in(own_key, 6)
    for position, blocks in pieces:
        steps = jnp.exp(jax.random.uniform(jax.random.fold_in(own, position), (blocks,), jnp.float32, smallest / len(pieces), high / len(pieces)))
        level = level * jnp.repeat(steps, dims[position] // blocks).reshape([-1 if axis == position else 1 for axis in range(len(dims))])
    return level


def deal_out(key, own, number, rows, number_of, top, most, lean):
    sequence = jax.random.permutation(key, number_of)
    packed, ordinary = load_shares(number_of, rows * top, most, lean, True), load_shares(number_of, rows * top, most, lean, False)
    places = jnp.arange(number_of)

    def named(tallies, turn):
        used = int((tallies > 0).sum())
        fixed = max(1, used // 4)
        moved = fixed + (places - fixed + turn * (used - fixed)) % max(1, number_of - fixed)
        return jnp.zeros((number_of,), jnp.int32).at[sequence[jnp.where(places < fixed, places, moved)]].set(jnp.asarray(tallies, jnp.int32))

    tallies = jnp.where(number % 4 == 0, named(packed, number // 4), named(ordinary, number - number // 4 - 1))
    mixed = jax.random.permutation(jax.random.fold_in(own, 3), number_of)
    donor, receiver = mixed[0:number_of // 2 * 2:2], mixed[1:number_of // 2 * 2:2]
    room = jnp.minimum(tallies[donor] - 1, most - tallies[receiver]) // 2
    room = jnp.where((donor == sequence[0]) | (receiver == sequence[0]) | (tallies[receiver] == 0), 0, jnp.maximum(room, 0))
    moved = jax.random.randint(jax.random.fold_in(own, 4), (number_of // 2,), 0, 1 << 20) % (room + 1)
    tallies = tallies.at[donor].add(-moved).at[receiver].add(moved)
    items = jnp.searchsorted(jnp.cumsum(tallies), jnp.arange(rows * top), side="right").astype(jnp.int32)
    listing = items.reshape(top, rows).T
    listing = listing[jax.random.permutation(jax.random.fold_in(own, 1), rows)]
    turn = jax.random.randint(jax.random.fold_in(own, 2), (rows, 1), 0, top)
    return jnp.take_along_axis(listing, (jnp.arange(top)[None, :] + turn) % top, axis=1)


def load_shares(amount, total, reach, skew, full):
    portions = [(1 << 20) // math.isqrt(standing ** skew) + 1 for standing in range(1, amount + 1)]
    largest = reach if full else min(reach, max(-(-total // amount), total * portions[0] // sum(portions)))
    least = 1 if total - largest >= amount - 1 else 0
    given, rest = [largest] + [least] * (amount - 1), total - largest - least * (amount - 1)
    while rest > 0:
        movable = [i for i in range(1, amount) if given[i] < largest] or [i for i in range(1, amount) if given[i] < reach]
        whole, remaining = sum([portions[i] for i in movable]), rest
        for i in movable:
            more = min(reach - given[i], max(1, remaining * portions[i] // whole), rest)
            given[i] = given[i] + more
            rest = rest - more
    return np.array(given)


def bell_draw(stream_key, dims, spread, reach, cuts=(), kind=jnp.bfloat16):
    values = jax.random.normal(stream_key, dims, jnp.float32) * spread
    if len(cuts) > 0:
        values = levels(stream_key, dims, cuts, -0.22, 0.18) * values
    return jnp.clip(values, min=-reach, max=reach).astype(kind)


def setup_inputs(seed: int = 0) -> dict:
    arg_keys = jax.random.split(jax.random.key(seed), 19)
    hidden = bell_draw(arg_keys[0], (BATCH_SEQUENCES, D), 1.0, 6.0, ((0, 16),))
    attn_gain = jnp.clip(1.0 + 0.18 * jax.random.normal(arg_keys[1], (D,), jnp.float32), 0.099609375, 1.8984375).astype(jnp.bfloat16)
    query_weight = bell_draw(arg_keys[2], (D, HEADS * HD), D ** -0.5, 0.125, ((1, 2),))
    key_weight = bell_draw(arg_keys[3], (D, KV_HEADS * HD), D ** -0.5, 0.125, ((1, 2),))
    value_weight = bell_draw(arg_keys[4], (D, KV_HEADS * HD), D ** -0.5, 0.125, ((1, 2),))
    forget_weight = bell_draw(arg_keys[5], (D, HEADS), D ** -0.5, 0.125, ((1, 2),))
    forget_bias = jnp.clip(-1.0 + 5.0 * jax.random.uniform(arg_keys[6], (HEADS,), jnp.float32) ** levels(arg_keys[6], (HEADS,), ((0, 2),), -0.2, 0.2), -1.0, 4.0)
    cache_keys = draw_cache_keys(jax.random.fold_in(arg_keys[18], 71), 0)
    cache_values = bell_draw(arg_keys[8], (BATCH_SEQUENCES, KV_HEADS, HD, CACHE_POSITIONS), 1.0, 6.0, ((0, 16), (1, 2)))
    cache_logsum = draw_cache_logsum(jax.random.fold_in(arg_keys[18], 71), 0)
    lengths = draw_lengths(jax.random.fold_in(arg_keys[18], 71), 0)
    out_weight = bell_draw(arg_keys[11], (D, HEADS * HD), (HEADS * HD) ** -0.5, 0.125, ((0, 16),))
    ffn_gain = jnp.clip(1.0 + 0.18 * jax.random.normal(arg_keys[12], (D,), jnp.float32), 0.099609375, 1.8984375).astype(jnp.bfloat16)
    expert_ids_keys = jax.random.split(jax.random.fold_in(arg_keys[13], 1), BATCH_SEQUENCES // SEQ_DEV)
    expert_ids_turns = jax.random.permutation(jax.random.fold_in(arg_keys[13], 3), BATCH_SEQUENCES // SEQ_DEV)
    expert_ids = jax.vmap(lambda own, number: deal_out(jax.random.fold_in(arg_keys[13], 2), own, number, SEQ_DEV, EXPERTS, TOP_K, CAP, 2))(expert_ids_keys, expert_ids_turns).reshape((BATCH_SEQUENCES, TOP_K))
    expert_scores = jnp.clip(jnp.exp(math.log(1.0) - 2.3025851 * jax.random.uniform(arg_keys[14], (BATCH_SEQUENCES, TOP_K), jnp.float32) ** levels(arg_keys[14], (BATCH_SEQUENCES, TOP_K), ((0, 16),), -0.2, 0.2)), 0.1, 1.0)
    gate_weights = bell_draw(arg_keys[15], (EXPERTS, D, DEXP), D ** -0.5, 0.125, ((0, 16), (2, 2)))
    up_weights = bell_draw(arg_keys[16], (EXPERTS, D, DEXP), D ** -0.5, 0.125, ((0, 16), (2, 2)))
    down_weights = bell_draw(arg_keys[17], (EXPERTS, DEXP, D), DEXP ** -0.5, 0.25, ((0, 16), (1, 2)))
    return {"hidden": hidden, "attn_gain": attn_gain, "query_weight": query_weight, "key_weight": key_weight, "value_weight": value_weight, "forget_weight": forget_weight, "forget_bias": forget_bias, "cache_keys": cache_keys, "cache_values": cache_values, "cache_logsum": cache_logsum, "lengths": lengths, "out_weight": out_weight, "ffn_gain": ffn_gain, "expert_ids": expert_ids, "expert_scores": expert_scores, "gate_weights": gate_weights, "up_weights": up_weights, "down_weights": down_weights}


epsilon = 1e-06

def root_norm(values_in, gain):
    floats = values_in.astype(jnp.float32)
    inv_root = lax.rsqrt(lax.optimization_barrier(jnp.mean(floats * floats, axis=-1, keepdims=True)) + epsilon)
    return floats * inv_root * gain.astype(jnp.float32)

def attend(block):
    queries, keys_block, values_block, logsum_block, lengths_block, key_new, value_new, newsum = block
    rows_here = queries.shape[0]
    query_heads = queries.shape[1] // HD
    key_heads = keys_block.shape[1]
    group_size = query_heads // key_heads
    score_scale = HD ** (-0.5)
    grouped = queries.astype(jnp.float32).reshape(rows_here, key_heads, group_size, HD)
    scores = jnp.einsum('sgjd,sgdp->sgjp', grouped, keys_block.astype(jnp.float32))
    scores = scores.reshape(rows_here, query_heads, CACHE_POSITIONS) * score_scale
    scores = scores + newsum[:, :, None] - logsum_block
    positions = jnp.arange(CACHE_POSITIONS, dtype=jnp.int32)
    is_live = positions[None, :] < lengths_block[:, None]
    scores = jnp.where(is_live[:, None, :], scores, -jnp.inf)
    own_score = jnp.einsum('sgjd,sgd->sgj', grouped, key_new.astype(jnp.float32)).reshape(rows_here, query_heads) * score_scale
    top_score = jnp.maximum(lax.optimization_barrier(jnp.max(scores, axis=-1)), own_score)
    past_exp = jnp.exp(scores - top_score[:, :, None])
    own_exp = jnp.exp(own_score - top_score)
    denominator = lax.optimization_barrier(jnp.sum(past_exp, axis=-1)) + own_exp
    past_weight = (past_exp / denominator[:, :, None]).astype(jnp.bfloat16)
    own_weight = (own_exp / denominator).astype(jnp.bfloat16)
    attended = jnp.einsum('sgjp,sgdp->sgjd', past_weight.astype(jnp.float32).reshape(rows_here, key_heads, group_size, CACHE_POSITIONS), values_block.astype(jnp.float32))
    attended = attended + own_weight.astype(jnp.float32).reshape(rows_here, key_heads, group_size)[:, :, :, None] * value_new.astype(jnp.float32)[:, :, None, :]
    return attended.reshape(rows_here, query_heads * HD).astype(jnp.bfloat16)

def blocked(array):
    return array.reshape((BATCH_SEQUENCES // SEQ_DEV, SEQ_DEV) + array.shape[1:])

def reference(hidden, attn_gain, query_weight, key_weight, value_weight, forget_weight, forget_bias, cache_keys, cache_values, cache_logsum, lengths, out_weight, ffn_gain, expert_ids, expert_scores, gate_weights, up_weights, down_weights):
    normed = root_norm(hidden, attn_gain).astype(jnp.bfloat16)
    queries = jnp.dot(normed, query_weight, preferred_element_type=jnp.float32).astype(jnp.bfloat16)
    new_key = jnp.dot(normed, key_weight, preferred_element_type=jnp.float32).astype(jnp.bfloat16).reshape(BATCH_SEQUENCES, KV_HEADS, HD)
    new_value = jnp.dot(normed, value_weight, preferred_element_type=jnp.float32).astype(jnp.bfloat16).reshape(BATCH_SEQUENCES, KV_HEADS, HD)
    log_forget = jax.nn.log_sigmoid(jnp.dot(normed, forget_weight, preferred_element_type=jnp.float32) + forget_bias)
    positions = jnp.arange(CACHE_POSITIONS, dtype=jnp.int32)
    is_last = positions[None, :] == (lengths - 1)[:, None]
    new_logsum = lax.optimization_barrier(jnp.sum(jnp.where(is_last[:, None, :], cache_logsum, 0.0), axis=-1)) + log_forget
    blocks = tuple((blocked(array) for array in (queries, cache_keys, cache_values, cache_logsum, lengths, new_key, new_value, new_logsum)))
    attended = lax.map(attend, blocks).reshape(BATCH_SEQUENCES, HEADS * HD)
    mixed = jnp.dot(attended, out_weight.T, preferred_element_type=jnp.float32).astype(jnp.bfloat16)
    residual = hidden.astype(jnp.float32) + mixed.astype(jnp.float32)
    ffn_in = root_norm(residual, ffn_gain).astype(jnp.bfloat16)
    route_count = BATCH_SEQUENCES * TOP_K
    flat_ids = expert_ids.reshape(route_count)
    onehot = (flat_ids[:, None] == jnp.arange(EXPERTS, dtype=jnp.int32)[None, :]).astype(jnp.int32)
    running = jnp.cumsum(onehot.reshape(N_EP, SEQ_DEV * TOP_K, EXPERTS), axis=1).reshape(route_count, EXPERTS)
    slot_index = lax.optimization_barrier(jnp.sum(running * onehot, axis=1)) - 1
    source = jnp.arange(route_count, dtype=jnp.int32) // (SEQ_DEV * TOP_K)
    placement = flat_ids * (N_EP * CAP) + source * CAP + slot_index
    token_of_route = jnp.arange(route_count, dtype=jnp.int32) // TOP_K
    slot_table = jnp.full((EXPERTS * N_EP * CAP,), BATCH_SEQUENCES, dtype=jnp.int32).at[placement].set(token_of_route)
    padded = jnp.concatenate([ffn_in, jnp.zeros((1, D), jnp.bfloat16)], axis=0)
    expert_rows = padded[slot_table].reshape(EXPERTS, N_EP * CAP, D)
    share_width = DEXP // N_TP

    def run_expert(block):
        rows_in, gate_one, up_one, down_one = block
        gate_act = jnp.dot(rows_in, gate_one, preferred_element_type=jnp.float32)
        up_act = jnp.dot(rows_in, up_one, preferred_element_type=jnp.float32)
        hidden_act = (jax.nn.silu(gate_act) * up_act).astype(jnp.bfloat16)
        summed = jnp.zeros((rows_in.shape[0], D), jnp.float32)
        for block_index in range(N_TP):
            lower = block_index * share_width
            partial_value = jnp.dot(hidden_act[:, lower:lower + share_width], down_one[lower:lower + share_width], preferred_element_type=jnp.float32)
            summed = summed + partial_value.astype(jnp.bfloat16).astype(jnp.float32)
        return summed.astype(jnp.bfloat16)
    expert_outputs = lax.map(run_expert, (expert_rows, gate_weights, up_weights, down_weights))
    route_out = expert_outputs.reshape(EXPERTS * N_EP * CAP, D)[placement].astype(jnp.float32).reshape(BATCH_SEQUENCES, TOP_K, D)
    route_weight = expert_scores / lax.optimization_barrier(jnp.sum(expert_scores, axis=-1, keepdims=True))
    updated = (residual + lax.optimization_barrier(jnp.sum(route_out * route_weight[:, :, None], axis=1))).astype(jnp.bfloat16)
    return (updated, new_key, new_value, new_logsum)
```

```python
import functools
import math

import jax
import jax.numpy as jnp
from jax import lax
from jax.experimental import pallas as pl
from jax.experimental.pallas import tpu as pltpu
from jax.sharding import PartitionSpec as P

HD = 64
TOP_K = 6


epsilon = 1e-06


def root_norm(values_in, gain):
    floats = values_in.astype(jnp.float32)
    inv_root = lax.rsqrt(jnp.mean(floats * floats, axis=-1, keepdims=True) + epsilon)
    return floats * inv_root * gain.astype(jnp.float32)


def attend(hidden, attn_gain, query_weight, key_weight, value_weight, forget_weight, forget_bias,
           cache_keys, cache_values, cache_logsum, lengths):
    rows_here = hidden.shape[0]
    query_heads = query_weight.shape[1] // HD
    key_heads = key_weight.shape[1] // HD
    group_size = query_heads // key_heads
    cache_len = cache_keys.shape[-1]
    score_scale = HD ** (-0.5)
    normed = root_norm(hidden, attn_gain).astype(jnp.bfloat16)
    queries = jnp.dot(normed, query_weight, preferred_element_type=jnp.float32).astype(jnp.bfloat16)
    key_new = (
        jnp.dot(normed, key_weight, preferred_element_type=jnp.float32)
        .astype(jnp.bfloat16)
        .reshape(rows_here, key_heads, HD)
    )
    value_new = (
        jnp.dot(normed, value_weight, preferred_element_type=jnp.float32)
        .astype(jnp.bfloat16)
        .reshape(rows_here, key_heads, HD)
    )
    log_forget = jax.nn.log_sigmoid(
        jnp.dot(normed, forget_weight, preferred_element_type=jnp.float32) + forget_bias
    )
    positions = jnp.arange(cache_len, dtype=jnp.int32)
    is_last = positions[None, :] == (lengths - 1)[:, None]
    new_logsum = jnp.sum(jnp.where(is_last[:, None, :], cache_logsum, 0.0), axis=-1) + log_forget
    grouped = queries.reshape(rows_here, key_heads, group_size, HD)
    scores = jnp.einsum("sgjd,sgdp->sgjp", grouped, cache_keys, preferred_element_type=jnp.float32)
    scores = scores.reshape(rows_here, query_heads, cache_len) * score_scale
    scores = scores + new_logsum[:, :, None] - cache_logsum
    is_live = positions[None, :] < lengths[:, None]
    scores = jnp.where(is_live[:, None, :], scores, -jnp.inf)
    own_score = (
        jnp.einsum("sgjd,sgd->sgj", grouped, key_new, preferred_element_type=jnp.float32).reshape(
            rows_here, query_heads
        )
        * score_scale
    )
    top_score = jnp.maximum(jnp.max(scores, axis=-1), own_score)
    past_exp = jnp.exp(scores - top_score[:, :, None])
    own_exp = jnp.exp(own_score - top_score)
    denominator = jnp.sum(past_exp, axis=-1) + own_exp
    past_weight = (past_exp / denominator[:, :, None]).astype(jnp.bfloat16)
    own_weight = (own_exp / denominator).astype(jnp.bfloat16)
    attended = jnp.einsum(
        "sgjp,sgdp->sgjd",
        past_weight.reshape(rows_here, key_heads, group_size, cache_len),
        cache_values,
        preferred_element_type=jnp.float32,
    )
    attended = (
        attended
        + own_weight.astype(jnp.float32).reshape(rows_here, key_heads, group_size)[:, :, :, None]
        * value_new.astype(jnp.float32)[:, :, None, :]
    )
    attended = attended.reshape(rows_here, query_heads * HD).astype(jnp.bfloat16)
    return attended, key_new, value_new, new_logsum


def rest_general(attended, hidden, out_weight, ffn_gain, expert_ids, expert_scores,
                 gate_weights, up_weights, down_weights):
    rows_here = hidden.shape[0]
    whole_heads = lax.all_gather(attended, "tp", axis=1, tiled=True)
    projected = lax.dot_general(
        lax.all_gather(whole_heads, "ep", axis=0, tiled=True),
        out_weight,
        (((1,), (1,)), ((), ())),
        preferred_element_type=jnp.float32,
    ).astype(jnp.bfloat16)
    mixed = lax.all_to_all(projected, "ep", split_axis=0, concat_axis=1, tiled=True)
    residual = hidden.astype(jnp.float32) + mixed.astype(jnp.float32)
    ffn_in = root_norm(residual, ffn_gain).astype(jnp.bfloat16)
    ep_size = lax.axis_size("ep")
    local_experts = gate_weights.shape[0]
    experts = ep_size * local_experts
    route_count = rows_here * TOP_K
    capacity = 2 * ((route_count + experts - 1) // experts)
    flat_ids = expert_ids.reshape(route_count)
    onehot = (flat_ids[:, None] == jnp.arange(experts, dtype=jnp.int32)[None, :]).astype(jnp.int32)
    running = jnp.cumsum(onehot, axis=0)
    slot_index = jnp.sum(running * onehot, axis=1) - 1
    target = flat_ids * capacity + slot_index
    dispatch_map = (
        target[:, None] == jnp.arange(experts * capacity, dtype=jnp.int32)[None, :]
    ).astype(jnp.bfloat16)
    route_rows = jnp.repeat(ffn_in, TOP_K, axis=0)
    outgoing = lax.dot_general(
        dispatch_map, route_rows, (((0,), (0,)), ((), ())), preferred_element_type=jnp.float32
    )
    outgoing = outgoing.astype(jnp.bfloat16).reshape(
        ep_size, local_experts, capacity, ffn_in.shape[1]
    )
    arrived = lax.all_to_all(outgoing, "ep", split_axis=0, concat_axis=0, tiled=True)
    gate_act = jnp.einsum(
        "sekd,edf->sekf", arrived, gate_weights, preferred_element_type=jnp.float32
    )
    up_act = jnp.einsum("sekd,edf->sekf", arrived, up_weights, preferred_element_type=jnp.float32)
    hidden_act = (jax.nn.silu(gate_act) * up_act).astype(jnp.bfloat16)
    partial_out = jnp.einsum(
        "sekf,efd->sekd", hidden_act, down_weights, preferred_element_type=jnp.float32
    )
    half_sum = lax.psum_scatter(
        partial_out.astype(jnp.bfloat16), "tp", scatter_dimension=3, tiled=True
    )
    sent_back = lax.all_to_all(half_sum, "ep", split_axis=0, concat_axis=0, tiled=True)
    share_width = sent_back.shape[-1]
    picked = jnp.dot(
        dispatch_map,
        sent_back.reshape(experts * capacity, share_width),
        preferred_element_type=jnp.float32,
    )
    route_weight = expert_scores / jnp.sum(expert_scores, axis=-1, keepdims=True)
    expert_mix = jnp.sum(
        picked.reshape(rows_here, TOP_K, share_width) * route_weight[:, :, None], axis=1
    )
    own_part = lax.dynamic_slice_in_dim(
        residual, lax.axis_index("tp") * share_width, share_width, 1
    )
    updated = lax.all_gather((own_part + expert_mix).astype(jnp.bfloat16), "tp", axis=1, tiled=True)
    return updated


MESH = pl.DeviceIdType.MESH
PLANE = 4


def step_body(n, len_ref, fbias_ref, hid_ref, again_ref, fgain_ref, ids_ref, rscore_ref,
              qw_hbm, kw_hbm, vw_hbm, fw_hbm, keys_hbm, vals_hbm, logs_hbm, ow_hbm, gate_hbm, up_hbm, down_hbm,
              out_ref, key_ref, val_ref, nlog_ref,
              qw, kw, vw, fw, keys, vals, logs, scores, maxes, lasts, sums, mixed_heads, att, ow, gate, up, down,
              hidl, psend, pin, mixl, mixin, rows, ssq, wts, gacc, uacc, act, eout, back, fsum, far, upd,
              send, recv, local):
    f32, bf16 = jnp.float32, jnp.bfloat16
    me, tp = lax.axis_index("ep"), lax.axis_index("tp")
    seqs, width = hid_ref.shape
    cols = qw.shape[1]
    heads = cols // HD
    cache_len = keys.shape[2]
    outer = n // PLANE
    feats = ow.shape[1]
    pf = PLANE * feats
    xq = pf // 2
    line = outer * seqs
    z, xy = me // PLANE, lax.rem(me, PLANE)
    x, y = lax.rem(xy, 2), xy // 2
    spots = [y * 2 + (1 - x), (1 - y) * 2 + x, (1 - y) * 2 + (1 - x)]
    plane = [z * PLANE + s for s in spots]

    def zdev(zz):
        return zz * PLANE + xy

    near_tables = [sorted([j for j in range(outer) if j != i], key=lambda j: (abs(j - i), j)) for i in range(outer)]

    def nth(k):
        value = near_tables[0][k]
        for i in range(1, outer):
            value = jnp.where(z == i, near_tables[i][k], value)
        return value

    zs = [nth(k) for k in range(outer - 1)]
    used = {"s": 0, "r": 0, "l": 0}

    def take(kind, count=1):
        base = used[kind]
        used[kind] += count
        return base

    sent = []

    def copy(src, dst, s, r, ep, core):
        return pltpu.make_async_remote_copy(src_ref=src, dst_ref=dst, send_sem=send.at[s], recv_sem=recv.at[r],
                                            device_id=(ep, core), device_id_type=MESH)

    def begin(src, dst, r, ep, core):
        c = copy(src, dst, take("s"), r, ep, core)
        c.start()
        sent.append(c)
        return c

    def arrived(dst, r):
        copy(dst, dst, 0, r, me, 1 - tp).wait_recv()

    def load(src, dst):
        c = pltpu.make_async_copy(src, dst, local.at[take("l")])
        c.start()
        return c

    def sl(i, size):
        return pl.ds(pl.multiple_of(i * size, size), size)

    ow_load = load(ow_hbm.at[:, sl(tp, cols)], ow.at[xy])
    small = [load(kw_hbm, kw), load(vw_hbm, vw), load(fw_hbm, fw)]
    qchunk = width // 4
    qw_loads = [load(qw_hbm.at[pl.ds(i * qchunk, qchunk)], qw.at[pl.ds(i * qchunk, qchunk)]) for i in range(4)]
    part = seqs // 4
    key_loads = [load(keys_hbm.at[pl.ds(i * part, part), 0], keys.at[pl.ds(i * part, part)]) for i in range(4)]
    log_loads = [load(logs_hbm.at[pl.ds(i * part, part)], logs.at[pl.ds(i * part, part)]) for i in range(4)]
    val_loads = [load(vals_hbm.at[pl.ds(i * part, part), 0], vals.at[pl.ds(i * part, part)]) for i in range(4)]

    barrier = pltpu.get_barrier_semaphore()
    for d in range(1, outer):
        pl.semaphore_signal(barrier, inc=1, device_id=(zdev(lax.rem(z + d, outer)), tp), device_id_type=MESH)
    for p in plane:
        pl.semaphore_signal(barrier, inc=1, device_id=(p, tp), device_id_type=MESH)
    pl.semaphore_signal(barrier, inc=1, device_id=(me, 1 - tp), device_id_type=MESH)

    normed = root_norm(hid_ref[...], again_ref[...]).astype(bf16)
    rscore = rscore_ref[...]
    route = rscore / jnp.sum(rscore, axis=-1, keepdims=True)
    lanes = lax.broadcasted_iota(jnp.int32, (seqs, 128), 1)
    table = jnp.zeros((seqs, 128), f32)
    for k in range(TOP_K):
        table = table + jnp.where(lanes == ids_ref[:, k:k + 1], route[:, k:k + 1], 0.0)
    wts[xy, sl(z, seqs), :] = table

    pl.semaphore_wait(barrier, outer - 1 + 3 + 1)

    hf = feats // 2
    lo, hi = pl.ds(0, hf), pl.ds(hf, hf)
    ow_load.wait()
    ow_r = take("r", 6)
    begin(ow.at[xy, lo], ow.at[xy, lo], ow_r, plane[0], tp)
    begin(ow.at[xy, hi], ow.at[xy, hi], ow_r + 3, plane[1], tp)
    begin(ow.at[xy, hi], ow.at[xy, hi], ow_r + 1, plane[0], tp)
    begin(ow.at[xy, lo], ow.at[xy, lo], ow_r + 2, plane[1], tp)
    hid_r = take("r", outer)
    for zz in zs:
        begin(hid_ref.at[:, pl.ds(pl.multiple_of(zz * pf + tp * xq, xq), xq)], hidl.at[sl(z, seqs)],
              hid_r + z, zdev(zz), tp)
    hidl[sl(z, seqs), :] = hid_ref[:, pl.ds(pl.multiple_of(z * pf + tp * xq, xq), xq)]
    wt_r = take("r", outer)
    for zz in zs:
        begin(wts.at[xy, sl(z, seqs)], wts.at[xy, sl(z, seqs)], wt_r + z, zdev(zz), tp)

    acc = jnp.zeros((seqs, cols), f32)
    for i in range(4):
        qw_loads[i].wait()
        acc = acc + jnp.dot(normed[:, i * qchunk:(i + 1) * qchunk], qw[pl.ds(i * qchunk, qchunk), :],
                            preferred_element_type=f32)
    queries = acc.astype(bf16).astype(f32) * (HD ** -0.5)
    for c in small:
        c.wait()
    key_new = jnp.dot(normed, kw[...], preferred_element_type=f32).astype(bf16)
    value_new = jnp.dot(normed, vw[...], preferred_element_type=f32).astype(bf16)
    key_ref[...] = key_new
    val_ref[...] = value_new
    hl = lax.broadcasted_iota(jnp.int32, (seqs, heads), 1)
    fb = jnp.zeros((seqs, heads), f32)
    for h in range(heads):
        fb = jnp.where(hl == h, fbias_ref[h], fb)
    pre = jnp.dot(normed, fw[...], preferred_element_type=f32) + fb
    log_forget = jnp.minimum(pre, 0.0) - jnp.log1p(jnp.exp(-jnp.abs(pre)))

    gate_loads, up_loads = [], []
    for t in range(2):
        for zc in range(outer):
            rows_from = pl.ds(zc * pf + t * xq, xq)
            gate_loads.append(load(gate_hbm.at[0, rows_from], gate.at[t * outer + zc]))
            up_loads.append(load(up_hbm.at[0, rows_from], up.at[t * outer + zc]))
    down_loads, down_r = [], take("r", outer)
    for zc in range(outer):
        mine = pl.ds(pl.multiple_of(zc * pf + tp * xq, xq), xq)
        other = pl.ds(pl.multiple_of(zc * pf + (1 - tp) * xq, xq), xq)
        down_loads.append(load(down_hbm.at[0, :, mine], down.at[tp, :, pl.ds(zc * xq, xq)]))
        begin(down_hbm.at[0, :, other], down.at[tp, :, pl.ds(zc * xq, xq)], down_r + zc, me, 1 - tp)

    total = seqs * heads

    def spread(v):
        return jnp.broadcast_to(v[:, None, :], (seqs, heads, v.shape[1])).reshape(total, v.shape[1])

    row_head = lax.rem(lax.broadcasted_iota(jnp.int32, (total, 128), 0), heads)
    picked = jnp.zeros((total, 128), f32)
    for j in range(cols // 128):
        picked = jnp.where(row_head // 2 == j, spread(queries[:, j * 128:(j + 1) * 128]), picked)
    picked = jnp.where(lax.rem(row_head, 2) == 0, picked, pltpu.roll(picked, HD, 1))[:, :HD]
    per_head = picked.astype(bf16)
    own = jnp.sum(picked * spread(key_new.astype(f32)), axis=-1, keepdims=True)

    positions = lax.broadcasted_iota(jnp.int32, (heads, cache_len), 1)
    for s in range(seqs):
        if s % part == 0:
            key_loads[s // part].wait()
            log_loads[s // part].wait()
        here = pl.ds(s * heads, heads)
        size = len_ref[s]
        level = logs[s]
        dots = jnp.dot(per_head[s * heads:(s + 1) * heads, :], keys[s], preferred_element_type=f32)
        past = jnp.where(positions < size, dots - level, -jnp.inf)
        scores[here, :] = past
        maxes[here, :] = jnp.broadcast_to(jnp.max(past, axis=-1, keepdims=True), (heads, 128))
        last = jnp.sum(jnp.where(positions == size - 1, level, 0.0), axis=-1, keepdims=True)
        lasts[here, :] = jnp.broadcast_to(last, (heads, 128))
    own_lane = lax.broadcasted_iota(jnp.int32, (total, heads), 1)
    own_row = lax.rem(lax.broadcasted_iota(jnp.int32, (total, heads), 0), heads)
    forget_col = jnp.sum(jnp.where(own_lane == own_row, spread(log_forget), 0.0), axis=-1, keepdims=True)
    newlog = lasts[:, :1] + forget_col
    nlog_ref[...] = jnp.sum(jnp.where(own_lane == own_row, jnp.broadcast_to(newlog, (total, heads)), 0.0)
                            .reshape(seqs, heads, heads), axis=1)
    own = own - newlog
    peak = jnp.maximum(maxes[:, :1], own)
    maxes[...] = jnp.broadcast_to(peak, (total, 128))
    for s in range(seqs):
        if s % part == 0:
            val_loads[s // part].wait()
        here = pl.ds(s * heads, heads)
        weights = jnp.exp(scores[here, :] - maxes[here, :][:, :1])
        sums[here, :] = jnp.broadcast_to(jnp.sum(weights, axis=-1, keepdims=True), (heads, 128))
        mixed_heads[here, :HD] = lax.dot_general(weights.astype(bf16), vals[s], (((1,), (1,)), ((), ())),
                                                 preferred_element_type=f32)
    own_exp = jnp.exp(own - peak)
    inverse = 1.0 / (sums[:, :1] + own_exp)
    outs = (mixed_heads[:, :HD] + own_exp * spread(value_new.astype(f32))) * inverse
    mixed_heads[:, :HD] = outs
    mixed_heads[:, HD:] = outs
    wide = lax.broadcasted_iota(jnp.int32, (seqs, 128), 1)
    for j in range(cols // 128):
        even = mixed_heads[pl.ds(2 * j, seqs, stride=heads), :]
        odd = mixed_heads[pl.ds(2 * j + 1, seqs, stride=heads), :]
        att[sl(z, seqs), j * 128:(j + 1) * 128] = jnp.where(wide < HD, even, odd).astype(bf16)

    att_r = take("r", outer)
    for zz in reversed(zs):
        begin(att.at[sl(z, seqs)], att.at[sl(z, seqs)], att_r + z, zdev(zz), tp)
    arrived(ow.at[spots[0], lo], ow_r)
    relay_r = take("r", 2)
    begin(ow.at[spots[0], lo], ow.at[spots[0], lo], relay_r, plane[1], tp)
    arrived(ow.at[spots[1], hi], ow_r + 3)
    begin(ow.at[spots[1], hi], ow.at[spots[1], hi], relay_r + 1, plane[0], tp)
    for zz in zs:
        arrived(wts.at[xy, sl(zz, seqs)], wt_r + zz)
    wline_r = take("r", 3)
    for i in range(3):
        begin(wts.at[xy], wts.at[xy], wline_r + i, plane[i], tp)
    arrived(ow.at[spots[0], hi], ow_r + 1)
    arrived(ow.at[spots[1], lo], ow_r + 2)
    for zz in zs:
        arrived(hidl.at[sl(zz, seqs)], hid_r + zz)
    for zz in zs:
        arrived(att.at[sl(zz, seqs)], att_r + zz)
    arrived(ow.at[spots[2], lo], relay_r)
    arrived(ow.at[spots[2], hi], relay_r + 1)
    lines = att[...]

    def project(t):
        return [lax.dot_general(lines, ow[2 * t + i], (((1,), (1,)), ((), ())), preferred_element_type=f32)
                for i in range(2)]

    for i, v in enumerate(project(1 - tp)):
        psend[:, i * feats:(i + 1) * feats] = v
    p_r = take("r")
    begin(psend, pin, p_r, me, 1 - tp)
    kept = jnp.concatenate(project(tp), axis=1)
    arrived(pin, p_r)
    mixed = (kept + pin[...]).astype(bf16)
    residual = hidl[...].astype(f32) + mixed.astype(f32)
    gain = fgain_ref[:, pl.ds(pl.multiple_of(z * pf + tp * xq, xq), xq)].astype(f32)
    block = tp * outer + z
    rows[block, xy] = (residual * gain).astype(bf16)
    square = jnp.sum(residual * residual, axis=-1, keepdims=True)
    eye = (lax.broadcasted_iota(jnp.int32, (line, line), 0) == lax.broadcasted_iota(jnp.int32, (line, line), 1))
    flat = jnp.sum(jnp.where(eye, jnp.broadcast_to(square, (line, line)), 0.0), axis=0, keepdims=True)
    ssq[block, xy] = jnp.broadcast_to(flat, (8, line))
    mixl[...] = mixed

    zrow_r, zsq_r = take("r", outer), take("r", outer)
    prow_r, psq_r = take("r", 3 * outer), take("r", 3 * outer)
    crow_r, csq_r = take("r", 4 * outer), take("r", 4 * outer)

    def out_to_plane(zz):
        b = tp * outer + zz
        for i in range(3):
            begin(rows.at[b, xy], rows.at[b, xy], prow_r + i * outer + zz, plane[i], tp)
            begin(ssq.at[b, xy], ssq.at[b, xy], psq_r + i * outer + zz, plane[i], tp)

    def to_partner(zz, i, spot):
        b = tp * outer + zz
        begin(rows.at[b, spot], rows.at[b, spot], crow_r + i * outer + zz, me, 1 - tp)
        begin(ssq.at[b, spot], ssq.at[b, spot], csq_r + i * outer + zz, me, 1 - tp)

    for zz in reversed(zs):
        begin(rows.at[block, xy], rows.at[block, xy], zrow_r + z, zdev(zz), tp)
        begin(ssq.at[block, xy], ssq.at[block, xy], zsq_r + z, zdev(zz), tp)
    out_to_plane(z)
    to_partner(z, 3, xy)
    mix_r = take("r", outer)
    for zz in zs:
        begin(mixl.at[sl(zz, seqs)], mixin.at[z], mix_r + z, zdev(zz), tp)
    mixin[z] = mixl[sl(z, seqs), :]
    for zz in zs:
        b = tp * outer + zz
        arrived(rows.at[b, xy], zrow_r + zz)
        arrived(ssq.at[b, xy], zsq_r + zz)
        out_to_plane(zz)
        to_partner(zz, 3, xy)
    for c in gate_loads + up_loads + down_loads:
        c.wait()
    for i in range(3):
        arrived(wts.at[spots[i]], wline_r + i)

    def gather_block(t, zz, first):
        b = t * outer + zz
        left = rows[b].reshape(PLANE * line, xq)
        g = jnp.dot(left, gate[b], preferred_element_type=f32)
        u = jnp.dot(left, up[b], preferred_element_type=f32)
        gacc[...] = g if first else gacc[...] + g
        uacc[...] = u if first else uacc[...] + u

    order = [z] + zs
    for k in range(outer + 1):
        if k < outer:
            b = tp * outer + order[k]
            for i in range(3):
                arrived(rows.at[b, spots[i]], prow_r + i * outer + order[k])
                arrived(ssq.at[b, spots[i]], psq_r + i * outer + order[k])
                to_partner(order[k], i, spots[i])
            gather_block(tp, order[k], k == 0)
        if k > 0:
            b = (1 - tp) * outer + order[k - 1]
            for i, spot in enumerate(spots + [xy]):
                arrived(rows.at[b, spot], crow_r + i * outer + order[k - 1])
                arrived(ssq.at[b, spot], csq_r + i * outer + order[k - 1])
            gather_block(1 - tp, order[k - 1], False)
    for q in range(PLANE):
        whole = ssq[0, q][:1, :]
        for b in range(1, 2 * outer):
            whole = whole + ssq[b, q][:1, :]
        scale = lax.rsqrt(whole * (1.0 / width) + epsilon)
        scale = jnp.sum(jnp.where(eye, jnp.broadcast_to(scale, (line, line)), 0.0), axis=1, keepdims=True)
        g = gacc[pl.ds(q * line, line), :] * scale
        u = uacc[pl.ds(q * line, line), :] * scale
        act[tp, q] = (g / (1.0 + jnp.exp(-g)) * u).astype(bf16)
    act_r = take("r")
    begin(act.at[tp], act.at[tp], act_r, me, 1 - tp)
    for zc in range(outer):
        arrived(down.at[1 - tp, :, pl.ds(zc * xq, xq)], down_r + zc)
    arrived(act.at[1 - tp], act_r)

    back_r = take("r", 3 * outer)
    out_order = list(reversed(zs)) + [z]
    which = lax.broadcasted_iota(jnp.int32, (PLANE * seqs, 128), 1) == me
    for zz in out_order:
        def tokens(ref):
            return ref[:, sl(zz, seqs), :].reshape(PLANE * seqs, ref.shape[2])

        weight = jnp.sum(jnp.where(which, tokens(wts), 0.0), axis=-1, keepdims=True)
        made = (jnp.dot(tokens(act.at[0]), down[0], preferred_element_type=f32)
                + jnp.dot(tokens(act.at[1]), down[1], preferred_element_type=f32)) * weight
        eout[zz] = made.astype(bf16).reshape(PLANE, seqs, made.shape[1])
        for i in (2, 0, 1):
            begin(eout.at[zz, spots[i]], back.at[i, zz], back_r + i * outer + zz, plane[i], tp)
    far_r = take("r", outer)
    for zz in out_order:
        summed = eout[zz, xy].astype(f32)
        for i in range(3):
            arrived(back.at[i, zz], back_r + i * outer + zz)
            summed = summed + back[i, zz].astype(f32)
        if zz is not z:
            fsum[zz] = summed.astype(bf16)
            begin(fsum.at[zz], far.at[z], far_r + z, zdev(zz), tp)
    for zz in zs:
        arrived(mixin.at[zz], mix_r + zz)
    for zz in zs:
        arrived(far.at[zz], far_r + zz)
        summed = summed + far[zz].astype(f32)
    for zc in range(outer):
        here = hid_ref[:, pl.ds(pl.multiple_of(zc * pf + tp * xq, xq), xq)].astype(f32) + mixin[zc].astype(f32)
        upd[tp, :, zc * xq:(zc + 1) * xq] = (here + summed[:, zc * xq:(zc + 1) * xq]).astype(bf16)
    u_r = take("r")
    begin(upd.at[tp], upd.at[tp], u_r, me, 1 - tp)
    arrived(upd.at[1 - tp], u_r)
    for t in range(2):
        for zc in range(outer):
            out_ref[:, zc * pf + t * xq:zc * pf + (t + 1) * xq] = upd[t, :, zc * xq:(zc + 1) * xq]
    for c in sent:
        c.wait_send()
    assert used["s"] <= send.shape[0] and used["r"] <= recv.shape[0] and used["l"] <= local.shape[0], used


def step_kernel(hidden, attn_gain, query_weight, key_weight, value_weight, forget_weight, forget_bias,
                cache_keys, cache_values, cache_logsum, lengths, out_weight, ffn_gain, expert_ids, expert_scores,
                gate_weights, up_weights, down_weights):
    n = lax.axis_size("ep")
    seqs, width = hidden.shape
    cols = query_weight.shape[1]
    heads = cols // HD
    cache_len = cache_keys.shape[3]
    feats = out_weight.shape[0]
    units = gate_weights.shape[2]
    outer = n // PLANE
    line = outer * seqs
    xq = PLANE * feats // 2
    half = width // 2
    bf16, f32 = jnp.bfloat16, jnp.float32
    vmem = pl.BlockSpec(memory_space=pltpu.VMEM)
    smem = pl.BlockSpec(memory_space=pltpu.SMEM)
    hbm = pl.BlockSpec(memory_space=pl.ANY)
    v = pltpu.VMEM
    updated, key_new, value_new, new_logsum = pl.pallas_call(
        functools.partial(step_body, n),
        out_shape=[jax.ShapeDtypeStruct((seqs, width), bf16), jax.ShapeDtypeStruct((seqs, HD), bf16),
                   jax.ShapeDtypeStruct((seqs, HD), bf16), jax.ShapeDtypeStruct((seqs, heads), f32)],
        in_specs=[smem] * 2 + [vmem] * 5 + [hbm] * 11,
        out_specs=[vmem] * 4,
        scratch_shapes=[
            v((width, cols), bf16), v((width, HD), bf16), v((width, HD), bf16), v((width, heads), bf16),
            v((seqs, HD, cache_len), bf16), v((seqs, HD, cache_len), bf16), v((seqs, heads, cache_len), f32),
            v((seqs * heads, cache_len), f32), v((seqs * heads, 128), f32), v((seqs * heads, 128), f32),
            v((seqs * heads, 128), f32), v((seqs * heads, 2 * HD), f32),
            v((line, cols), bf16), v((PLANE, feats, cols), bf16),
            v((2 * outer, xq, units), bf16), v((2 * outer, xq, units), bf16), v((2, units, half), bf16),
            v((line, xq), bf16), v((line, xq), f32), v((line, xq), f32), v((line, xq), bf16),
            v((outer, seqs, xq), bf16),
            v((2 * outer, PLANE, line, xq), bf16), v((2 * outer, PLANE, 8, line), f32), v((PLANE, line, 128), f32),
            v((PLANE * line, units), f32), v((PLANE * line, units), f32), v((2, PLANE, line, units), bf16),
            v((outer, PLANE, seqs, half), bf16), v((3, outer, seqs, half), bf16),
            v((outer, seqs, half), bf16), v((outer, seqs, half), bf16), v((2, seqs, half), bf16),
            pltpu.SemaphoreType.DMA((200,)), pltpu.SemaphoreType.DMA((200,)), pltpu.SemaphoreType.DMA((64,)),
        ],
        compiler_params=pltpu.CompilerParams(
            collective_id=0, has_side_effects=True, vmem_limit_bytes=60 * 1024 * 1024),
    )(lengths, forget_bias, hidden, attn_gain[None, :], ffn_gain[None, :], expert_ids, expert_scores,
      query_weight, key_weight, value_weight, forget_weight, cache_keys, cache_values, cache_logsum,
      out_weight, gate_weights, up_weights, down_weights)
    return updated, key_new.reshape(seqs, 1, HD), value_new.reshape(seqs, 1, HD), new_logsum


def per_device(hidden, attn_gain, query_weight, key_weight, value_weight, forget_weight, forget_bias,
               cache_keys, cache_values, cache_logsum, lengths, out_weight, ffn_gain, expert_ids, expert_scores,
               gate_weights, up_weights, down_weights):
    n = lax.axis_size("ep")
    seqs, width = hidden.shape
    fits = (
        n % PLANE == 0
        and lax.axis_size("tp") == 2
        and gate_weights.shape[0] == 1
        and cache_keys.shape[1] == 1
        and seqs % 16 == 0
        and (query_weight.shape[1] // HD) % 16 == 0
        and out_weight.shape[0] % 128 == 0
        and n <= 128
    )
    if fits:
        return step_kernel(
            hidden, attn_gain, query_weight, key_weight, value_weight, forget_weight, forget_bias,
            cache_keys, cache_values, cache_logsum, lengths, out_weight, ffn_gain, expert_ids, expert_scores,
            gate_weights, up_weights, down_weights)
    attended, key_new, value_new, new_logsum = attend(
        hidden, attn_gain, query_weight, key_weight, value_weight, forget_weight, forget_bias,
        cache_keys, cache_values, cache_logsum, lengths)
    updated = rest_general(attended, hidden, out_weight, ffn_gain, expert_ids, expert_scores,
                           gate_weights, up_weights, down_weights)
    return (updated, key_new, value_new, new_logsum)


def solution(mesh):
    in_specs = (
        P("ep", None),
        P(),
        P(None, "tp"),
        P(None, "tp"),
        P(None, "tp"),
        P(None, "tp"),
        P("tp"),
        P("ep", "tp", None, None),
        P("ep", "tp", None, None),
        P("ep", "tp", None),
        P("ep"),
        P("ep", None),
        P(),
        P("ep", None),
        P("ep", None),
        P("ep", None, "tp"),
        P("ep", None, "tp"),
        P("ep", "tp", None),
    )
    out_specs = (P("ep", None), P("ep", "tp", None), P("ep", "tp", None), P("ep", "tp"))
    return jax.shard_map(
        per_device, mesh=mesh, in_specs=in_specs, out_specs=out_specs, check_vma=False
    )
```

```python
import functools
import math

import jax
import jax.numpy as jnp
from jax import lax
from jax.experimental import pallas as pl
from jax.experimental.pallas import tpu as pltpu
from jax.sharding import PartitionSpec as P

HD = 64
TOP_K = 6


epsilon = 1e-06


def root_norm(values_in, gain):
    floats = values_in.astype(jnp.float32)
    inv_root = lax.rsqrt(jnp.mean(floats * floats, axis=-1, keepdims=True) + epsilon)
    return floats * inv_root * gain.astype(jnp.float32)


def attend(hidden, attn_gain, query_weight, key_weight, value_weight, forget_weight, forget_bias,
           cache_keys, cache_values, cache_logsum, lengths):
    rows_here = hidden.shape[0]
    query_heads = query_weight.shape[1] // HD
    key_heads = key_weight.shape[1] // HD
    group_size = query_heads // key_heads
    cache_len = cache_keys.shape[-1]
    score_scale = HD ** (-0.5)
    normed = root_norm(hidden, attn_gain).astype(jnp.bfloat16)
    queries = jnp.dot(normed, query_weight, preferred_element_type=jnp.float32).astype(jnp.bfloat16)
    key_new = (
        jnp.dot(normed, key_weight, preferred_element_type=jnp.float32)
        .astype(jnp.bfloat16)
        .reshape(rows_here, key_heads, HD)
    )
    value_new = (
        jnp.dot(normed, value_weight, preferred_element_type=jnp.float32)
        .astype(jnp.bfloat16)
        .reshape(rows_here, key_heads, HD)
    )
    log_forget = jax.nn.log_sigmoid(
        jnp.dot(normed, forget_weight, preferred_element_type=jnp.float32) + forget_bias
    )
    positions = jnp.arange(cache_len, dtype=jnp.int32)
    is_last = positions[None, :] == (lengths - 1)[:, None]
    new_logsum = jnp.sum(jnp.where(is_last[:, None, :], cache_logsum, 0.0), axis=-1) + log_forget
    grouped = queries.reshape(rows_here, key_heads, group_size, HD)
    scores = jnp.einsum("sgjd,sgdp->sgjp", grouped, cache_keys, preferred_element_type=jnp.float32)
    scores = scores.reshape(rows_here, query_heads, cache_len) * score_scale
    scores = scores + new_logsum[:, :, None] - cache_logsum
    is_live = positions[None, :] < lengths[:, None]
    scores = jnp.where(is_live[:, None, :], scores, -jnp.inf)
    own_score = (
        jnp.einsum("sgjd,sgd->sgj", grouped, key_new, preferred_element_type=jnp.float32).reshape(
            rows_here, query_heads
        )
        * score_scale
    )
    top_score = jnp.maximum(jnp.max(scores, axis=-1), own_score)
    past_exp = jnp.exp(scores - top_score[:, :, None])
    own_exp = jnp.exp(own_score - top_score)
    denominator = jnp.sum(past_exp, axis=-1) + own_exp
    past_weight = (past_exp / denominator[:, :, None]).astype(jnp.bfloat16)
    own_weight = (own_exp / denominator).astype(jnp.bfloat16)
    attended = jnp.einsum(
        "sgjp,sgdp->sgjd",
        past_weight.reshape(rows_here, key_heads, group_size, cache_len),
        cache_values,
        preferred_element_type=jnp.float32,
    )
    attended = (
        attended
        + own_weight.astype(jnp.float32).reshape(rows_here, key_heads, group_size)[:, :, :, None]
        * value_new.astype(jnp.float32)[:, :, None, :]
    )
    attended = attended.reshape(rows_here, query_heads * HD).astype(jnp.bfloat16)
    return attended, key_new, value_new, new_logsum


def rest_general(attended, hidden, out_weight, ffn_gain, expert_ids, expert_scores,
                 gate_weights, up_weights, down_weights):
    rows_here = hidden.shape[0]
    whole_heads = lax.all_gather(attended, "tp", axis=1, tiled=True)
    projected = lax.dot_general(
        lax.all_gather(whole_heads, "ep", axis=0, tiled=True),
        out_weight,
        (((1,), (1,)), ((), ())),
        preferred_element_type=jnp.float32,
    ).astype(jnp.bfloat16)
    mixed = lax.all_to_all(projected, "ep", split_axis=0, concat_axis=1, tiled=True)
    residual = hidden.astype(jnp.float32) + mixed.astype(jnp.float32)
    ffn_in = root_norm(residual, ffn_gain).astype(jnp.bfloat16)
    ep_size = lax.axis_size("ep")
    local_experts = gate_weights.shape[0]
    experts = ep_size * local_experts
    route_count = rows_here * TOP_K
    capacity = 2 * ((route_count + experts - 1) // experts)
    flat_ids = expert_ids.reshape(route_count)
    onehot = (flat_ids[:, None] == jnp.arange(experts, dtype=jnp.int32)[None, :]).astype(jnp.int32)
    running = jnp.cumsum(onehot, axis=0)
    slot_index = jnp.sum(running * onehot, axis=1) - 1
    target = flat_ids * capacity + slot_index
    dispatch_map = (
        target[:, None] == jnp.arange(experts * capacity, dtype=jnp.int32)[None, :]
    ).astype(jnp.bfloat16)
    route_rows = jnp.repeat(ffn_in, TOP_K, axis=0)
    outgoing = lax.dot_general(
        dispatch_map, route_rows, (((0,), (0,)), ((), ())), preferred_element_type=jnp.float32
    )
    outgoing = outgoing.astype(jnp.bfloat16).reshape(
        ep_size, local_experts, capacity, ffn_in.shape[1]
    )
    arrived = lax.all_to_all(outgoing, "ep", split_axis=0, concat_axis=0, tiled=True)
    gate_act = jnp.einsum(
        "sekd,edf->sekf", arrived, gate_weights, preferred_element_type=jnp.float32
    )
    up_act = jnp.einsum("sekd,edf->sekf", arrived, up_weights, preferred_element_type=jnp.float32)
    hidden_act = (jax.nn.silu(gate_act) * up_act).astype(jnp.bfloat16)
    partial_out = jnp.einsum(
        "sekf,efd->sekd", hidden_act, down_weights, preferred_element_type=jnp.float32
    )
    half_sum = lax.psum_scatter(
        partial_out.astype(jnp.bfloat16), "tp", scatter_dimension=3, tiled=True
    )
    sent_back = lax.all_to_all(half_sum, "ep", split_axis=0, concat_axis=0, tiled=True)
    share_width = sent_back.shape[-1]
    picked = jnp.dot(
        dispatch_map,
        sent_back.reshape(experts * capacity, share_width),
        preferred_element_type=jnp.float32,
    )
    route_weight = expert_scores / jnp.sum(expert_scores, axis=-1, keepdims=True)
    expert_mix = jnp.sum(
        picked.reshape(rows_here, TOP_K, share_width) * route_weight[:, :, None], axis=1
    )
    own_part = lax.dynamic_slice_in_dim(
        residual, lax.axis_index("tp") * share_width, share_width, 1
    )
    updated = lax.all_gather((own_part + expert_mix).astype(jnp.bfloat16), "tp", axis=1, tiled=True)
    return updated


MESH = pl.DeviceIdType.MESH
PLANE = 4


def step_body(n, len_hbm, fbias_hbm, hid_hbm, again_hbm, fgain_hbm, ids_hbm, rscore_hbm,
              qw_hbm, kw_hbm, vw_hbm, fw_hbm, keys_hbm, vals_hbm, logs_hbm, ow_hbm, gate_hbm, up_hbm, down_hbm,
              out_ref, key_ref, val_ref, nlog_ref,
              len_ref, fbias_ref, hid_ref, again, fgain, fgain_row, ids_ref, rscore_ref, qw, kw, vw, fw, keys, vals, logs, scores, maxes, lasts, sums, mixed_heads, att, ow, gate, up, down,
              hidl, psend, pin, mixl, mixin, rows, ssqz, ssqp, ssqt, wts, gacc, uacc, act, eout, back, fsum, far, upd,
              send, recv, local):
    f32, bf16 = jnp.float32, jnp.bfloat16
    me, tp = lax.axis_index("ep"), lax.axis_index("tp")
    seqs, width = hid_ref.shape
    cols = qw.shape[1]
    heads = cols // HD
    cache_len = keys.shape[2]
    outer = n // PLANE
    feats = ow.shape[1]
    pf = PLANE * feats
    xq = pf // 2
    line = outer * seqs
    z, xy = me // PLANE, lax.rem(me, PLANE)
    x, y = lax.rem(xy, 2), xy // 2
    spots = [y * 2 + (1 - x), (1 - y) * 2 + x, (1 - y) * 2 + (1 - x)]
    plane = [z * PLANE + s for s in spots]

    def zdev(zz):
        return zz * PLANE + xy

    near_tables = [sorted([j for j in range(outer) if j != i], key=lambda j: (abs(j - i), j)) for i in range(outer)]

    def nth(k):
        value = near_tables[0][k]
        for i in range(1, outer):
            value = jnp.where(z == i, near_tables[i][k], value)
        return value

    zs = [nth(k) for k in range(outer - 1)]
    used = {"s": 0, "r": 0, "l": 0}

    def take(kind, count=1):
        base = used[kind]
        used[kind] += count
        return base

    def copy(src, dst, s, r, ep, core):
        return pltpu.make_async_remote_copy(src_ref=src, dst_ref=dst, send_sem=send.at[s], recv_sem=recv.at[r],
                                            device_id=(ep, core), device_id_type=MESH)

    groups = []

    def group(whole):
        groups.append((take("s"), whole))
        return groups[-1][0]

    def begin(src, dst, s, r, ep, core):
        copy(src, dst, s, r, ep, core).start()

    def arrived(dst, r):
        copy(dst, dst, 0, r, me, 1 - tp).wait_recv()

    def load(src, dst, l=None):
        c = pltpu.make_async_copy(src, dst, local.at[take("l") if l is None else l])
        c.start()
        return c

    def sl(i, size):
        return pl.ds(pl.multiple_of(i * size, size), size)

    first = [load(hid_hbm, hid_ref), load(again_hbm, again), load(ids_hbm, ids_ref), load(rscore_hbm, rscore_ref)]
    scalars = [load(fbias_hbm, fbias_ref), load(len_hbm, len_ref), load(fgain_hbm, fgain)]
    ow_load = load(ow_hbm.at[:, sl(tp, cols)], ow.at[xy])
    small = [load(kw_hbm, kw), load(vw_hbm, vw), load(fw_hbm, fw)]
    qchunk = width // 4
    qw_loads = [load(qw_hbm.at[pl.ds(i * qchunk, qchunk)], qw.at[pl.ds(i * qchunk, qchunk)]) for i in range(4)]
    part = seqs // 4
    key_loads = [load(keys_hbm.at[pl.ds(i * part, part), 0], keys.at[pl.ds(i * part, part)]) for i in range(4)]
    log_loads = [load(logs_hbm.at[pl.ds(i * part, part)], logs.at[pl.ds(i * part, part)]) for i in range(4)]
    val_loads = [load(vals_hbm.at[pl.ds(i * part, part), 0], vals.at[pl.ds(i * part, part)]) for i in range(4)]

    barrier = pltpu.get_barrier_semaphore()
    for d in range(1, outer):
        pl.semaphore_signal(barrier, inc=1, device_id=(zdev(lax.rem(z + d, outer)), tp), device_id_type=MESH)
    for p in plane:
        pl.semaphore_signal(barrier, inc=1, device_id=(p, tp), device_id_type=MESH)
    pl.semaphore_signal(barrier, inc=1, device_id=(me, 1 - tp), device_id_type=MESH)

    pl.semaphore_wait(barrier, outer - 1 + 3 + 1)

    hf = feats // 2
    lo, hi = pl.ds(0, hf), pl.ds(hf, hf)
    ow_load.wait()
    ow_s, ow_r = group(ow.at[pl.ds(0, 3)]), take("r", 3)
    begin(ow.at[xy, lo], ow.at[xy, lo], ow_s, ow_r, plane[0], tp)
    begin(ow.at[xy, hi], ow.at[xy, hi], ow_s, ow_r + 1, plane[1], tp)
    begin(ow.at[xy, hi], ow.at[xy, hi], ow_s, ow_r + 2, plane[0], tp)
    begin(ow.at[xy, lo], ow.at[xy, lo], ow_s, ow_r + 2, plane[1], tp)

    for c in first:
        c.wait()
    normed = root_norm(hid_ref[...], again[...][None, :]).astype(bf16)
    rscore = rscore_ref[...]
    route = rscore / jnp.sum(rscore, axis=0, keepdims=True)
    ids = ids_ref[...].astype(f32)
    lanes = lax.broadcasted_iota(jnp.int32, (seqs, 128), 1).astype(f32)
    small_eye = (lax.broadcasted_iota(jnp.int32, (seqs, seqs), 0) == lax.broadcasted_iota(jnp.int32, (seqs, seqs), 1))

    def column(row):
        return jnp.sum(jnp.where(small_eye, jnp.broadcast_to(row, (seqs, seqs)), 0.0), axis=1, keepdims=True)

    table = jnp.zeros((seqs, 128), f32)
    for k in range(TOP_K):
        table = table + jnp.where(lanes == column(ids[k:k + 1, :]), column(route[k:k + 1, :]), 0.0)
    wts[3, sl(z, seqs), :] = table

    others = pl.ds(0, (outer - 1) * seqs)
    hid_s, hid_r = group(hidl.at[others]), take("r")
    for zz in zs:
        begin(hid_ref.at[:, pl.ds(pl.multiple_of(zz * pf + tp * xq, xq), xq)], hidl.at[sl(z, seqs)],
              hid_s, hid_r, zdev(zz), tp)
    hidl[sl(z, seqs), :] = hid_ref[:, pl.ds(pl.multiple_of(z * pf + tp * xq, xq), xq)]
    wt_s, wt_r = group(wts.at[0, others]), take("r")
    for zz in zs:
        begin(wts.at[3, sl(z, seqs)], wts.at[3, sl(z, seqs)], wt_s, wt_r, zdev(zz), tp)

    acc = jnp.zeros((seqs, cols), f32)
    for i in range(4):
        qw_loads[i].wait()
        acc = acc + jnp.dot(normed[:, i * qchunk:(i + 1) * qchunk], qw[pl.ds(i * qchunk, qchunk), :],
                            preferred_element_type=f32)
    queries = acc.astype(bf16).astype(f32) * (HD ** -0.5)
    for c in small:
        c.wait()
    for c in scalars:
        c.wait()
    fgain_row[...] = fgain[...].astype(f32)[None, :]

    def new_token(w):
        return lax.dot_general(normed, w[...], (((1,), (1,)), ((), ())), preferred_element_type=f32)

    key_new = new_token(kw).astype(bf16)
    value_new = new_token(vw).astype(bf16)
    key_ref[...] = key_new
    val_ref[...] = value_new
    hl = lax.broadcasted_iota(jnp.int32, (seqs, heads), 1)
    fb = jnp.zeros((seqs, heads), f32)
    for h in range(heads):
        fb = jnp.where(hl == h, fbias_ref[h], fb)
    pre = new_token(fw) + fb
    log_forget = jnp.minimum(pre, 0.0) - jnp.log1p(jnp.exp(-jnp.abs(pre)))

    gate_l, up_l, down_l = take("l"), take("l"), take("l")
    for t in range(2):
        for zc in range(outer):
            rows_from = pl.ds(zc * pf + t * xq, xq)
            load(gate_hbm.at[0, rows_from], gate.at[t * outer + zc], gate_l)
            load(up_hbm.at[0, rows_from], up.at[t * outer + zc], up_l)
    down_s, down_r = group(down.at[0]), take("r")
    for zc in range(outer):
        mine = pl.ds(pl.multiple_of(zc * pf + tp * xq, xq), xq)
        other = pl.ds(pl.multiple_of(zc * pf + (1 - tp) * xq, xq), xq)
        load(down_hbm.at[0, :, mine], down.at[tp, :, pl.ds(zc * xq, xq)], down_l)
        begin(down_hbm.at[0, :, other], down.at[tp, :, pl.ds(zc * xq, xq)], down_s, down_r, me, 1 - tp)

    total = seqs * heads

    def spread(v):
        return jnp.broadcast_to(v[:, None, :], (seqs, heads, v.shape[1])).reshape(total, v.shape[1])

    row_head = lax.rem(lax.broadcasted_iota(jnp.int32, (total, 128), 0), heads)
    picked = jnp.zeros((total, 128), f32)
    for j in range(cols // 128):
        picked = jnp.where(row_head // 2 == j, spread(queries[:, j * 128:(j + 1) * 128]), picked)
    picked = jnp.where(lax.rem(row_head, 2) == 0, picked, pltpu.roll(picked, HD, 1))[:, :HD]
    per_head = picked.astype(bf16)
    own = jnp.sum(picked * spread(key_new.astype(f32)), axis=-1, keepdims=True)

    positions = lax.broadcasted_iota(jnp.int32, (heads, cache_len), 1)
    for s in range(seqs):
        if s % part == 0:
            key_loads[s // part].wait()
            log_loads[s // part].wait()
        here = pl.ds(s * heads, heads)
        size = len_ref[s]
        level = logs[s]
        dots = jnp.dot(per_head[s * heads:(s + 1) * heads, :], keys[s], preferred_element_type=f32)
        past = jnp.where(positions < size, dots - level, -jnp.inf)
        scores[here, :] = past
        maxes[here, :] = jnp.broadcast_to(jnp.max(past, axis=-1, keepdims=True), (heads, 128))
        last = jnp.sum(jnp.where(positions == size - 1, level, 0.0), axis=-1, keepdims=True)
        lasts[here, :] = jnp.broadcast_to(last, (heads, 128))
    own_lane = lax.broadcasted_iota(jnp.int32, (total, heads), 1)
    own_row = lax.rem(lax.broadcasted_iota(jnp.int32, (total, heads), 0), heads)
    forget_col = jnp.sum(jnp.where(own_lane == own_row, spread(log_forget), 0.0), axis=-1, keepdims=True)
    newlog = lasts[:, :1] + forget_col
    nlog_ref[...] = jnp.sum(jnp.where(own_lane == own_row, jnp.broadcast_to(newlog, (total, heads)), 0.0)
                            .reshape(seqs, heads, heads), axis=1)
    own = own - newlog
    peak = jnp.maximum(maxes[:, :1], own)
    maxes[...] = jnp.broadcast_to(peak, (total, 128))
    for s in range(seqs):
        if s % part == 0:
            val_loads[s // part].wait()
        here = pl.ds(s * heads, heads)
        weights = jnp.exp(scores[here, :] - maxes[here, :][:, :1])
        sums[here, :] = jnp.broadcast_to(jnp.sum(weights, axis=-1, keepdims=True), (heads, 128))
        mixed_heads[here, :HD] = lax.dot_general(weights.astype(bf16), vals[s], (((1,), (1,)), ((), ())),
                                                 preferred_element_type=f32)
    own_exp = jnp.exp(own - peak)
    inverse = 1.0 / (sums[:, :1] + own_exp)
    outs = (mixed_heads[:, :HD] + own_exp * spread(value_new.astype(f32))) * inverse
    mixed_heads[:, :HD] = outs
    mixed_heads[:, HD:] = outs
    wide = lax.broadcasted_iota(jnp.int32, (seqs, 128), 1)
    for j in range(cols // 128):
        even = mixed_heads[pl.ds(2 * j, seqs, stride=heads), :]
        odd = mixed_heads[pl.ds(2 * j + 1, seqs, stride=heads), :]
        att[sl(z, seqs), j * 128:(j + 1) * 128] = jnp.where(wide < HD, even, odd).astype(bf16)

    att_s, att_r = group(att.at[others]), take("r")
    for zz in reversed(zs):
        begin(att.at[sl(z, seqs)], att.at[sl(z, seqs)], att_s, att_r, zdev(zz), tp)
    arrived(ow.at[spots[0], lo], ow_r)
    relay_r = take("r")
    begin(ow.at[spots[0], lo], ow.at[spots[0], lo], ow_s, relay_r, plane[1], tp)
    arrived(ow.at[spots[1], hi], ow_r + 1)
    begin(ow.at[spots[1], hi], ow.at[spots[1], hi], ow_s, relay_r, plane[0], tp)
    arrived(wts.at[0, others], wt_r)
    wline_s, wline_r = group(wts.at[pl.ds(0, 3)]), take("r")
    for i in range(3):
        begin(wts.at[3], wts.at[i], wline_s, wline_r, plane[i], tp)
    arrived(ow.at[0], ow_r + 2)
    arrived(hidl.at[others], hid_r)
    arrived(att.at[others], att_r)
    arrived(ow.at[spots[2]], relay_r)
    lines = att[...]

    def project(t):
        return [lax.dot_general(lines, ow[2 * t + i], (((1,), (1,)), ((), ())), preferred_element_type=f32)
                for i in range(2)]

    for i, v in enumerate(project(1 - tp)):
        psend[:, i * feats:(i + 1) * feats] = v
    p_s, p_r = group(psend), take("r")
    begin(psend, pin, p_s, p_r, me, 1 - tp)
    kept = jnp.concatenate(project(tp), axis=1)
    arrived(pin, p_r)
    mixed = (kept + pin[...]).astype(bf16)
    residual = hidl[...].astype(f32) + mixed.astype(f32)
    gain = fgain_row[:, pl.ds(pl.multiple_of(z * pf + tp * xq, xq), xq)]
    block = tp * outer + z
    rows[block, 3] = (residual * gain).astype(bf16)
    square = jnp.sum(residual * residual, axis=-1, keepdims=True)
    eye = (lax.broadcasted_iota(jnp.int32, (line, line), 0) == lax.broadcasted_iota(jnp.int32, (line, line), 1))
    flat = jnp.sum(jnp.where(eye, jnp.broadcast_to(square, (line, line)), 0.0), axis=0, keepdims=True)
    ssqz[z] = jnp.broadcast_to(flat, (8, line))
    mixl[...] = mixed

    zrow_s, zrow_r = group(rows.at[0, pl.ds(0, outer - 1)]), take("r", outer)
    prow_s, prow_r = group(rows.at[pl.ds(0, 3)]), take("r", outer)
    crow_s, crow_r = group(rows.at[pl.ds(0, outer)]), take("r", outer)
    zsq_s, zsq_r = group(ssqz.at[pl.ds(0, outer - 1)]), take("r")
    psq_s, psq_r = group(ssqt.at[pl.ds(0, 3)]), take("r")
    csq_s, csq_r = group(ssqp.at[0]), take("r")
    mix_s, mix_r = group(mixl.at[others]), take("r")

    def out_to_plane(zz):
        b = tp * outer + zz
        for i in (2, 0, 1):
            begin(rows.at[b, 3], rows.at[b, i], prow_s, prow_r + zz, plane[i], tp)

    def own_to_partner(zz):
        b = tp * outer + zz
        begin(rows.at[b, 3], rows.at[b, 3], crow_s, crow_r + zz, me, 1 - tp)

    for zz in reversed(zs):
        begin(rows.at[block, 3], rows.at[block, 3], zrow_s, zrow_r + z, zdev(zz), tp)
    out_to_plane(z)
    own_to_partner(z)
    for zz in zs:
        begin(ssqz.at[z], ssqz.at[z], zsq_s, zsq_r, zdev(zz), tp)
    mixin[z] = mixl[sl(z, seqs), :]
    for zz in zs:
        arrived(rows.at[tp * outer + zz, 3], zrow_r + zz)
        out_to_plane(zz)
        own_to_partner(zz)
    arrived(ssqz.at[pl.ds(0, outer - 1)], zsq_r)
    squares = ssqz[0]
    for i in range(1, outer):
        squares = squares + ssqz[i]
    ssqp[tp] = squares
    begin(ssqp.at[tp], ssqp.at[tp], csq_s, csq_r, me, 1 - tp)
    for zz in zs:
        begin(mixl.at[sl(zz, seqs)], mixin.at[z], mix_s, mix_r, zdev(zz), tp)
    pltpu.make_async_copy(gate, gate, local.at[gate_l]).wait()
    pltpu.make_async_copy(up, up, local.at[up_l]).wait()
    pltpu.make_async_copy(down.at[0], down.at[0], local.at[down_l]).wait()
    arrived(wts.at[pl.ds(0, 3)], wline_r)

    def gather_block(t, zz, first):
        b = t * outer + zz
        left = rows[b].reshape(PLANE * line, xq)
        g = jnp.dot(left, gate[b], preferred_element_type=f32)
        u = jnp.dot(left, up[b], preferred_element_type=f32)
        gacc[...] = g if first else gacc[...] + g
        uacc[...] = u if first else uacc[...] + u

    order = [z] + zs
    for k in range(outer + 1):
        if k < outer:
            b = tp * outer + order[k]
            theirs = rows.at[b, pl.ds(0, 3)]
            arrived(theirs, prow_r + order[k])
            begin(theirs, theirs, crow_s, crow_r + order[k], me, 1 - tp)
            gather_block(tp, order[k], k == 0)
        if k == 0:
            arrived(ssqp.at[1 - tp], csq_r)
            ssqt[3] = ssqp[0] + ssqp[1]
            for i in range(3):
                begin(ssqt.at[3], ssqt.at[i], psq_s, psq_r, plane[i], tp)
        if k > 0:
            b = (1 - tp) * outer + order[k - 1]
            arrived(rows.at[b], crow_r + order[k - 1])
            gather_block(1 - tp, order[k - 1], False)
    arrived(ssqt.at[pl.ds(0, 3)], psq_r)
    for q in range(PLANE):
        scale = lax.rsqrt(ssqt[q][:1, :] * (1.0 / width) + epsilon)
        scale = jnp.sum(jnp.where(eye, jnp.broadcast_to(scale, (line, line)), 0.0), axis=1, keepdims=True)
        g = gacc[pl.ds(q * line, line), :] * scale
        u = uacc[pl.ds(q * line, line), :] * scale
        act[tp, q] = (g / (1.0 + jnp.exp(-g)) * u).astype(bf16)
    act_s, act_r = group(act.at[0]), take("r")
    begin(act.at[tp], act.at[tp], act_s, act_r, me, 1 - tp)
    arrived(down.at[1 - tp], down_r)
    arrived(act.at[1 - tp], act_r)

    back_s, back_r = group(eout.at[pl.ds(0, 3)]), take("r", outer)
    out_order = list(reversed(zs)) + [z]
    which = lax.broadcasted_iota(jnp.int32, (PLANE * seqs, 128), 1) == me
    for zz in out_order:
        def tokens(ref):
            return ref[:, sl(zz, seqs), :].reshape(PLANE * seqs, ref.shape[2])

        weight = jnp.sum(jnp.where(which, tokens(wts), 0.0), axis=-1, keepdims=True)
        made = (jnp.dot(tokens(act.at[0]), down[0], preferred_element_type=f32)
                + jnp.dot(tokens(act.at[1]), down[1], preferred_element_type=f32)) * weight
        eout[zz] = made.astype(bf16).reshape(PLANE, seqs, made.shape[1])
        for i in (2, 0, 1):
            begin(eout.at[zz, i], back.at[zz, i], back_s, back_r + zz, plane[i], tp)
    far_s, far_r = group(fsum.at[pl.ds(0, outer - 1)]), take("r")
    for zz in out_order:
        summed = eout[zz, 3].astype(f32)
        arrived(back.at[zz], back_r + zz)
        for i in range(3):
            summed = summed + back[zz, i].astype(f32)
        if zz is not z:
            fsum[zz] = summed.astype(bf16)
            begin(fsum.at[zz], far.at[z], far_s, far_r, zdev(zz), tp)
    arrived(mixin.at[pl.ds(0, outer - 1)], mix_r)
    arrived(far.at[pl.ds(0, outer - 1)], far_r)
    for zz in zs:
        summed = summed + far[zz].astype(f32)
    for zc in range(outer):
        here = hid_ref[:, pl.ds(pl.multiple_of(zc * pf + tp * xq, xq), xq)].astype(f32) + mixin[zc].astype(f32)
        upd[tp, :, zc * xq:(zc + 1) * xq] = (here + summed[:, zc * xq:(zc + 1) * xq]).astype(bf16)
    u_s, u_r = group(upd.at[0]), take("r")
    begin(upd.at[tp], upd.at[tp], u_s, u_r, me, 1 - tp)
    arrived(upd.at[1 - tp], u_r)
    for t in range(2):
        for zc in range(outer):
            out_ref[:, zc * pf + t * xq:zc * pf + (t + 1) * xq] = upd[t, :, zc * xq:(zc + 1) * xq]
    for s, whole in groups:
        copy(whole, whole, s, 0, me, 1 - tp).wait_send()
    assert used["s"] == send.shape[0] and used["r"] == recv.shape[0] and used["l"] == local.shape[0], used


def step_kernel(hidden, attn_gain, query_weight, key_weight, value_weight, forget_weight, forget_bias,
                cache_keys, cache_values, cache_logsum, lengths, out_weight, ffn_gain, expert_ids, expert_scores,
                gate_weights, up_weights, down_weights):
    n = lax.axis_size("ep")
    seqs, width = hidden.shape
    cols = query_weight.shape[1]
    heads = cols // HD
    cache_len = cache_keys.shape[3]
    feats = out_weight.shape[0]
    units = gate_weights.shape[2]
    outer = n // PLANE
    line = outer * seqs
    xq = PLANE * feats // 2
    half = width // 2
    bf16, f32 = jnp.bfloat16, jnp.float32
    vmem = pl.BlockSpec(memory_space=pltpu.VMEM)
    hbm = pl.BlockSpec(memory_space=pltpu.HBM)
    v = pltpu.VMEM
    results = pl.pallas_call(
        functools.partial(step_body, n),
        out_shape=[v((seqs, width), bf16), v((seqs, HD), bf16), v((seqs, HD), bf16), v((seqs, heads), f32)],
        in_specs=[hbm] * 18,
        out_specs=[vmem] * 4,
        scratch_shapes=[
            pltpu.SMEM((seqs,), jnp.int32), pltpu.SMEM((heads,), f32), v((seqs, width), bf16), v((width,), bf16),
            v((width,), bf16), v((1, width), f32), v((TOP_K, seqs), jnp.int32), v((TOP_K, seqs), f32),
            v((width, cols), bf16), v((HD, width), bf16), v((HD, width), bf16), v((heads, width), bf16),
            v((seqs, HD, cache_len), bf16), v((seqs, HD, cache_len), bf16), v((seqs, heads, cache_len), f32),
            v((seqs * heads, cache_len), f32), v((seqs * heads, 128), f32), v((seqs * heads, 128), f32),
            v((seqs * heads, 128), f32), v((seqs * heads, 2 * HD), f32),
            v((line, cols), bf16), v((PLANE, feats, cols), bf16),
            v((2 * outer, xq, units), bf16), v((2 * outer, xq, units), bf16), v((2, units, half), bf16),
            v((line, xq), bf16), v((line, xq), f32), v((line, xq), f32), v((line, xq), bf16),
            v((outer, seqs, xq), bf16),
            v((2 * outer, PLANE, line, xq), bf16), v((outer, 8, line), f32), v((2, 8, line), f32),
            v((PLANE, 8, line), f32), v((PLANE, line, 128), f32),
            v((PLANE * line, units), f32), v((PLANE * line, units), f32), v((2, PLANE, line, units), bf16),
            v((outer, PLANE, seqs, half), bf16), v((outer, 3, seqs, half), bf16),
            v((outer, seqs, half), bf16), v((outer, seqs, half), bf16), v((2, seqs, half), bf16),
            pltpu.SemaphoreType.DMA((18,)), pltpu.SemaphoreType.DMA((17 + 4 * outer,)), pltpu.SemaphoreType.DMA((30,)),
        ],
        compiler_params=pltpu.CompilerParams(
            collective_id=0, has_side_effects=True, vmem_limit_bytes=40 * 1024 * 1024),
    )(*[pltpu.with_memory_space_constraint(a, pltpu.HBM) for a in (
        lengths, forget_bias, hidden, attn_gain, ffn_gain, expert_ids.T, expert_scores.T,
        query_weight, key_weight.T, value_weight.T, forget_weight.T, cache_keys, cache_values, cache_logsum,
        out_weight, gate_weights, up_weights, down_weights)])

    def hand_out(*refs):
        for i in range(4):
            refs[4 + i][...] = refs[i][...]

    updated, key_new, value_new, new_logsum = pl.pallas_call(
        hand_out,
        out_shape=[jax.ShapeDtypeStruct(r.shape, r.dtype) for r in results],
        in_specs=[vmem] * 4,
        out_specs=[vmem] * 4,
    )(*[pltpu.with_memory_space_constraint(r, pltpu.VMEM) for r in results])
    return updated, key_new.reshape(seqs, 1, HD), value_new.reshape(seqs, 1, HD), new_logsum


def per_device(hidden, attn_gain, query_weight, key_weight, value_weight, forget_weight, forget_bias,
               cache_keys, cache_values, cache_logsum, lengths, out_weight, ffn_gain, expert_ids, expert_scores,
               gate_weights, up_weights, down_weights):
    n = lax.axis_size("ep")
    seqs, width = hidden.shape
    fits = (
        n % PLANE == 0
        and lax.axis_size("tp") == 2
        and gate_weights.shape[0] == 1
        and cache_keys.shape[1] == 1
        and seqs % 16 == 0
        and (query_weight.shape[1] // HD) % 16 == 0
        and out_weight.shape[0] % 128 == 0
        and n <= 128
    )
    if fits:
        return step_kernel(
            hidden, attn_gain, query_weight, key_weight, value_weight, forget_weight, forget_bias,
            cache_keys, cache_values, cache_logsum, lengths, out_weight, ffn_gain, expert_ids, expert_scores,
            gate_weights, up_weights, down_weights)
    attended, key_new, value_new, new_logsum = attend(
        hidden, attn_gain, query_weight, key_weight, value_weight, forget_weight, forget_bias,
        cache_keys, cache_values, cache_logsum, lengths)
    updated = rest_general(attended, hidden, out_weight, ffn_gain, expert_ids, expert_scores,
                           gate_weights, up_weights, down_weights)
    return (updated, key_new, value_new, new_logsum)


def solution(mesh):
    in_specs = (
        P("ep", None),
        P(),
        P(None, "tp"),
        P(None, "tp"),
        P(None, "tp"),
        P(None, "tp"),
        P("tp"),
        P("ep", "tp", None, None),
        P("ep", "tp", None, None),
        P("ep", "tp", None),
        P("ep"),
        P("ep", None),
        P(),
        P("ep", None),
        P("ep", None),
        P("ep", None, "tp"),
        P("ep", None, "tp"),
        P("ep", "tp", None),
    )
    out_specs = (P("ep", None), P("ep", "tp", None), P("ep", "tp", None), P("ep", "tp"))
    return jax.shard_map(
        per_device, mesh=mesh, in_specs=in_specs, out_specs=out_specs, check_vma=False
    )
```

```python
import functools
import math

import jax
import jax.numpy as jnp
from jax import lax
from jax.experimental import pallas as pl
from jax.experimental.pallas import tpu as pltpu
from jax.sharding import PartitionSpec as P

HD = 64
TOP_K = 6


epsilon = 1e-06


def root_norm(values_in, gain):
    floats = values_in.astype(jnp.float32)
    inv_root = lax.rsqrt(jnp.mean(floats * floats, axis=-1, keepdims=True) + epsilon)
    return floats * inv_root * gain.astype(jnp.float32)


def attend(hidden, attn_gain, query_weight, key_weight, value_weight, forget_weight, forget_bias,
           cache_keys, cache_values, cache_logsum, lengths):
    rows_here = hidden.shape[0]
    query_heads = query_weight.shape[1] // HD
    key_heads = key_weight.shape[1] // HD
    group_size = query_heads // key_heads
    cache_len = cache_keys.shape[-1]
    score_scale = HD ** (-0.5)
    normed = root_norm(hidden, attn_gain).astype(jnp.bfloat16)
    queries = jnp.dot(normed, query_weight, preferred_element_type=jnp.float32).astype(jnp.bfloat16)
    key_new = (
        jnp.dot(normed, key_weight, preferred_element_type=jnp.float32)
        .astype(jnp.bfloat16)
        .reshape(rows_here, key_heads, HD)
    )
    value_new = (
        jnp.dot(normed, value_weight, preferred_element_type=jnp.float32)
        .astype(jnp.bfloat16)
        .reshape(rows_here, key_heads, HD)
    )
    log_forget = jax.nn.log_sigmoid(
        jnp.dot(normed, forget_weight, preferred_element_type=jnp.float32) + forget_bias
    )
    positions = jnp.arange(cache_len, dtype=jnp.int32)
    is_last = positions[None, :] == (lengths - 1)[:, None]
    new_logsum = jnp.sum(jnp.where(is_last[:, None, :], cache_logsum, 0.0), axis=-1) + log_forget
    grouped = queries.reshape(rows_here, key_heads, group_size, HD)
    scores = jnp.einsum("sgjd,sgdp->sgjp", grouped, cache_keys, preferred_element_type=jnp.float32)
    scores = scores.reshape(rows_here, query_heads, cache_len) * score_scale
    scores = scores + new_logsum[:, :, None] - cache_logsum
    is_live = positions[None, :] < lengths[:, None]
    scores = jnp.where(is_live[:, None, :], scores, -jnp.inf)
    own_score = (
        jnp.einsum("sgjd,sgd->sgj", grouped, key_new, preferred_element_type=jnp.float32).reshape(
            rows_here, query_heads
        )
        * score_scale
    )
    top_score = jnp.maximum(jnp.max(scores, axis=-1), own_score)
    past_exp = jnp.exp(scores - top_score[:, :, None])
    own_exp = jnp.exp(own_score - top_score)
    denominator = jnp.sum(past_exp, axis=-1) + own_exp
    past_weight = (past_exp / denominator[:, :, None]).astype(jnp.bfloat16)
    own_weight = (own_exp / denominator).astype(jnp.bfloat16)
    attended = jnp.einsum(
        "sgjp,sgdp->sgjd",
        past_weight.reshape(rows_here, key_heads, group_size, cache_len),
        cache_values,
        preferred_element_type=jnp.float32,
    )
    attended = (
        attended
        + own_weight.astype(jnp.float32).reshape(rows_here, key_heads, group_size)[:, :, :, None]
        * value_new.astype(jnp.float32)[:, :, None, :]
    )
    attended = attended.reshape(rows_here, query_heads * HD).astype(jnp.bfloat16)
    return attended, key_new, value_new, new_logsum


def rest_general(attended, hidden, out_weight, ffn_gain, expert_ids, expert_scores,
                 gate_weights, up_weights, down_weights):
    rows_here = hidden.shape[0]
    whole_heads = lax.all_gather(attended, "tp", axis=1, tiled=True)
    projected = lax.dot_general(
        lax.all_gather(whole_heads, "ep", axis=0, tiled=True),
        out_weight,
        (((1,), (1,)), ((), ())),
        preferred_element_type=jnp.float32,
    ).astype(jnp.bfloat16)
    mixed = lax.all_to_all(projected, "ep", split_axis=0, concat_axis=1, tiled=True)
    residual = hidden.astype(jnp.float32) + mixed.astype(jnp.float32)
    ffn_in = root_norm(residual, ffn_gain).astype(jnp.bfloat16)
    ep_size = lax.axis_size("ep")
    local_experts = gate_weights.shape[0]
    experts = ep_size * local_experts
    route_count = rows_here * TOP_K
    capacity = 2 * ((route_count + experts - 1) // experts)
    flat_ids = expert_ids.reshape(route_count)
    onehot = (flat_ids[:, None] == jnp.arange(experts, dtype=jnp.int32)[None, :]).astype(jnp.int32)
    running = jnp.cumsum(onehot, axis=0)
    slot_index = jnp.sum(running * onehot, axis=1) - 1
    target = flat_ids * capacity + slot_index
    dispatch_map = (
        target[:, None] == jnp.arange(experts * capacity, dtype=jnp.int32)[None, :]
    ).astype(jnp.bfloat16)
    route_rows = jnp.repeat(ffn_in, TOP_K, axis=0)
    outgoing = lax.dot_general(
        dispatch_map, route_rows, (((0,), (0,)), ((), ())), preferred_element_type=jnp.float32
    )
    outgoing = outgoing.astype(jnp.bfloat16).reshape(
        ep_size, local_experts, capacity, ffn_in.shape[1]
    )
    arrived = lax.all_to_all(outgoing, "ep", split_axis=0, concat_axis=0, tiled=True)
    gate_act = jnp.einsum(
        "sekd,edf->sekf", arrived, gate_weights, preferred_element_type=jnp.float32
    )
    up_act = jnp.einsum("sekd,edf->sekf", arrived, up_weights, preferred_element_type=jnp.float32)
    hidden_act = (jax.nn.silu(gate_act) * up_act).astype(jnp.bfloat16)
    partial_out = jnp.einsum(
        "sekf,efd->sekd", hidden_act, down_weights, preferred_element_type=jnp.float32
    )
    half_sum = lax.psum_scatter(
        partial_out.astype(jnp.bfloat16), "tp", scatter_dimension=3, tiled=True
    )
    sent_back = lax.all_to_all(half_sum, "ep", split_axis=0, concat_axis=0, tiled=True)
    share_width = sent_back.shape[-1]
    picked = jnp.dot(
        dispatch_map,
        sent_back.reshape(experts * capacity, share_width),
        preferred_element_type=jnp.float32,
    )
    route_weight = expert_scores / jnp.sum(expert_scores, axis=-1, keepdims=True)
    expert_mix = jnp.sum(
        picked.reshape(rows_here, TOP_K, share_width) * route_weight[:, :, None], axis=1
    )
    own_part = lax.dynamic_slice_in_dim(
        residual, lax.axis_index("tp") * share_width, share_width, 1
    )
    updated = lax.all_gather((own_part + expert_mix).astype(jnp.bfloat16), "tp", axis=1, tiled=True)
    return updated


MESH = pl.DeviceIdType.MESH
PLANE = 4


def step_body(n, len_hbm, fbias_hbm, hid_hbm, again_hbm, fgain_hbm, ids_hbm, rscore_hbm,
              qw_hbm, kw_hbm, vw_hbm, fw_hbm, keys_hbm, vals_hbm, logs_hbm, ow_hbm, gate_hbm, up_hbm, down_hbm,
              out_ref, key_ref, val_ref, nlog_ref,
              len_ref, fbias_ref, hid_ref, again, fgain, fgain_row, ids_ref, rscore_ref, qw, kw, vw, fw, keys, vals, logs, scores, maxes, lasts, sums, mixed_heads, att, ow, gate, up, down,
              hidl, part, pin, mixl, mixin, rows, ssq, ssqp, scales, wts, act, eout, back, fsum, far, upd,
              send, recv, local):
    f32, bf16 = jnp.float32, jnp.bfloat16
    me, tp = lax.axis_index("ep"), lax.axis_index("tp")
    seqs, width = hid_ref.shape
    cols = qw.shape[1]
    heads = cols // HD
    cache_len = keys.shape[2]
    outer = n // PLANE
    feats = ow.shape[1]
    pf = PLANE * feats
    xq = pf // 2
    line = outer * seqs
    z, xy = me // PLANE, lax.rem(me, PLANE)
    x, y = lax.rem(xy, 2), xy // 2
    spots = [y * 2 + (1 - x), (1 - y) * 2 + x, (1 - y) * 2 + (1 - x)]
    plane = [z * PLANE + s for s in spots]

    def zdev(zz):
        return zz * PLANE + xy

    near_tables = [sorted([j for j in range(outer) if j != i], key=lambda j: (abs(j - i), j)) for i in range(outer)]
    far_tables = [sorted(range(outer), key=lambda j: (-abs(j - i), j)) for i in range(outer)]

    def pick(tables, k, zz):
        value = tables[0][k]
        for i in range(1, outer):
            value = jnp.where(zz == i, tables[i][k], value)
        return value

    zs = [pick(near_tables, k, z) for k in range(outer - 1)]
    dests = [pick(far_tables, k, z) for k in range(outer - 1)] + [z]

    def rows_of(g, zz):
        return sl(zz if g == outer - 1 else pick(far_tables, g, zz), seqs)

    used = {"s": 0, "r": 0, "l": 0}

    def take(kind, count=1):
        base = used[kind]
        used[kind] += count
        return base

    def copy(src, dst, s, r, ep, core):
        return pltpu.make_async_remote_copy(src_ref=src, dst_ref=dst, send_sem=send.at[s], recv_sem=recv.at[r],
                                            device_id=(ep, core), device_id_type=MESH)

    wholes = [0, 0]

    def group(whole):
        size = math.prod(whole.shape) * whole.dtype.itemsize
        kind = 0 if size % (32 * cols) == 0 else 1
        wholes[kind] += size
        return kind

    def begin(src, dst, s, r, ep, core):
        copy(src, dst, s, r, ep, core).start()

    def arrived(dst, r):
        copy(dst, dst, 0, r, me, 1 - tp).wait_recv()

    def load(src, dst, l=None):
        c = pltpu.make_async_copy(src, dst, local.at[take("l") if l is None else l])
        c.start()
        return c

    def sl(i, size):
        return pl.ds(pl.multiple_of(i * size, size), size)

    barrier = pltpu.get_barrier_semaphore()
    for d in range(1, outer):
        pl.semaphore_signal(barrier, inc=1, device_id=(zdev(lax.rem(z + d, outer)), tp), device_id_type=MESH)
    for p in plane:
        pl.semaphore_signal(barrier, inc=1, device_id=(p, tp), device_id_type=MESH)
    pl.semaphore_signal(barrier, inc=1, device_id=(me, 1 - tp), device_id_type=MESH)

    ow_load = load(ow_hbm.at[:, sl(tp, cols)], ow.at[xy])
    first = [load(hid_hbm, hid_ref), load(again_hbm, again), load(ids_hbm, ids_ref), load(rscore_hbm, rscore_ref)]
    scalars = [load(fbias_hbm, fbias_ref), load(len_hbm, len_ref), load(fgain_hbm, fgain)]
    small = [load(kw_hbm, kw), load(vw_hbm, vw), load(fw_hbm, fw)]
    qchunk = width // 4
    qw_loads = [load(qw_hbm.at[pl.ds(i * qchunk, qchunk)], qw.at[pl.ds(i * qchunk, qchunk)]) for i in range(4)]
    batch = seqs // 2
    key_loads = [load(keys_hbm.at[pl.ds(i * batch, batch), 0], keys.at[pl.ds(i * batch, batch)]) for i in range(2)]
    log_loads = [load(logs_hbm.at[pl.ds(i * batch, batch)], logs.at[pl.ds(i * batch, batch)]) for i in range(2)]
    val_loads = [load(vals_hbm.at[pl.ds(i * batch, batch), 0], vals.at[pl.ds(i * batch, batch)]) for i in range(2)]

    pl.semaphore_wait(barrier, outer - 1 + 3 + 1)

    hf = feats // 2
    lo, hi = pl.ds(0, hf), pl.ds(hf, hf)
    ow_load.wait()
    ow_s, ow_r = group(ow.at[pl.ds(0, 3)]), take("r", 3)
    begin(ow.at[xy, lo], ow.at[xy, lo], ow_s, ow_r, plane[0], tp)
    begin(ow.at[xy, hi], ow.at[xy, hi], ow_s, ow_r + 1, plane[1], tp)
    begin(ow.at[xy, hi], ow.at[xy, hi], ow_s, ow_r + 2, plane[0], tp)
    begin(ow.at[xy, lo], ow.at[xy, lo], ow_s, ow_r + 2, plane[1], tp)

    for c in first:
        c.wait()
    normed = root_norm(hid_ref[...], again[...][None, :]).astype(bf16)
    rscore = rscore_ref[...]
    route = rscore / jnp.sum(rscore, axis=0, keepdims=True)
    ids = ids_ref[...].astype(f32)
    lanes = lax.broadcasted_iota(jnp.int32, (seqs, 128), 1).astype(f32)
    small_eye = (lax.broadcasted_iota(jnp.int32, (seqs, seqs), 0) == lax.broadcasted_iota(jnp.int32, (seqs, seqs), 1))

    def column(row):
        return jnp.sum(jnp.where(small_eye, jnp.broadcast_to(row, (seqs, seqs)), 0.0), axis=1, keepdims=True)

    table = jnp.zeros((seqs, 128), f32)
    for k in range(TOP_K):
        table = table + jnp.where(lanes == column(ids[k:k + 1, :]), column(route[k:k + 1, :]), 0.0)
    wts[3, sl(z, seqs), :] = table

    others = pl.ds(0, (outer - 1) * seqs)
    hid_s, hid_r = group(hidl.at[others]), take("r")
    for zz in zs:
        begin(hid_ref.at[:, pl.ds(pl.multiple_of(zz * pf + tp * xq, xq), xq)], hidl.at[sl(z, seqs)],
              hid_s, hid_r, zdev(zz), tp)
    hidl[sl(z, seqs), :] = hid_ref[:, pl.ds(pl.multiple_of(z * pf + tp * xq, xq), xq)]
    wt_s, wt_r = group(wts.at[0, others]), take("r")
    for zz in zs:
        begin(wts.at[3, sl(z, seqs)], wts.at[3, sl(z, seqs)], wt_s, wt_r, zdev(zz), tp)

    acc = jnp.zeros((seqs, cols), f32)
    for i in range(4):
        qw_loads[i].wait()
        acc = acc + jnp.dot(normed[:, i * qchunk:(i + 1) * qchunk], qw[pl.ds(i * qchunk, qchunk), :],
                            preferred_element_type=f32)
    queries = acc.astype(bf16).astype(f32) * (HD ** -0.5)
    for c in small:
        c.wait()
    for c in scalars:
        c.wait()
    fgain_row[...] = fgain[...].astype(f32)[None, :]

    def new_token(w):
        return lax.dot_general(normed, w[...], (((1,), (1,)), ((), ())), preferred_element_type=f32)

    key_new = new_token(kw).astype(bf16)
    value_new = new_token(vw).astype(bf16)
    key_ref[...] = key_new
    val_ref[...] = value_new
    hl = lax.broadcasted_iota(jnp.int32, (seqs, heads), 1)
    fb = jnp.zeros((seqs, heads), f32)
    for h in range(heads):
        fb = jnp.where(hl == h, fbias_ref[h], fb)
    pre = new_token(fw) + fb
    log_forget = jnp.minimum(pre, 0.0) - jnp.log1p(jnp.exp(-jnp.abs(pre)))

    gate_l, up_l, down_l = take("l"), take("l"), take("l")
    for t in range(2):
        for zc in range(outer):
            rows_from = pl.ds(zc * pf + t * xq, xq)
            load(gate_hbm.at[0, rows_from], gate.at[t * outer + zc], gate_l)
            load(up_hbm.at[0, rows_from], up.at[t * outer + zc], up_l)
    down_s, down_r = group(down.at[0]), take("r")
    for zc in range(outer):
        mine = pl.ds(pl.multiple_of(zc * pf + tp * xq, xq), xq)
        other = pl.ds(pl.multiple_of(zc * pf + (1 - tp) * xq, xq), xq)
        load(down_hbm.at[0, :, mine], down.at[tp, :, pl.ds(zc * xq, xq)], down_l)
        begin(down_hbm.at[0, :, other], down.at[tp, :, pl.ds(zc * xq, xq)], down_s, down_r, me, 1 - tp)

    total = seqs * heads

    def spread(v):
        return jnp.broadcast_to(v[:, None, :], (seqs, heads, v.shape[1])).reshape(total, v.shape[1])

    row_head = lax.rem(lax.broadcasted_iota(jnp.int32, (total, 128), 0), heads)
    picked = jnp.zeros((total, 128), f32)
    for j in range(cols // 128):
        picked = jnp.where(row_head // 2 == j, spread(queries[:, j * 128:(j + 1) * 128]), picked)
    picked = jnp.where(lax.rem(row_head, 2) == 0, picked, pltpu.roll(picked, HD, 1))[:, :HD]
    per_head = picked.astype(bf16)
    own = jnp.sum(picked * spread(key_new.astype(f32)), axis=-1, keepdims=True)

    positions = lax.broadcasted_iota(jnp.int32, (heads, cache_len), 1)
    for s in range(seqs):
        if s % batch == 0:
            key_loads[s // batch].wait()
            log_loads[s // batch].wait()
        here = pl.ds(s * heads, heads)
        size = len_ref[s]
        level = logs[s]
        dots = jnp.dot(per_head[s * heads:(s + 1) * heads, :], keys[s], preferred_element_type=f32)
        past = jnp.where(positions < size, dots - level, -jnp.inf)
        scores[here, :] = past
        maxes[here, :] = jnp.broadcast_to(jnp.max(past, axis=-1, keepdims=True), (heads, 128))
        last = jnp.sum(jnp.where(positions == size - 1, level, 0.0), axis=-1, keepdims=True)
        lasts[here, :] = jnp.broadcast_to(last, (heads, 128))
    own_lane = lax.broadcasted_iota(jnp.int32, (total, heads), 1)
    own_row = lax.rem(lax.broadcasted_iota(jnp.int32, (total, heads), 0), heads)
    forget_col = jnp.sum(jnp.where(own_lane == own_row, spread(log_forget), 0.0), axis=-1, keepdims=True)
    newlog = lasts[:, :1] + forget_col
    nlog_ref[...] = jnp.sum(jnp.where(own_lane == own_row, jnp.broadcast_to(newlog, (total, heads)), 0.0)
                            .reshape(seqs, heads, heads), axis=1)
    own = own - newlog
    peak = jnp.maximum(maxes[:, :1], own)
    maxes[...] = jnp.broadcast_to(peak, (total, 128))
    for s in range(seqs):
        if s % batch == 0:
            val_loads[s // batch].wait()
        here = pl.ds(s * heads, heads)
        weights = jnp.exp(scores[here, :] - maxes[here, :][:, :1])
        sums[here, :] = jnp.broadcast_to(jnp.sum(weights, axis=-1, keepdims=True), (heads, 128))
        mixed_heads[here, :HD] = lax.dot_general(weights.astype(bf16), vals[s], (((1,), (1,)), ((), ())),
                                                 preferred_element_type=f32)
    own_exp = jnp.exp(own - peak)
    inverse = 1.0 / (sums[:, :1] + own_exp)
    outs = (mixed_heads[:, :HD] + own_exp * spread(value_new.astype(f32))) * inverse
    mixed_heads[:, :HD] = outs
    mixed_heads[:, HD:] = outs
    wide = lax.broadcasted_iota(jnp.int32, (seqs, 128), 1)
    for j in range(cols // 128):
        even = mixed_heads[pl.ds(2 * j, seqs, stride=heads), :]
        odd = mixed_heads[pl.ds(2 * j + 1, seqs, stride=heads), :]
        att[sl(z, seqs), j * 128:(j + 1) * 128] = jnp.where(wide < HD, even, odd).astype(bf16)

    att_s, att_r = group(att.at[others]), take("r")
    for zz in reversed(zs):
        begin(att.at[sl(z, seqs)], att.at[sl(z, seqs)], att_s, att_r, zdev(zz), tp)
    arrived(ow.at[spots[0], lo], ow_r)
    relay_r = take("r")
    begin(ow.at[spots[0], lo], ow.at[spots[0], lo], ow_s, relay_r, plane[1], tp)
    arrived(ow.at[spots[1], hi], ow_r + 1)
    begin(ow.at[spots[1], hi], ow.at[spots[1], hi], ow_s, relay_r, plane[0], tp)
    arrived(wts.at[0, others], wt_r)
    wline_s, wline_r = group(wts.at[pl.ds(0, 3)]), take("r")
    for i in range(3):
        begin(wts.at[3], wts.at[i], wline_s, wline_r, plane[i], tp)
    arrived(ow.at[0], ow_r + 2)
    arrived(hidl.at[others], hid_r)
    arrived(att.at[others], att_r)
    lines = att[...]

    def project(i):
        part[i] = lax.dot_general(lines, ow[i], (((1,), (1,)), ((), ())), preferred_element_type=f32)

    for i in [xy] + spots[:2]:
        project(i)
    arrived(ow.at[spots[2]], relay_r)
    project(spots[2])
    p_s, p_r = group(pin), take("r")
    begin(part.at[pl.ds(2 * (1 - tp), 2)], pin, p_s, p_r, me, 1 - tp)
    arrived(pin, p_r)
    mixed = jnp.concatenate([part[2 * tp + i] + pin[i] for i in range(2)], axis=1).astype(bf16)
    residual = hidl[...].astype(f32) + mixed.astype(f32)
    gain = fgain_row[:, pl.ds(pl.multiple_of(z * pf + tp * xq, xq), xq)]
    block = tp * outer + z
    rows[block, 3] = (residual * gain).astype(bf16)
    square = jnp.sum(residual * residual, axis=-1, keepdims=True)
    eye = (lax.broadcasted_iota(jnp.int32, (line, line), 0) == lax.broadcasted_iota(jnp.int32, (line, line), 1))
    flat = jnp.sum(jnp.where(eye, jnp.broadcast_to(square, (line, line)), 0.0), axis=0, keepdims=True)
    ssq[z, 3] = jnp.broadcast_to(flat, (8, line))
    mixl[...] = mixed

    zrow_s, zrow_r = group(rows.at[0, pl.ds(0, outer - 1)]), take("r", outer * outer)
    prow_s, prow_r = group(rows.at[pl.ds(0, 3)]), take("r", outer)
    crow_s, crow_r = group(rows.at[pl.ds(0, outer)]), take("r", outer)
    zsq_s, zsq_r = 2, take("r")
    psq_s, psq_r = 3, take("r")
    csq_s, csq_r = 3, take("r")
    mix_s, mix_r = group(mixl.at[others]), take("r")

    def out_to_plane(g, zz):
        b, some = tp * outer + zz, rows_of(g, z)
        for i in (2, 0, 1):
            begin(rows.at[b, 3, some], rows.at[b, i, some], prow_s, prow_r + g, plane[i], tp)

    for g in range(outer):
        for zz in reversed(zs):
            some = rows_of(g, zz)
            begin(rows.at[block, 3, some], rows.at[block, 3, some], zrow_s, zrow_r + g * outer + z, zdev(zz), tp)
        if g == 0:
            for zz in reversed(zs):
                begin(ssq.at[z, 3], ssq.at[z, 3], zsq_s, zsq_r, zdev(zz), tp)
        out_to_plane(g, z)
    mixin[z] = mixl[sl(z, seqs), :]
    for g in range(outer):
        for zz in zs:
            arrived(rows.at[tp * outer + zz, 3, rows_of(g, z)], zrow_r + g * outer + zz)
            out_to_plane(g, zz)
        if g == 0:
            arrived(ssq.at[0, pl.ds(0, outer - 1)], zsq_r)
            for i in range(3):
                begin(ssq.at[:, 3], ssq.at[:, i], psq_s, psq_r, plane[i], tp)
    for zz in zs:
        begin(mixl.at[sl(zz, seqs)], mixin.at[z], mix_s, mix_r, zdev(zz), tp)
    pltpu.make_async_copy(gate, gate, local.at[gate_l]).wait()
    pltpu.make_async_copy(up, up, local.at[up_l]).wait()
    pltpu.make_async_copy(down.at[0], down.at[0], local.at[down_l]).wait()
    arrived(wts.at[pl.ds(0, 3)], wline_r)

    parts = [[g] for g in range(outer // 2)] + [list(range(outer // 2, outer))]

    def product(part_groups, t):
        left = jnp.concatenate([
            jnp.concatenate([rows[t * outer + i, :, rows_of(g, z), :].reshape(PLANE * seqs, xq) for g in part_groups],
                            axis=0) for i in range(outer)], axis=1)
        span = pl.ds(t * outer, outer)
        return [jnp.dot(left, w[span].reshape(outer * xq, w.shape[2]), preferred_element_type=f32) for w in (gate, up)]

    def pass_on(part_groups):
        for g in part_groups:
            span, some = pl.ds(tp * outer, outer), rows_of(g, z)
            arrived(rows.at[span, pl.ds(0, 3), some], prow_r + g)
            block_rows = rows.at[span, :, some]
            begin(block_rows, block_rows, crow_s, crow_r + g, me, 1 - tp)

    def collect(part_groups, early):
        for g in part_groups:
            arrived(rows.at[pl.ds((1 - tp) * outer, outer), :, rows_of(g, z)], crow_r + g)
        late = product(part_groups, 1 - tp)
        return early[0] + late[0], early[1] + late[1]

    act_s, act_r = group(act.at[0]), take("r", outer)

    def span_of(part_groups):
        return pl.ds(part_groups[0], len(part_groups))

    def activate(part_groups, a, u):
        scale = jnp.concatenate([scales[:, rows_of(g, z), :].reshape(PLANE * seqs, 128)[:, :1] for g in part_groups],
                                axis=0)
        a, u = a * scale, u * scale
        made = (a / (1.0 + jnp.exp(-a)) * u).astype(bf16)
        here = act.at[tp, span_of(part_groups)]
        here[...] = made.reshape(len(part_groups), PLANE * seqs, made.shape[1])
        begin(here, here, act_s, act_r + part_groups[0], me, 1 - tp)

    back_s, back_r = group(eout.at[pl.ds(0, 3)]), take("r", outer)
    which = lax.broadcasted_iota(jnp.int32, (PLANE * seqs, 128), 1) == me

    def give(part_groups):
        span = span_of(part_groups)
        arrived(act.at[1 - tp, span], act_r + part_groups[0])
        lefts = [act[t, span].reshape(len(part_groups) * PLANE * seqs, act.shape[3]) for t in range(2)]
        made = (jnp.dot(lefts[0], down[0], preferred_element_type=f32)
                + jnp.dot(lefts[1], down[1], preferred_element_type=f32))
        for j, g in enumerate(part_groups):
            zz = dests[g]
            wt = wts[:, sl(zz, seqs), :].reshape(PLANE * seqs, 128)
            weight = jnp.sum(jnp.where(which, wt, 0.0), axis=-1, keepdims=True)
            scaled = made[j * PLANE * seqs:(j + 1) * PLANE * seqs] * weight
            eout[zz] = scaled.astype(bf16).reshape(PLANE, seqs, made.shape[1])
            for i in (2, 0, 1):
                begin(eout.at[zz, i], back.at[zz, i], back_s, back_r + zz, plane[i], tp)

    arrived(ssq.at[:, pl.ds(0, 3)], psq_r)
    squares = ssq[0]
    for i in range(1, outer):
        squares = squares + ssq[i]
    ssqp[tp] = squares
    begin(ssqp.at[tp], ssqp.at[tp], csq_s, csq_r, me, 1 - tp)
    pass_on(parts[0])
    early = product(parts[0], tp)
    pass_on(parts[1])
    a, u = collect(parts[0], early)
    arrived(ssqp.at[1 - tp], csq_r)
    squares = ssqp[0] + ssqp[1]
    for q in range(PLANE):
        scale = lax.rsqrt(squares[q, :1, :] * (1.0 / width) + epsilon)
        scale = jnp.sum(jnp.where(eye, jnp.broadcast_to(scale, (line, line)), 0.0), axis=1, keepdims=True)
        scales[q] = jnp.broadcast_to(scale, (line, 128))
    activate(parts[0], a, u)
    arrived(down.at[1 - tp], down_r)
    for k in range(1, len(parts)):
        early = product(parts[k], tp)
        if k + 1 < len(parts):
            pass_on(parts[k + 1])
        a, u = collect(parts[k], early)
        activate(parts[k], a, u)
        give(parts[k - 1])
    give(parts[-1])
    far_s, far_r = group(fsum.at[pl.ds(0, outer - 1)]), take("r")
    for zz in dests:
        summed = eout[zz, 3].astype(f32)
        arrived(back.at[zz], back_r + zz)
        for i in range(3):
            summed = summed + back[zz, i].astype(f32)
        if zz is not z:
            fsum[zz] = summed.astype(bf16)
            begin(fsum.at[zz], far.at[z], far_s, far_r, zdev(zz), tp)
    arrived(mixin.at[pl.ds(0, outer - 1)], mix_r)
    arrived(far.at[pl.ds(0, outer - 1)], far_r)
    for zz in zs:
        summed = summed + far[zz].astype(f32)
    for zc in range(outer):
        here = hid_ref[:, pl.ds(pl.multiple_of(zc * pf + tp * xq, xq), xq)].astype(f32) + mixin[zc].astype(f32)
        upd[tp, :, zc * xq:(zc + 1) * xq] = (here + summed[:, zc * xq:(zc + 1) * xq]).astype(bf16)
    u_s, u_r = group(upd.at[0]), take("r")
    begin(upd.at[tp], upd.at[tp], u_s, u_r, me, 1 - tp)
    arrived(upd.at[1 - tp], u_r)
    for t in range(2):
        for zc in range(outer):
            out_ref[:, zc * pf + t * xq:zc * pf + (t + 1) * xq] = upd[t, :, zc * xq:(zc + 1) * xq]
    assert wholes[0] % (32 * cols) == 0 and wholes[1] % 4096 == 0, wholes
    for s, whole in enumerate((qw.at[pl.ds(0, wholes[0] // (2 * cols))], maxes.at[pl.ds(0, wholes[1] // 512)],
                               ssq.at[0, pl.ds(0, outer - 1)], ssq)):
        copy(whole, whole, s, 0, me, 1 - tp).wait_send()
    assert used["r"] == recv.shape[0] and used["l"] == local.shape[0], used


def step_kernel(hidden, attn_gain, query_weight, key_weight, value_weight, forget_weight, forget_bias,
                cache_keys, cache_values, cache_logsum, lengths, out_weight, ffn_gain, expert_ids, expert_scores,
                gate_weights, up_weights, down_weights):
    n = lax.axis_size("ep")
    seqs, width = hidden.shape
    cols = query_weight.shape[1]
    heads = cols // HD
    cache_len = cache_keys.shape[3]
    feats = out_weight.shape[0]
    units = gate_weights.shape[2]
    outer = n // PLANE
    line = outer * seqs
    xq = PLANE * feats // 2
    half = width // 2
    bf16, f32 = jnp.bfloat16, jnp.float32
    vmem = pl.BlockSpec(memory_space=pltpu.VMEM)
    hbm = pl.BlockSpec(memory_space=pltpu.HBM)
    v = pltpu.VMEM
    results = pl.pallas_call(
        functools.partial(step_body, n),
        out_shape=[v((seqs, width), bf16), v((seqs, HD), bf16), v((seqs, HD), bf16), v((seqs, heads), f32)],
        in_specs=[hbm] * 18,
        out_specs=[vmem] * 4,
        scratch_shapes=[
            pltpu.SMEM((seqs,), jnp.int32), pltpu.SMEM((heads,), f32), v((seqs, width), bf16), v((width,), bf16),
            v((width,), bf16), v((1, width), f32), v((TOP_K, seqs), jnp.int32), v((TOP_K, seqs), f32),
            v((width, cols), bf16), v((HD, width), bf16), v((HD, width), bf16), v((heads, width), bf16),
            v((seqs, HD, cache_len), bf16), v((seqs, HD, cache_len), bf16), v((seqs, heads, cache_len), f32),
            v((seqs * heads, cache_len), f32), v((seqs * heads, 128), f32), v((seqs * heads, 128), f32),
            v((seqs * heads, 128), f32), v((seqs * heads, 2 * HD), f32),
            v((line, cols), bf16), v((PLANE, feats, cols), bf16),
            v((2 * outer, xq, units), bf16), v((2 * outer, xq, units), bf16), v((2, units, half), bf16),
            v((line, xq), bf16), v((PLANE, line, feats), f32), v((2, line, feats), f32), v((line, xq), bf16),
            v((outer, seqs, xq), bf16),
            v((2 * outer, PLANE, line, xq), bf16), v((outer, PLANE, 8, line), f32), v((2, PLANE, 8, line), f32),
            v((PLANE, line, 128), f32), v((PLANE, line, 128), f32),
                        v((2, outer, PLANE * seqs, units), bf16),
            v((outer, PLANE, seqs, half), bf16), v((outer, 3, seqs, half), bf16),
            v((outer, seqs, half), bf16), v((outer, seqs, half), bf16), v((2, seqs, half), bf16),
            pltpu.SemaphoreType.DMA((4,)), pltpu.SemaphoreType.DMA((16 + 4 * outer + outer * outer,)), pltpu.SemaphoreType.DMA((24,)),
        ],
        compiler_params=pltpu.CompilerParams(
            collective_id=0, has_side_effects=True, vmem_limit_bytes=40 * 1024 * 1024),
    )(*[pltpu.with_memory_space_constraint(a, pltpu.HBM) for a in (
        lengths, forget_bias, hidden, attn_gain, ffn_gain, expert_ids.T, expert_scores.T,
        query_weight, key_weight.T, value_weight.T, forget_weight.T, cache_keys, cache_values, cache_logsum,
        out_weight, gate_weights, up_weights, down_weights)])

    def hand_out(*refs):
        for i in range(4):
            refs[4 + i][...] = refs[i][...]

    updated, key_new, value_new, new_logsum = pl.pallas_call(
        hand_out,
        out_shape=[jax.ShapeDtypeStruct(r.shape, r.dtype) for r in results],
        in_specs=[vmem] * 4,
        out_specs=[vmem] * 4,
    )(*[pltpu.with_memory_space_constraint(r, pltpu.VMEM) for r in results])
    return updated, key_new.reshape(seqs, 1, HD), value_new.reshape(seqs, 1, HD), new_logsum


def per_device(hidden, attn_gain, query_weight, key_weight, value_weight, forget_weight, forget_bias,
               cache_keys, cache_values, cache_logsum, lengths, out_weight, ffn_gain, expert_ids, expert_scores,
               gate_weights, up_weights, down_weights):
    n = lax.axis_size("ep")
    seqs, width = hidden.shape
    fits = (
        n % (2 * PLANE) == 0
        and lax.axis_size("tp") == 2
        and gate_weights.shape[0] == 1
        and cache_keys.shape[1] == 1
        and seqs % 16 == 0
        and (query_weight.shape[1] // HD) % 16 == 0
        and out_weight.shape[0] % 128 == 0
        and n <= 128
    )
    if fits:
        return step_kernel(
            hidden, attn_gain, query_weight, key_weight, value_weight, forget_weight, forget_bias,
            cache_keys, cache_values, cache_logsum, lengths, out_weight, ffn_gain, expert_ids, expert_scores,
            gate_weights, up_weights, down_weights)
    attended, key_new, value_new, new_logsum = attend(
        hidden, attn_gain, query_weight, key_weight, value_weight, forget_weight, forget_bias,
        cache_keys, cache_values, cache_logsum, lengths)
    updated = rest_general(attended, hidden, out_weight, ffn_gain, expert_ids, expert_scores,
                           gate_weights, up_weights, down_weights)
    return (updated, key_new, value_new, new_logsum)


def solution(mesh):
    in_specs = (
        P("ep", None),
        P(),
        P(None, "tp"),
        P(None, "tp"),
        P(None, "tp"),
        P(None, "tp"),
        P("tp"),
        P("ep", "tp", None, None),
        P("ep", "tp", None, None),
        P("ep", "tp", None),
        P("ep"),
        P("ep", None),
        P(),
        P("ep", None),
        P("ep", None),
        P("ep", None, "tp"),
        P("ep", None, "tp"),
        P("ep", "tp", None),
    )
    out_specs = (P("ep", None), P("ep", "tp", None), P("ep", "tp", None), P("ep", "tp"))
    return jax.shard_map(
        per_device, mesh=mesh, in_specs=in_specs, out_specs=out_specs, check_vma=False
    )
```

```python
import functools
import math

import jax
import jax.numpy as jnp
from jax import lax
from jax.experimental import pallas as pl
from jax.experimental.pallas import tpu as pltpu
from jax.sharding import PartitionSpec as P

HD = 64
TOP_K = 6


epsilon = 1e-06


def root_norm(values_in, gain):
    floats = values_in.astype(jnp.float32)
    inv_root = lax.rsqrt(jnp.mean(floats * floats, axis=-1, keepdims=True) + epsilon)
    return floats * inv_root * gain.astype(jnp.float32)


def attend(hidden, attn_gain, query_weight, key_weight, value_weight, forget_weight, forget_bias,
           cache_keys, cache_values, cache_logsum, lengths):
    rows_here = hidden.shape[0]
    query_heads = query_weight.shape[1] // HD
    key_heads = key_weight.shape[1] // HD
    group_size = query_heads // key_heads
    cache_len = cache_keys.shape[-1]
    score_scale = HD ** (-0.5)
    normed = root_norm(hidden, attn_gain).astype(jnp.bfloat16)
    queries = jnp.dot(normed, query_weight, preferred_element_type=jnp.float32).astype(jnp.bfloat16)
    key_new = (
        jnp.dot(normed, key_weight, preferred_element_type=jnp.float32)
        .astype(jnp.bfloat16)
        .reshape(rows_here, key_heads, HD)
    )
    value_new = (
        jnp.dot(normed, value_weight, preferred_element_type=jnp.float32)
        .astype(jnp.bfloat16)
        .reshape(rows_here, key_heads, HD)
    )
    log_forget = jax.nn.log_sigmoid(
        jnp.dot(normed, forget_weight, preferred_element_type=jnp.float32) + forget_bias
    )
    positions = jnp.arange(cache_len, dtype=jnp.int32)
    is_last = positions[None, :] == (lengths - 1)[:, None]
    new_logsum = jnp.sum(jnp.where(is_last[:, None, :], cache_logsum, 0.0), axis=-1) + log_forget
    grouped = queries.reshape(rows_here, key_heads, group_size, HD)
    scores = jnp.einsum("sgjd,sgdp->sgjp", grouped, cache_keys, preferred_element_type=jnp.float32)
    scores = scores.reshape(rows_here, query_heads, cache_len) * score_scale
    scores = scores + new_logsum[:, :, None] - cache_logsum
    is_live = positions[None, :] < lengths[:, None]
    scores = jnp.where(is_live[:, None, :], scores, -jnp.inf)
    own_score = (
        jnp.einsum("sgjd,sgd->sgj", grouped, key_new, preferred_element_type=jnp.float32).reshape(
            rows_here, query_heads
        )
        * score_scale
    )
    top_score = jnp.maximum(jnp.max(scores, axis=-1), own_score)
    past_exp = jnp.exp(scores - top_score[:, :, None])
    own_exp = jnp.exp(own_score - top_score)
    denominator = jnp.sum(past_exp, axis=-1) + own_exp
    past_weight = (past_exp / denominator[:, :, None]).astype(jnp.bfloat16)
    own_weight = (own_exp / denominator).astype(jnp.bfloat16)
    attended = jnp.einsum(
        "sgjp,sgdp->sgjd",
        past_weight.reshape(rows_here, key_heads, group_size, cache_len),
        cache_values,
        preferred_element_type=jnp.float32,
    )
    attended = (
        attended
        + own_weight.astype(jnp.float32).reshape(rows_here, key_heads, group_size)[:, :, :, None]
        * value_new.astype(jnp.float32)[:, :, None, :]
    )
    attended = attended.reshape(rows_here, query_heads * HD).astype(jnp.bfloat16)
    return attended, key_new, value_new, new_logsum


def rest_general(attended, hidden, out_weight, ffn_gain, expert_ids, expert_scores,
                 gate_weights, up_weights, down_weights):
    rows_here = hidden.shape[0]
    whole_heads = lax.all_gather(attended, "tp", axis=1, tiled=True)
    projected = lax.dot_general(
        lax.all_gather(whole_heads, "ep", axis=0, tiled=True),
        out_weight,
        (((1,), (1,)), ((), ())),
        preferred_element_type=jnp.float32,
    ).astype(jnp.bfloat16)
    mixed = lax.all_to_all(projected, "ep", split_axis=0, concat_axis=1, tiled=True)
    residual = hidden.astype(jnp.float32) + mixed.astype(jnp.float32)
    ffn_in = root_norm(residual, ffn_gain).astype(jnp.bfloat16)
    ep_size = lax.axis_size("ep")
    local_experts = gate_weights.shape[0]
    experts = ep_size * local_experts
    route_count = rows_here * TOP_K
    capacity = 2 * ((route_count + experts - 1) // experts)
    flat_ids = expert_ids.reshape(route_count)
    onehot = (flat_ids[:, None] == jnp.arange(experts, dtype=jnp.int32)[None, :]).astype(jnp.int32)
    running = jnp.cumsum(onehot, axis=0)
    slot_index = jnp.sum(running * onehot, axis=1) - 1
    target = flat_ids * capacity + slot_index
    dispatch_map = (
        target[:, None] == jnp.arange(experts * capacity, dtype=jnp.int32)[None, :]
    ).astype(jnp.bfloat16)
    route_rows = jnp.repeat(ffn_in, TOP_K, axis=0)
    outgoing = lax.dot_general(
        dispatch_map, route_rows, (((0,), (0,)), ((), ())), preferred_element_type=jnp.float32
    )
    outgoing = outgoing.astype(jnp.bfloat16).reshape(
        ep_size, local_experts, capacity, ffn_in.shape[1]
    )
    arrived = lax.all_to_all(outgoing, "ep", split_axis=0, concat_axis=0, tiled=True)
    gate_act = jnp.einsum(
        "sekd,edf->sekf", arrived, gate_weights, preferred_element_type=jnp.float32
    )
    up_act = jnp.einsum("sekd,edf->sekf", arrived, up_weights, preferred_element_type=jnp.float32)
    hidden_act = (jax.nn.silu(gate_act) * up_act).astype(jnp.bfloat16)
    partial_out = jnp.einsum(
        "sekf,efd->sekd", hidden_act, down_weights, preferred_element_type=jnp.float32
    )
    half_sum = lax.psum_scatter(
        partial_out.astype(jnp.bfloat16), "tp", scatter_dimension=3, tiled=True
    )
    sent_back = lax.all_to_all(half_sum, "ep", split_axis=0, concat_axis=0, tiled=True)
    share_width = sent_back.shape[-1]
    picked = jnp.dot(
        dispatch_map,
        sent_back.reshape(experts * capacity, share_width),
        preferred_element_type=jnp.float32,
    )
    route_weight = expert_scores / jnp.sum(expert_scores, axis=-1, keepdims=True)
    expert_mix = jnp.sum(
        picked.reshape(rows_here, TOP_K, share_width) * route_weight[:, :, None], axis=1
    )
    own_part = lax.dynamic_slice_in_dim(
        residual, lax.axis_index("tp") * share_width, share_width, 1
    )
    updated = lax.all_gather((own_part + expert_mix).astype(jnp.bfloat16), "tp", axis=1, tiled=True)
    return updated


MESH = pl.DeviceIdType.MESH
PLANE = 4


def step_body(n, len_hbm, fbias_hbm, hid_hbm, again_hbm, fgain_hbm, ids_hbm, rscore_hbm,
              qw_hbm, kw_hbm, vw_hbm, fw_hbm, keys_hbm, vals_hbm, logs_hbm, ow_hbm, gate_hbm, up_hbm, down_hbm,
              out_ref, key_ref, val_ref, nlog_ref,
              len_ref, fbias_ref, hid_ref, again, fgain, fgain_row, ids_ref, rscore_ref, qw, kw, vw, fw, keys, vals, logs, scores, maxes, lasts, sums, mixed_heads, att, wsend, ow, gate, up, down,
              hidl, part, mixl, mixin, rows, ssq, ssqp, scales, wts, act, eout, back, fsum, far, upd,
              send, recv, local):
    f32, bf16 = jnp.float32, jnp.bfloat16
    me, tp = lax.axis_index("ep"), lax.axis_index("tp")
    seqs, width = hid_ref.shape
    cols = qw.shape[1]
    heads = cols // HD
    cache_len = keys.shape[2]
    outer = n // PLANE
    feats = wsend.shape[0]
    pf = PLANE * feats
    xq = pf // 2
    line = outer * seqs
    z, xy = me // PLANE, lax.rem(me, PLANE)
    x, y = lax.rem(xy, 2), xy // 2
    spots = [y * 2 + (1 - x), (1 - y) * 2 + x, (1 - y) * 2 + (1 - x)]
    plane = [z * PLANE + s for s in spots]

    def zdev(zz):
        return zz * PLANE + xy

    near_tables = [sorted([j for j in range(outer) if j != i], key=lambda j: (abs(j - i), j)) for i in range(outer)]
    far_tables = [sorted(range(outer), key=lambda j: (-abs(j - i), j)) for i in range(outer)]

    def pick(tables, k, zz):
        value = tables[0][k]
        for i in range(1, outer):
            value = jnp.where(zz == i, tables[i][k], value)
        return value

    zs = [pick(near_tables, k, z) for k in range(outer - 1)]
    dests = [pick(far_tables, k, z) for k in range(outer - 1)] + [z]

    def rows_of(g, zz):
        return sl(zz if g == outer - 1 else pick(far_tables, g, zz), seqs)

    used = {"s": 0, "r": 0, "l": 0}

    def take(kind, count=1):
        base = used[kind]
        used[kind] += count
        return base

    def copy(src, dst, s, r, ep, core):
        return pltpu.make_async_remote_copy(src_ref=src, dst_ref=dst, send_sem=send.at[s], recv_sem=recv.at[r],
                                            device_id=(ep, core), device_id_type=MESH)

    wholes = [0, 0]

    def group(whole):
        size = math.prod(whole.shape) * whole.dtype.itemsize
        kind = 0 if size % (32 * cols) == 0 else 1
        wholes[kind] += size
        return kind

    def begin(src, dst, s, r, ep, core):
        copy(src, dst, s, r, ep, core).start()

    def arrived(dst, r):
        copy(dst, dst, 0, r, me, 1 - tp).wait_recv()

    def load(src, dst, l=None):
        c = pltpu.make_async_copy(src, dst, local.at[take("l") if l is None else l])
        c.start()
        return c

    def sl(i, size):
        return pl.ds(pl.multiple_of(i * size, size), size)

    barrier = pltpu.get_barrier_semaphore()
    for d in range(1, outer):
        pl.semaphore_signal(barrier, inc=1, device_id=(zdev(lax.rem(z + d, outer)), tp), device_id_type=MESH)
    for p in plane:
        pl.semaphore_signal(barrier, inc=1, device_id=(p, tp), device_id_type=MESH)
    for p in plane[:2]:
        pl.semaphore_signal(barrier, inc=1, device_id=(p, 1 - tp), device_id_type=MESH)
    pl.semaphore_signal(barrier, inc=1, device_id=(me, 1 - tp), device_id_type=MESH)

    ow_load = load(ow_hbm.at[:, sl(tp, cols)], wsend)
    first_core, slot, own_l = xy // 2, lax.rem(xy, 2), take("l")

    @pl.when(tp == first_core)
    def own_rows():
        load(ow_hbm, ow.at[slot], own_l)

    first = [load(hid_hbm, hid_ref), load(again_hbm, again), load(ids_hbm, ids_ref), load(rscore_hbm, rscore_ref)]
    scalars = [load(fbias_hbm, fbias_ref), load(len_hbm, len_ref), load(fgain_hbm, fgain)]
    small_l, qw_l, keys_l, logs_l, vals_l = [take("l") for _ in range(5)]
    for src, dst in ((kw_hbm, kw), (vw_hbm, vw), (fw_hbm, fw)):
        load(src, dst, small_l)
    qchunk = width // 4
    for i in range(4):
        load(qw_hbm.at[pl.ds(i * qchunk, qchunk)], qw.at[pl.ds(i * qchunk, qchunk)], qw_l)
    batch = seqs // 4
    for i in range(4):
        some = pl.ds(i * batch, batch)
        load(keys_hbm.at[some, 0], keys.at[some], keys_l)
        load(logs_hbm.at[some], logs.at[some], logs_l)
    for i in range(4):
        some = pl.ds(i * batch, batch)
        load(vals_hbm.at[some, 0], vals.at[some], vals_l)

    def loaded(ref, l):
        pltpu.make_async_copy(ref, ref, local.at[l]).wait()

    pl.semaphore_wait(barrier, outer - 1 + 3 + 2 + 1)

    hf = feats // 2
    lo, hi = pl.ds(0, hf), pl.ds(hf, hf)
    ow_load.wait()
    ow_s, ow_r = group(ow.at[0]), take("r", 3)
    for i, some, r in ((0, lo, 0), (1, hi, 1), (0, hi, 2), (1, lo, 2)):
        begin(wsend.at[some], ow.at[slot, some, sl(tp, cols)], ow_s, ow_r + r, plane[i], first_core)

    for c in first:
        c.wait()
    normed = root_norm(hid_ref[...], again[...][None, :]).astype(bf16)
    rscore = rscore_ref[...]
    route = rscore / jnp.sum(rscore, axis=0, keepdims=True)
    ids = ids_ref[...].astype(f32)
    lanes = lax.broadcasted_iota(jnp.int32, (seqs, 128), 1).astype(f32)
    small_eye = (lax.broadcasted_iota(jnp.int32, (seqs, seqs), 0) == lax.broadcasted_iota(jnp.int32, (seqs, seqs), 1))

    def column(row):
        return jnp.sum(jnp.where(small_eye, jnp.broadcast_to(row, (seqs, seqs)), 0.0), axis=1, keepdims=True)

    table = jnp.zeros((seqs, 128), f32)
    for k in range(TOP_K):
        table = table + jnp.where(lanes == column(ids[k:k + 1, :]), column(route[k:k + 1, :]), 0.0)
    wts[3, sl(z, seqs), :] = table

    others = pl.ds(0, (outer - 1) * seqs)
    hid_s, hid_r = group(hidl.at[others]), take("r")
    for zz in zs:
        begin(hid_ref.at[:, pl.ds(pl.multiple_of(zz * pf + tp * xq, xq), xq)], hidl.at[sl(z, seqs)],
              hid_s, hid_r, zdev(zz), tp)
    hidl[sl(z, seqs), :] = hid_ref[:, pl.ds(pl.multiple_of(z * pf + tp * xq, xq), xq)]
    wt_s, wt_r = group(wts.at[0, others]), take("r")
    for zz in zs:
        begin(wts.at[3, sl(z, seqs)], wts.at[3, sl(z, seqs)], wt_s, wt_r, zdev(zz), tp)

    loaded(qw, qw_l)
    acc = jnp.dot(normed, qw[...], preferred_element_type=f32)
    queries = acc.astype(bf16).astype(f32) * (HD ** -0.5)
    loaded(qw.at[pl.ds(0, (2 * HD + heads) * width // cols)], small_l)
    for c in scalars:
        c.wait()
    fgain_row[...] = fgain[...].astype(f32)[None, :]

    def new_token(w):
        return lax.dot_general(normed, w[...], (((1,), (1,)), ((), ())), preferred_element_type=f32)

    key_new = new_token(kw).astype(bf16)
    value_new = new_token(vw).astype(bf16)
    key_ref[...] = key_new
    val_ref[...] = value_new
    hl = lax.broadcasted_iota(jnp.int32, (seqs, heads), 1)
    fb = jnp.zeros((seqs, heads), f32)
    for h in range(heads):
        fb = jnp.where(hl == h, fbias_ref[h], fb)
    pre = new_token(fw) + fb
    log_forget = jnp.minimum(pre, 0.0) - jnp.log1p(jnp.exp(-jnp.abs(pre)))

    expert_l = take("l")
    for t in range(2):
        for zc in range(outer):
            rows_from = pl.ds(zc * pf + t * xq, xq)
            load(gate_hbm.at[0, rows_from], gate.at[t * outer + zc], expert_l)
            load(up_hbm.at[0, rows_from], up.at[t * outer + zc], expert_l)
    down_s, down_r = group(down.at[0]), take("r")
    for zc in range(outer):
        mine = pl.ds(pl.multiple_of(zc * pf + tp * xq, xq), xq)
        other = pl.ds(pl.multiple_of(zc * pf + (1 - tp) * xq, xq), xq)
        load(down_hbm.at[0, :, mine], down.at[tp, :, pl.ds(zc * xq, xq)], expert_l)
        begin(down_hbm.at[0, :, other], down.at[tp, :, pl.ds(zc * xq, xq)], down_s, down_r, me, 1 - tp)

    total = seqs * heads

    def spread(v):
        return jnp.broadcast_to(v[:, None, :], (seqs, heads, v.shape[1])).reshape(total, v.shape[1])

    row_head = lax.rem(lax.broadcasted_iota(jnp.int32, (total, 128), 0), heads)
    picked = jnp.zeros((total, 128), f32)
    for j in range(cols // 128):
        picked = jnp.where(row_head // 2 == j, spread(queries[:, j * 128:(j + 1) * 128]), picked)
    picked = jnp.where(lax.rem(row_head, 2) == 0, picked, pltpu.roll(picked, HD, 1))[:, :HD]
    per_head = picked.astype(bf16)
    own = jnp.sum(picked * spread(key_new.astype(f32)), axis=-1, keepdims=True)

    positions = lax.broadcasted_iota(jnp.int32, (heads, cache_len), 1)
    for s in range(seqs):
        if s == 0:
            loaded(keys, keys_l)
            loaded(logs, logs_l)
        here = pl.ds(s * heads, heads)
        size = len_ref[s]
        level = logs[s]
        dots = jnp.dot(per_head[s * heads:(s + 1) * heads, :], keys[s], preferred_element_type=f32)
        past = jnp.where(positions < size, dots - level, -jnp.inf)
        scores[here, :] = past
        maxes[here, :] = jnp.broadcast_to(jnp.max(past, axis=-1, keepdims=True), (heads, 128))
        last = jnp.sum(jnp.where(positions == size - 1, level, 0.0), axis=-1, keepdims=True)
        lasts[here, :] = jnp.broadcast_to(last, (heads, 128))
    own_lane = lax.broadcasted_iota(jnp.int32, (total, heads), 1)
    own_row = lax.rem(lax.broadcasted_iota(jnp.int32, (total, heads), 0), heads)
    forget_col = jnp.sum(jnp.where(own_lane == own_row, spread(log_forget), 0.0), axis=-1, keepdims=True)
    newlog = lasts[:, :1] + forget_col
    nlog_ref[...] = jnp.sum(jnp.where(own_lane == own_row, jnp.broadcast_to(newlog, (total, heads)), 0.0)
                            .reshape(seqs, heads, heads), axis=1)
    own = own - newlog
    peak = jnp.maximum(maxes[:, :1], own)
    maxes[...] = jnp.broadcast_to(peak, (total, 128))
    for s in range(seqs):
        if s == 0:
            loaded(vals, vals_l)
        here = pl.ds(s * heads, heads)
        weights = jnp.exp(scores[here, :] - maxes[here, :][:, :1])
        sums[here, :] = jnp.broadcast_to(jnp.sum(weights, axis=-1, keepdims=True), (heads, 128))
        mixed_heads[here, :HD] = lax.dot_general(weights.astype(bf16), vals[s], (((1,), (1,)), ((), ())),
                                                 preferred_element_type=f32)
    own_exp = jnp.exp(own - peak)
    inverse = 1.0 / (sums[:, :1] + own_exp)
    outs = (mixed_heads[:, :HD] + own_exp * spread(value_new.astype(f32))) * inverse
    mixed_heads[:, :HD] = outs
    mixed_heads[:, HD:] = outs
    wide = lax.broadcasted_iota(jnp.int32, (seqs, 128), 1)
    for j in range(cols // 128):
        even = mixed_heads[pl.ds(2 * j, seqs, stride=heads), :]
        odd = mixed_heads[pl.ds(2 * j + 1, seqs, stride=heads), :]
        att[tp, sl(z, seqs), j * 128:(j + 1) * 128] = jnp.where(wide < HD, even, odd).astype(bf16)

    att_s, att_r = group(att.at[0, others]), take("r")
    for zz in reversed(zs):
        begin(att.at[tp, sl(z, seqs)], att.at[tp, sl(z, seqs)], att_s, att_r, zdev(zz), tp)
    relay_s, relay_r = group(ow.at[0, lo]), take("r")

    @pl.when(tp == first_core)
    def relay_along_y():
        half = ow.at[1 - slot, lo]
        arrived(half, ow_r)
        begin(half, half, relay_s, relay_r, plane[1], tp)

    @pl.when(tp != first_core)
    def relay_along_x():
        half = ow.at[slot, hi]
        arrived(half, ow_r + 1)
        begin(half, half, relay_s, relay_r, plane[0], tp)

    arrived(wts.at[0, others], wt_r)
    wline_s, wline_r = group(wts.at[pl.ds(0, 3)]), take("r")
    for i in range(3):
        begin(wts.at[3], wts.at[i], wline_s, wline_r, plane[i], tp)
    arrived(hidl.at[others], hid_r)
    arrived(att.at[0, others], att_r)
    both_s, both_r = group(att.at[0]), take("r")
    begin(att.at[tp], att.at[tp], both_s, both_r, me, 1 - tp)
    arrived(ow.at[0, lo], ow_r + 2)

    @pl.when(tp == first_core)
    def own_rows_there():
        loaded(ow.at[slot], own_l)

    arrived(att.at[1 - tp], both_r)
    lines = jnp.concatenate([att[0], att[1]], axis=1)

    def project(i):
        part[i] = lax.dot_general(lines, ow[i], (((1,), (1,)), ((), ())), preferred_element_type=f32)

    project(slot)

    @pl.when(tp != first_core)
    def last_rows_there():
        arrived(ow.at[1 - slot], relay_r)

    project(1 - slot)
    mixed = jnp.concatenate([part[0], part[1]], axis=1).astype(bf16)
    residual = hidl[...].astype(f32) + mixed.astype(f32)
    gain = fgain_row[:, pl.ds(pl.multiple_of(z * pf + tp * xq, xq), xq)]
    block = tp * outer + z
    rows[block, 3] = (residual * gain).astype(bf16)
    square = jnp.sum(residual * residual, axis=-1, keepdims=True)
    eye = (lax.broadcasted_iota(jnp.int32, (line, line), 0) == lax.broadcasted_iota(jnp.int32, (line, line), 1))
    flat = jnp.sum(jnp.where(eye, jnp.broadcast_to(square, (line, line)), 0.0), axis=0, keepdims=True)
    ssq[z, 3] = jnp.broadcast_to(flat, (8, line))
    mixl[...] = mixed

    zrow_s, zrow_r = group(rows.at[0, pl.ds(0, outer - 1)]), take("r", 2 * outer - 1)
    prow_s, prow_r = group(rows.at[pl.ds(0, 3)]), take("r", outer)
    crow_s, crow_r = group(rows.at[pl.ds(0, outer)]), take("r", outer)
    zsq_s, zsq_r = 2, take("r")
    psq_s, psq_r = 3, take("r")
    csq_s, csq_r = 3, take("r")
    mix_s, mix_r = group(mixl.at[others]), take("r")

    def out_to_plane(g, zz):
        b, some = tp * outer + zz, rows_of(g, z)
        for i in (2, 0, 1):
            begin(rows.at[b, 3, some], rows.at[b, i, some], prow_s, prow_r + g, plane[i], tp)

    for g in range(outer):
        for zz in reversed(zs):
            some = rows_of(g, zz)
            begin(rows.at[block, 3, some], rows.at[block, 3, some], zrow_s, zrow_r + (z if g == 0 else outer - 1 + g), zdev(zz), tp)
        if g == 0:
            for zz in reversed(zs):
                begin(ssq.at[z, 3], ssq.at[z, 3], zsq_s, zsq_r, zdev(zz), tp)
        out_to_plane(g, z)
    mixin[z] = mixl[sl(z, seqs), :]
    for g in range(outer):
        if g:
            arrived(rows.at[pl.ds(0, outer - 1), 3, rows_of(g, z)], zrow_r + outer - 1 + g)
        for zz in zs:
            if g == 0:
                arrived(rows.at[tp * outer + zz, 3, rows_of(g, z)], zrow_r + zz)
            out_to_plane(g, zz)
        if g == 0:
            arrived(ssq.at[0, pl.ds(0, outer - 1)], zsq_r)
            for i in range(3):
                begin(ssq.at[:, 3], ssq.at[:, i], psq_s, psq_r, plane[i], tp)
    for zz in zs:
        begin(mixl.at[sl(zz, seqs)], mixin.at[z], mix_s, mix_r, zdev(zz), tp)
    units = gate.shape[2]
    loaded(qw.at[pl.ds(0, (2 * width * units + units * width // 2) // cols)], expert_l)
    arrived(wts.at[pl.ds(0, 3)], wline_r)

    parts = [[g] for g in range(outer)]

    def product(part_groups, t):
        left = jnp.concatenate([
            jnp.concatenate([rows[t * outer + i, :, rows_of(g, z), :].reshape(PLANE * seqs, xq) for g in part_groups],
                            axis=0) for i in range(outer)], axis=1)
        span = pl.ds(t * outer, outer)
        return [jnp.dot(left, w[span].reshape(outer * xq, w.shape[2]), preferred_element_type=f32) for w in (gate, up)]

    def pass_on(part_groups):
        for g in part_groups:
            span, some = pl.ds(tp * outer, outer), rows_of(g, z)
            arrived(rows.at[span, pl.ds(0, 3), some], prow_r + g)
            block_rows = rows.at[span, :, some]
            begin(block_rows, block_rows, crow_s, crow_r + g, me, 1 - tp)

    def collect(part_groups, early):
        for g in part_groups:
            arrived(rows.at[pl.ds((1 - tp) * outer, outer), :, rows_of(g, z)], crow_r + g)
        late = product(part_groups, 1 - tp)
        return early[0] + late[0], early[1] + late[1]

    act_s, act_r = group(act.at[0]), take("r", outer)

    def span_of(part_groups):
        return pl.ds(part_groups[0], len(part_groups))

    def activate(part_groups, a, u):
        scale = jnp.concatenate([scales[:, rows_of(g, z), :].reshape(PLANE * seqs, 128)[:, :1] for g in part_groups],
                                axis=0)
        a, u = a * scale, u * scale
        made = (a / (1.0 + jnp.exp(-a)) * u).astype(bf16)
        here = act.at[tp, span_of(part_groups)]
        here[...] = made.reshape(len(part_groups), PLANE * seqs, made.shape[1])
        begin(here, here, act_s, act_r + part_groups[0], me, 1 - tp)

    back_s, back_r = group(eout.at[pl.ds(0, 3)]), take("r", outer)
    which = lax.broadcasted_iota(jnp.int32, (PLANE * seqs, 128), 1) == me

    def give(part_groups):
        span = span_of(part_groups)
        arrived(act.at[1 - tp, span], act_r + part_groups[0])
        lefts = [act[t, span].reshape(len(part_groups) * PLANE * seqs, act.shape[3]) for t in range(2)]
        made = (jnp.dot(lefts[0], down[0], preferred_element_type=f32)
                + jnp.dot(lefts[1], down[1], preferred_element_type=f32))
        for j, g in enumerate(part_groups):
            zz = dests[g]
            wt = wts[:, sl(zz, seqs), :].reshape(PLANE * seqs, 128)
            weight = jnp.sum(jnp.where(which, wt, 0.0), axis=-1, keepdims=True)
            scaled = made[j * PLANE * seqs:(j + 1) * PLANE * seqs] * weight
            eout[zz] = scaled.astype(bf16).reshape(PLANE, seqs, made.shape[1])
            for i in (2, 0, 1):
                begin(eout.at[zz, i], back.at[zz, i], back_s, back_r + zz, plane[i], tp)

    arrived(ssq.at[:, pl.ds(0, 3)], psq_r)
    squares = ssq[0]
    for i in range(1, outer):
        squares = squares + ssq[i]
    ssqp[tp] = squares
    begin(ssqp.at[tp], ssqp.at[tp], csq_s, csq_r, me, 1 - tp)
    pass_on(parts[0])
    early = product(parts[0], tp)
    pass_on(parts[1])
    a, u = collect(parts[0], early)
    arrived(ssqp.at[1 - tp], csq_r)
    squares = ssqp[0] + ssqp[1]
    for q in range(PLANE):
        scale = lax.rsqrt(squares[q, :1, :] * (1.0 / width) + epsilon)
        scale = jnp.sum(jnp.where(eye, jnp.broadcast_to(scale, (line, line)), 0.0), axis=1, keepdims=True)
        scales[q] = jnp.broadcast_to(scale, (line, 128))
    activate(parts[0], a, u)
    arrived(down.at[1 - tp], down_r)
    far_s, far_r = group(fsum.at[pl.ds(0, outer - 1)]), take("r")

    def near(g):
        zz = dests[g]
        arrived(back.at[zz], back_r + zz)
        summed = eout[zz, 3].astype(f32)
        for i in range(3):
            summed = summed + back[zz, i].astype(f32)
        if g < outer - 1:
            fsum[zz] = summed.astype(bf16)
            begin(fsum.at[zz], far.at[z], far_s, far_r, zdev(zz), tp)
        return summed

    last = len(parts) - 1
    for k in range(1, len(parts)):
        early = product(parts[k], tp)
        if k == last:
            give(parts[k - 1])
        elif k > 1:
            pass_on(parts[k + 1])
        a, u = collect(parts[k], early)
        activate(parts[k], a, u)
        if k == 1:
            pass_on(parts[2])
        if k < last:
            give(parts[k - 1])
    near(0)
    give(parts[last])
    for g in range(1, outer):
        summed = near(g)
    arrived(mixin.at[pl.ds(0, outer - 1)], mix_r)
    arrived(far.at[pl.ds(0, outer - 1)], far_r)
    for zz in zs:
        summed = summed + far[zz].astype(f32)
    for zc in range(outer):
        here = hid_ref[:, pl.ds(pl.multiple_of(zc * pf + tp * xq, xq), xq)].astype(f32) + mixin[zc].astype(f32)
        upd[tp, :, zc * xq:(zc + 1) * xq] = (here + summed[:, zc * xq:(zc + 1) * xq]).astype(bf16)
    u_s, u_r = group(upd.at[0]), take("r")
    begin(upd.at[tp], upd.at[tp], u_s, u_r, me, 1 - tp)
    arrived(upd.at[1 - tp], u_r)
    for t in range(2):
        for zc in range(outer):
            out_ref[:, zc * pf + t * xq:zc * pf + (t + 1) * xq] = upd[t, :, zc * xq:(zc + 1) * xq]
    assert wholes[0] % (32 * cols) == 0 and wholes[1] % 4096 == 0, wholes
    for s, whole in enumerate((qw.at[pl.ds(0, wholes[0] // (2 * cols))], maxes.at[pl.ds(0, wholes[1] // 512)],
                               ssq.at[0, pl.ds(0, outer - 1)], ssq)):
        copy(whole, whole, s, 0, me, 1 - tp).wait_send()
    assert used["r"] == recv.shape[0] and used["l"] == local.shape[0], used


def step_kernel(hidden, attn_gain, query_weight, key_weight, value_weight, forget_weight, forget_bias,
                cache_keys, cache_values, cache_logsum, lengths, out_weight, ffn_gain, expert_ids, expert_scores,
                gate_weights, up_weights, down_weights):
    n = lax.axis_size("ep")
    seqs, width = hidden.shape
    cols = query_weight.shape[1]
    heads = cols // HD
    cache_len = cache_keys.shape[3]
    feats = out_weight.shape[0]
    units = gate_weights.shape[2]
    outer = n // PLANE
    line = outer * seqs
    xq = PLANE * feats // 2
    half = width // 2
    bf16, f32 = jnp.bfloat16, jnp.float32
    vmem = pl.BlockSpec(memory_space=pltpu.VMEM)
    hbm = pl.BlockSpec(memory_space=pltpu.HBM)
    v = pltpu.VMEM
    results = pl.pallas_call(
        functools.partial(step_body, n),
        out_shape=[v((seqs, width), bf16), v((seqs, HD), bf16), v((seqs, HD), bf16), v((seqs, heads), f32)],
        in_specs=[hbm] * 18,
        out_specs=[vmem] * 4,
        scratch_shapes=[
            pltpu.SMEM((seqs,), jnp.int32), pltpu.SMEM((heads,), f32), v((seqs, width), bf16), v((width,), bf16),
            v((width,), bf16), v((1, width), f32), v((TOP_K, seqs), jnp.int32), v((TOP_K, seqs), f32),
            v((width, cols), bf16), v((HD, width), bf16), v((HD, width), bf16), v((heads, width), bf16),
            v((seqs, HD, cache_len), bf16), v((seqs, HD, cache_len), bf16), v((seqs, heads, cache_len), f32),
            v((seqs * heads, cache_len), f32), v((seqs * heads, 128), f32), v((seqs * heads, 128), f32),
            v((seqs * heads, 128), f32), v((seqs * heads, 2 * HD), f32),
            v((2, line, cols), bf16), v((feats, cols), bf16), v((2, feats, 2 * cols), bf16),
            v((2 * outer, xq, units), bf16), v((2 * outer, xq, units), bf16), v((2, units, half), bf16),
            v((line, xq), bf16), v((2, line, feats), f32), v((line, xq), bf16),
            v((outer, seqs, xq), bf16),
            v((2 * outer, PLANE, line, xq), bf16), v((outer, PLANE, 8, line), f32), v((2, PLANE, 8, line), f32),
            v((PLANE, line, 128), f32), v((PLANE, line, 128), f32),
                        v((2, outer, PLANE * seqs, units), bf16),
            v((outer, PLANE, seqs, half), bf16), v((outer, 3, seqs, half), bf16),
            v((outer, seqs, half), bf16), v((outer, seqs, half), bf16), v((2, seqs, half), bf16),
            pltpu.SemaphoreType.DMA((4,)), pltpu.SemaphoreType.DMA((15 + 6 * outer,)), pltpu.SemaphoreType.DMA((15,)),
        ],
        compiler_params=pltpu.CompilerParams(
            collective_id=0, has_side_effects=True, vmem_limit_bytes=40 * 1024 * 1024),
    )(*[pltpu.with_memory_space_constraint(a, pltpu.HBM) for a in (
        lengths, forget_bias, hidden, attn_gain, ffn_gain, expert_ids.T, expert_scores.T,
        query_weight, key_weight.T, value_weight.T, forget_weight.T, cache_keys, cache_values, cache_logsum,
        out_weight, gate_weights, up_weights, down_weights)])

    def hand_out(*refs):
        for i in range(4):
            refs[4 + i][...] = refs[i][...]

    updated, key_new, value_new, new_logsum = pl.pallas_call(
        hand_out,
        out_shape=[jax.ShapeDtypeStruct(r.shape, r.dtype) for r in results],
        in_specs=[vmem] * 4,
        out_specs=[vmem] * 4,
    )(*[pltpu.with_memory_space_constraint(r, pltpu.VMEM) for r in results])
    return updated, key_new.reshape(seqs, 1, HD), value_new.reshape(seqs, 1, HD), new_logsum


def per_device(hidden, attn_gain, query_weight, key_weight, value_weight, forget_weight, forget_bias,
               cache_keys, cache_values, cache_logsum, lengths, out_weight, ffn_gain, expert_ids, expert_scores,
               gate_weights, up_weights, down_weights):
    n = lax.axis_size("ep")
    seqs, width = hidden.shape
    fits = (
        n % (2 * PLANE) == 0
        and lax.axis_size("tp") == 2
        and gate_weights.shape[0] == 1
        and cache_keys.shape[1] == 1
        and seqs % 16 == 0
        and (query_weight.shape[1] // HD) % 16 == 0
        and out_weight.shape[0] % 128 == 0
        and n >= 4 * PLANE
        and n <= 128
    )
    if fits:
        return step_kernel(
            hidden, attn_gain, query_weight, key_weight, value_weight, forget_weight, forget_bias,
            cache_keys, cache_values, cache_logsum, lengths, out_weight, ffn_gain, expert_ids, expert_scores,
            gate_weights, up_weights, down_weights)
    attended, key_new, value_new, new_logsum = attend(
        hidden, attn_gain, query_weight, key_weight, value_weight, forget_weight, forget_bias,
        cache_keys, cache_values, cache_logsum, lengths)
    updated = rest_general(attended, hidden, out_weight, ffn_gain, expert_ids, expert_scores,
                           gate_weights, up_weights, down_weights)
    return (updated, key_new, value_new, new_logsum)


def solution(mesh):
    in_specs = (
        P("ep", None),
        P(),
        P(None, "tp"),
        P(None, "tp"),
        P(None, "tp"),
        P(None, "tp"),
        P("tp"),
        P("ep", "tp", None, None),
        P("ep", "tp", None, None),
        P("ep", "tp", None),
        P("ep"),
        P("ep", None),
        P(),
        P("ep", None),
        P("ep", None),
        P("ep", None, "tp"),
        P("ep", None, "tp"),
        P("ep", "tp", None),
    )
    out_specs = (P("ep", None), P("ep", "tp", None), P("ep", "tp", None), P("ep", "tp"))
    return jax.shard_map(
        per_device, mesh=mesh, in_specs=in_specs, out_specs=out_specs, check_vma=False
    )
```

```python
import functools
import math

import jax
import jax.numpy as jnp
from jax import lax
from jax.experimental import pallas as pl
from jax.experimental.pallas import tpu as pltpu
from jax.sharding import PartitionSpec as P

HD = 64
TOP_K = 6


epsilon = 1e-06


def root_norm(values_in, gain):
    floats = values_in.astype(jnp.float32)
    inv_root = lax.rsqrt(jnp.mean(floats * floats, axis=-1, keepdims=True) + epsilon)
    return floats * inv_root * gain.astype(jnp.float32)


def attend(hidden, attn_gain, query_weight, key_weight, value_weight, forget_weight, forget_bias,
           cache_keys, cache_values, cache_logsum, lengths):
    rows_here = hidden.shape[0]
    query_heads = query_weight.shape[1] // HD
    key_heads = key_weight.shape[1] // HD
    group_size = query_heads // key_heads
    cache_len = cache_keys.shape[-1]
    score_scale = HD ** (-0.5)
    normed = root_norm(hidden, attn_gain).astype(jnp.bfloat16)
    queries = jnp.dot(normed, query_weight, preferred_element_type=jnp.float32).astype(jnp.bfloat16)
    key_new = (
        jnp.dot(normed, key_weight, preferred_element_type=jnp.float32)
        .astype(jnp.bfloat16)
        .reshape(rows_here, key_heads, HD)
    )
    value_new = (
        jnp.dot(normed, value_weight, preferred_element_type=jnp.float32)
        .astype(jnp.bfloat16)
        .reshape(rows_here, key_heads, HD)
    )
    log_forget = jax.nn.log_sigmoid(
        jnp.dot(normed, forget_weight, preferred_element_type=jnp.float32) + forget_bias
    )
    positions = jnp.arange(cache_len, dtype=jnp.int32)
    is_last = positions[None, :] == (lengths - 1)[:, None]
    new_logsum = jnp.sum(jnp.where(is_last[:, None, :], cache_logsum, 0.0), axis=-1) + log_forget
    grouped = queries.reshape(rows_here, key_heads, group_size, HD)
    scores = jnp.einsum("sgjd,sgdp->sgjp", grouped, cache_keys, preferred_element_type=jnp.float32)
    scores = scores.reshape(rows_here, query_heads, cache_len) * score_scale
    scores = scores + new_logsum[:, :, None] - cache_logsum
    is_live = positions[None, :] < lengths[:, None]
    scores = jnp.where(is_live[:, None, :], scores, -jnp.inf)
    own_score = (
        jnp.einsum("sgjd,sgd->sgj", grouped, key_new, preferred_element_type=jnp.float32).reshape(
            rows_here, query_heads
        )
        * score_scale
    )
    top_score = jnp.maximum(jnp.max(scores, axis=-1), own_score)
    past_exp = jnp.exp(scores - top_score[:, :, None])
    own_exp = jnp.exp(own_score - top_score)
    denominator = jnp.sum(past_exp, axis=-1) + own_exp
    past_weight = (past_exp / denominator[:, :, None]).astype(jnp.bfloat16)
    own_weight = (own_exp / denominator).astype(jnp.bfloat16)
    attended = jnp.einsum(
        "sgjp,sgdp->sgjd",
        past_weight.reshape(rows_here, key_heads, group_size, cache_len),
        cache_values,
        preferred_element_type=jnp.float32,
    )
    attended = (
        attended
        + own_weight.astype(jnp.float32).reshape(rows_here, key_heads, group_size)[:, :, :, None]
        * value_new.astype(jnp.float32)[:, :, None, :]
    )
    attended = attended.reshape(rows_here, query_heads * HD).astype(jnp.bfloat16)
    return attended, key_new, value_new, new_logsum


def rest_general(attended, hidden, out_weight, ffn_gain, expert_ids, expert_scores,
                 gate_weights, up_weights, down_weights):
    rows_here = hidden.shape[0]
    whole_heads = lax.all_gather(attended, "tp", axis=1, tiled=True)
    projected = lax.dot_general(
        lax.all_gather(whole_heads, "ep", axis=0, tiled=True),
        out_weight,
        (((1,), (1,)), ((), ())),
        preferred_element_type=jnp.float32,
    ).astype(jnp.bfloat16)
    mixed = lax.all_to_all(projected, "ep", split_axis=0, concat_axis=1, tiled=True)
    residual = hidden.astype(jnp.float32) + mixed.astype(jnp.float32)
    ffn_in = root_norm(residual, ffn_gain).astype(jnp.bfloat16)
    ep_size = lax.axis_size("ep")
    local_experts = gate_weights.shape[0]
    experts = ep_size * local_experts
    route_count = rows_here * TOP_K
    capacity = 2 * ((route_count + experts - 1) // experts)
    flat_ids = expert_ids.reshape(route_count)
    onehot = (flat_ids[:, None] == jnp.arange(experts, dtype=jnp.int32)[None, :]).astype(jnp.int32)
    running = jnp.cumsum(onehot, axis=0)
    slot_index = jnp.sum(running * onehot, axis=1) - 1
    target = flat_ids * capacity + slot_index
    dispatch_map = (
        target[:, None] == jnp.arange(experts * capacity, dtype=jnp.int32)[None, :]
    ).astype(jnp.bfloat16)
    route_rows = jnp.repeat(ffn_in, TOP_K, axis=0)
    outgoing = lax.dot_general(
        dispatch_map, route_rows, (((0,), (0,)), ((), ())), preferred_element_type=jnp.float32
    )
    outgoing = outgoing.astype(jnp.bfloat16).reshape(
        ep_size, local_experts, capacity, ffn_in.shape[1]
    )
    arrived = lax.all_to_all(outgoing, "ep", split_axis=0, concat_axis=0, tiled=True)
    gate_act = jnp.einsum(
        "sekd,edf->sekf", arrived, gate_weights, preferred_element_type=jnp.float32
    )
    up_act = jnp.einsum("sekd,edf->sekf", arrived, up_weights, preferred_element_type=jnp.float32)
    hidden_act = (jax.nn.silu(gate_act) * up_act).astype(jnp.bfloat16)
    partial_out = jnp.einsum(
        "sekf,efd->sekd", hidden_act, down_weights, preferred_element_type=jnp.float32
    )
    half_sum = lax.psum_scatter(
        partial_out.astype(jnp.bfloat16), "tp", scatter_dimension=3, tiled=True
    )
    sent_back = lax.all_to_all(half_sum, "ep", split_axis=0, concat_axis=0, tiled=True)
    share_width = sent_back.shape[-1]
    picked = jnp.dot(
        dispatch_map,
        sent_back.reshape(experts * capacity, share_width),
        preferred_element_type=jnp.float32,
    )
    route_weight = expert_scores / jnp.sum(expert_scores, axis=-1, keepdims=True)
    expert_mix = jnp.sum(
        picked.reshape(rows_here, TOP_K, share_width) * route_weight[:, :, None], axis=1
    )
    own_part = lax.dynamic_slice_in_dim(
        residual, lax.axis_index("tp") * share_width, share_width, 1
    )
    updated = lax.all_gather((own_part + expert_mix).astype(jnp.bfloat16), "tp", axis=1, tiled=True)
    return updated


MESH = pl.DeviceIdType.MESH
PLANE = 4


def step_body(n, len_hbm, fbias_hbm, hid_hbm, again_hbm, fgain_hbm, ids_hbm, rscore_hbm,
              qw_hbm, kw_hbm, vw_hbm, fw_hbm, keys_hbm, vals_hbm, logs_hbm, ow_hbm, gate_hbm, up_hbm, down_hbm,
              out_ref, key_ref, val_ref, nlog_ref,
              len_ref, fbias_ref, hid_ref, again, fgain, fgain_row, ids_ref, rscore_ref, qw, kw, vw, fw, keys, vals, logs, scores, maxes, lasts, sums, mixed_heads, att, wsend, ow, gate, up, down,
              hidl, part, mixl, mixin, rows, ssq, ssqp, scales, wts, begun, act, eout, back, fsum, far, upd,
              send, recv, local):
    f32, bf16 = jnp.float32, jnp.bfloat16
    me, tp = lax.axis_index("ep"), lax.axis_index("tp")
    seqs, width = hid_ref.shape
    cols = qw.shape[1]
    heads = cols // HD
    cache_len = keys.shape[2]
    outer = n // PLANE
    feats = wsend.shape[0]
    pf = PLANE * feats
    xq = pf // 2
    line = outer * seqs
    z, xy = me // PLANE, lax.rem(me, PLANE)
    x, y = lax.rem(xy, 2), xy // 2
    spots = [y * 2 + (1 - x), (1 - y) * 2 + x, (1 - y) * 2 + (1 - x)]
    plane = [z * PLANE + s for s in spots]

    def zdev(zz):
        return zz * PLANE + xy

    near_tables = [sorted([j for j in range(outer) if j != i], key=lambda j: (abs(j - i), j)) for i in range(outer)]
    far_tables = [sorted(range(outer), key=lambda j: (-abs(j - i), j)) for i in range(outer)]

    def pick(tables, k, zz):
        value = tables[0][k]
        for i in range(1, outer):
            value = jnp.where(zz == i, tables[i][k], value)
        return value

    zs = [pick(near_tables, k, z) for k in range(outer - 1)]
    dests = [pick(far_tables, k, z) for k in range(outer - 1)] + [z]

    def rows_of(g, zz):
        return sl(zz if g == outer - 1 else pick(far_tables, g, zz), seqs)

    used = {"s": 0, "r": 0, "l": 0}

    def take(kind, count=1):
        base = used[kind]
        used[kind] += count
        return base

    def copy(src, dst, s, r, ep, core):
        return pltpu.make_async_remote_copy(src_ref=src, dst_ref=dst, send_sem=send.at[s], recv_sem=recv.at[r],
                                            device_id=(ep, core), device_id_type=MESH)

    wholes = [0, 0]

    def group(whole):
        size = math.prod(whole.shape) * whole.dtype.itemsize
        kind = 0 if size % (32 * cols) == 0 else 1
        wholes[kind] += size
        return kind

    def begin(src, dst, s, r, ep, core):
        copy(src, dst, s, r, ep, core).start()

    def arrived(dst, r):
        copy(dst, dst, 0, r, me, 1 - tp).wait_recv()

    def load(src, dst, l=None):
        c = pltpu.make_async_copy(src, dst, local.at[take("l") if l is None else l])
        c.start()
        return c

    def sl(i, size):
        return pl.ds(pl.multiple_of(i * size, size), size)

    barrier = pltpu.get_barrier_semaphore()
    for d in range(1, outer):
        pl.semaphore_signal(barrier, inc=1, device_id=(zdev(lax.rem(z + d, outer)), tp), device_id_type=MESH)
    for p in plane:
        pl.semaphore_signal(barrier, inc=1, device_id=(p, tp), device_id_type=MESH)
    for p in plane[:2]:
        pl.semaphore_signal(barrier, inc=1, device_id=(p, 1 - tp), device_id_type=MESH)
    pl.semaphore_signal(barrier, inc=1, device_id=(me, 1 - tp), device_id_type=MESH)

    ow_load = load(ow_hbm.at[:, sl(tp, cols)], wsend)
    first_core, slot, own_l = xy // 2, lax.rem(xy, 2), take("l")

    first = [load(hid_hbm, hid_ref), load(again_hbm, again), load(ids_hbm, ids_ref), load(rscore_hbm, rscore_ref)]
    scalars = [load(fbias_hbm, fbias_ref), load(len_hbm, len_ref), load(fgain_hbm, fgain)]
    small_l, qw_l, keys_l, logs_l, vals_l = [take("l") for _ in range(5)]
    for src, dst in ((kw_hbm, kw), (vw_hbm, vw), (fw_hbm, fw)):
        load(src, dst, small_l)
    qchunk = width // 4
    for i in range(4):
        load(qw_hbm.at[pl.ds(i * qchunk, qchunk)], qw.at[pl.ds(i * qchunk, qchunk)], qw_l)
    batch = seqs // 4
    for i in range(4):
        some = pl.ds(i * batch, batch)
        load(keys_hbm.at[some, 0], keys.at[some], keys_l)
        load(logs_hbm.at[some], logs.at[some], logs_l)
    for i in range(4):
        some = pl.ds(i * batch, batch)
        load(vals_hbm.at[some, 0], vals.at[some], vals_l)

    def loaded(ref, l):
        pltpu.make_async_copy(ref, ref, local.at[l]).wait()

    pl.semaphore_wait(barrier, outer - 1 + 3 + 2 + 1)

    hf = feats // 2
    lo, hi = pl.ds(0, hf), pl.ds(hf, hf)
    ow_load.wait()
    ow_s, ow_r = group(ow.at[0]), take("r", 5)
    quarters = [pl.ds(k * hf // 2, hf // 2) for k in range(4)]
    for i, some, r in ((0, quarters[0], 0), (1, quarters[2], 1), (0, quarters[1], 2), (1, quarters[3], 3),
                       (0, hi, 4), (1, lo, 4)):
        begin(wsend.at[some], ow.at[slot, some, sl(tp, cols)], ow_s, ow_r + r, plane[i], first_core)

    @pl.when(tp == first_core)
    def own_rows():
        load(ow_hbm, ow.at[slot], own_l)

    for c in first:
        c.wait()
    normed = root_norm(hid_ref[...], again[...][None, :]).astype(bf16)
    rscore = rscore_ref[...]
    route = rscore / jnp.sum(rscore, axis=0, keepdims=True)
    ids = ids_ref[...].astype(f32)
    lanes = lax.broadcasted_iota(jnp.int32, (seqs, 128), 1).astype(f32)
    small_eye = (lax.broadcasted_iota(jnp.int32, (seqs, seqs), 0) == lax.broadcasted_iota(jnp.int32, (seqs, seqs), 1))

    def column(row):
        return jnp.sum(jnp.where(small_eye, jnp.broadcast_to(row, (seqs, seqs)), 0.0), axis=1, keepdims=True)

    table = jnp.zeros((seqs, 128), f32)
    for k in range(TOP_K):
        table = table + jnp.where(lanes == column(ids[k:k + 1, :]), column(route[k:k + 1, :]), 0.0)
    wts[3, sl(z, seqs), :] = table

    others = pl.ds(0, (outer - 1) * seqs)
    hid_s, hid_r = group(hidl.at[others]), take("r")
    for zz in zs:
        begin(hid_ref.at[:, pl.ds(pl.multiple_of(zz * pf + tp * xq, xq), xq)], hidl.at[sl(z, seqs)],
              hid_s, hid_r, zdev(zz), tp)
    hidl[sl(z, seqs), :] = hid_ref[:, pl.ds(pl.multiple_of(z * pf + tp * xq, xq), xq)]
    wt_s, wt_r = group(wts.at[0, others]), take("r")
    for zz in zs:
        begin(wts.at[3, sl(z, seqs)], wts.at[3, sl(z, seqs)], wt_s, wt_r, zdev(zz), tp)

    loaded(qw, qw_l)
    acc = jnp.dot(normed, qw[...], preferred_element_type=f32)
    queries = acc.astype(bf16).astype(f32) * (HD ** -0.5)
    loaded(qw.at[pl.ds(0, (2 * HD + heads) * width // cols)], small_l)
    for c in scalars:
        c.wait()
    fgain_row[...] = fgain[...].astype(f32)[None, :]

    def new_token(w):
        return lax.dot_general(normed, w[...], (((1,), (1,)), ((), ())), preferred_element_type=f32)

    key_new = new_token(kw).astype(bf16)
    value_new = new_token(vw).astype(bf16)
    key_ref[...] = key_new
    val_ref[...] = value_new
    hl = lax.broadcasted_iota(jnp.int32, (seqs, heads), 1)
    fb = jnp.zeros((seqs, heads), f32)
    for h in range(heads):
        fb = jnp.where(hl == h, fbias_ref[h], fb)
    pre = new_token(fw) + fb
    log_forget = jnp.minimum(pre, 0.0) - jnp.log1p(jnp.exp(-jnp.abs(pre)))

    expert_l = take("l")
    for t in range(2):
        for zc in range(outer):
            rows_from = pl.ds(zc * pf + t * xq, xq)
            load(gate_hbm.at[0, rows_from], gate.at[t * outer + zc], expert_l)
            load(up_hbm.at[0, rows_from], up.at[t * outer + zc], expert_l)
    down_s, down_r = group(down.at[0]), take("r")
    for zc in range(outer):
        mine = pl.ds(pl.multiple_of(zc * pf + tp * xq, xq), xq)
        other = pl.ds(pl.multiple_of(zc * pf + (1 - tp) * xq, xq), xq)
        load(down_hbm.at[0, :, mine], down.at[tp, :, pl.ds(zc * xq, xq)], expert_l)
        begin(down_hbm.at[0, :, other], down.at[tp, :, pl.ds(zc * xq, xq)], down_s, down_r, me, 1 - tp)

    total = seqs * heads

    def spread(v):
        return jnp.broadcast_to(v[:, None, :], (seqs, heads, v.shape[1])).reshape(total, v.shape[1])

    row_head = lax.rem(lax.broadcasted_iota(jnp.int32, (total, 128), 0), heads)
    picked = jnp.zeros((total, 128), f32)
    for j in range(cols // 128):
        picked = jnp.where(row_head // 2 == j, spread(queries[:, j * 128:(j + 1) * 128]), picked)
    picked = jnp.where(lax.rem(row_head, 2) == 0, picked, pltpu.roll(picked, HD, 1))[:, :HD]
    per_head = picked.astype(bf16)
    own = jnp.sum(picked * spread(key_new.astype(f32)), axis=-1, keepdims=True)

    positions = lax.broadcasted_iota(jnp.int32, (heads, cache_len), 1)
    for s in range(seqs):
        if s == 0:
            loaded(keys, keys_l)
            loaded(logs, logs_l)
        here = pl.ds(s * heads, heads)
        size = len_ref[s]
        level = logs[s]
        dots = jnp.dot(per_head[s * heads:(s + 1) * heads, :], keys[s], preferred_element_type=f32)
        past = jnp.where(positions < size, dots - level, -jnp.inf)
        scores[here, :] = past
        maxes[here, :] = jnp.broadcast_to(jnp.max(past, axis=-1, keepdims=True), (heads, 128))
        last = jnp.sum(jnp.where(positions == size - 1, level, 0.0), axis=-1, keepdims=True)
        lasts[here, :] = jnp.broadcast_to(last, (heads, 128))
    own_lane = lax.broadcasted_iota(jnp.int32, (total, heads), 1)
    own_row = lax.rem(lax.broadcasted_iota(jnp.int32, (total, heads), 0), heads)
    forget_col = jnp.sum(jnp.where(own_lane == own_row, spread(log_forget), 0.0), axis=-1, keepdims=True)
    newlog = lasts[:, :1] + forget_col
    nlog_ref[...] = jnp.sum(jnp.where(own_lane == own_row, jnp.broadcast_to(newlog, (total, heads)), 0.0)
                            .reshape(seqs, heads, heads), axis=1)
    own = own - newlog
    peak = jnp.maximum(maxes[:, :1], own)
    maxes[...] = jnp.broadcast_to(peak, (total, 128))
    for s in range(seqs):
        if s == 0:
            loaded(vals, vals_l)
        here = pl.ds(s * heads, heads)
        weights = jnp.exp(scores[here, :] - maxes[here, :][:, :1])
        sums[here, :] = jnp.broadcast_to(jnp.sum(weights, axis=-1, keepdims=True), (heads, 128))
        mixed_heads[here, :HD] = lax.dot_general(weights.astype(bf16), vals[s], (((1,), (1,)), ((), ())),
                                                 preferred_element_type=f32)
    own_exp = jnp.exp(own - peak)
    inverse = 1.0 / (sums[:, :1] + own_exp)
    outs = (mixed_heads[:, :HD] + own_exp * spread(value_new.astype(f32))) * inverse
    mixed_heads[:, :HD] = outs
    mixed_heads[:, HD:] = outs
    wide = lax.broadcasted_iota(jnp.int32, (seqs, 128), 1)
    for j in range(cols // 128):
        even = mixed_heads[pl.ds(2 * j, seqs, stride=heads), :]
        odd = mixed_heads[pl.ds(2 * j + 1, seqs, stride=heads), :]
        att[tp, sl(z, seqs), j * 128:(j + 1) * 128] = jnp.where(wide < HD, even, odd).astype(bf16)

    att_s, att_r = group(att.at[0, others]), take("r")
    for zz in reversed(zs):
        begin(att.at[tp, sl(z, seqs)], att.at[tp, sl(z, seqs)], att_s, att_r, zdev(zz), tp)
    relay_s, relay_r = group(ow.at[0, lo]), take("r")

    @pl.when(tp == first_core)
    def relay_along_y():
        for k in range(2):
            piece = ow.at[1 - slot, quarters[k]]
            arrived(piece, ow_r + 2 * k)
            begin(piece, piece, relay_s, relay_r, plane[1], tp)

    @pl.when(tp != first_core)
    def relay_along_x():
        for k in range(2):
            piece = ow.at[slot, quarters[2 + k]]
            arrived(piece, ow_r + 1 + 2 * k)
            begin(piece, piece, relay_s, relay_r, plane[0], tp)

    arrived(wts.at[0, others], wt_r)
    wline_s, wline_r = group(wts.at[pl.ds(0, 3)]), take("r")
    for i in range(3):
        begin(wts.at[3], wts.at[i], wline_s, wline_r, plane[i], tp)
    arrived(hidl.at[others], hid_r)
    arrived(att.at[0, others], att_r)
    both_s, both_r = group(att.at[0]), take("r")
    begin(att.at[tp], att.at[tp], both_s, both_r, me, 1 - tp)
    arrived(ow.at[0, lo], ow_r + 4)

    @pl.when(tp == first_core)
    def own_rows_there():
        loaded(ow.at[slot], own_l)

    arrived(att.at[1 - tp], both_r)
    lines = jnp.concatenate([att[0], att[1]], axis=1)

    def project(i):
        part[i] = lax.dot_general(lines, ow[i], (((1,), (1,)), ((), ())), preferred_element_type=f32)

    project(slot)

    @pl.when(tp != first_core)
    def last_rows_there():
        arrived(ow.at[1 - slot], relay_r)

    project(1 - slot)
    mixed = jnp.concatenate([part[0], part[1]], axis=1).astype(bf16)
    residual = hidl[...].astype(f32) + mixed.astype(f32)
    gain = fgain_row[:, pl.ds(pl.multiple_of(z * pf + tp * xq, xq), xq)]
    block = tp * outer + z
    rows[block, 3] = (residual * gain).astype(bf16)
    square = jnp.sum(residual * residual, axis=-1, keepdims=True)
    eye = (lax.broadcasted_iota(jnp.int32, (line, line), 0) == lax.broadcasted_iota(jnp.int32, (line, line), 1))
    flat = jnp.sum(jnp.where(eye, jnp.broadcast_to(square, (line, line)), 0.0), axis=0, keepdims=True)
    ssq[z, 3] = jnp.broadcast_to(flat, (8, line))
    mixl[...] = mixed

    zrow_s, zrow_r = group(rows.at[0, pl.ds(0, outer - 1)]), take("r", 2 * outer - 1)
    prow_s, prow_r = group(rows.at[pl.ds(0, 3)]), take("r", outer)
    crow_s, crow_r = group(rows.at[pl.ds(0, outer)]), take("r", outer)
    zsq_s, zsq_r = 2, take("r")
    psq_s, psq_r = 3, take("r")
    csq_s, csq_r = 3, take("r")
    mix_s, mix_r = group(mixl.at[others]), take("r")

    def out_to_plane(g, zz):
        b, some = tp * outer + zz, rows_of(g, z)
        for i in (2, 0, 1):
            begin(rows.at[b, 3, some], rows.at[b, i, some], prow_s, prow_r + g, plane[i], tp)

    for g in range(outer):
        for zz in reversed(zs):
            some = rows_of(g, zz)
            begin(rows.at[block, 3, some], rows.at[block, 3, some], zrow_s, zrow_r + (z if g == 0 else outer - 1 + g), zdev(zz), tp)
        if g == 0:
            for zz in reversed(zs):
                begin(ssq.at[z, 3], ssq.at[z, 3], zsq_s, zsq_r, zdev(zz), tp)
        out_to_plane(g, z)
    mixin[z] = mixl[sl(z, seqs), :]
    for g in range(outer):
        if g:
            arrived(rows.at[pl.ds(0, outer - 1), 3, rows_of(g, z)], zrow_r + outer - 1 + g)
        for zz in zs:
            if g == 0:
                arrived(rows.at[tp * outer + zz, 3, rows_of(g, z)], zrow_r + zz)
            out_to_plane(g, zz)
        if g == 0:
            arrived(ssq.at[0, pl.ds(0, outer - 1)], zsq_r)
            for i in range(3):
                begin(ssq.at[:, 3], ssq.at[:, i], psq_s, psq_r, plane[i], tp)
    for zz in zs:
        begin(mixl.at[sl(zz, seqs)], mixin.at[z], mix_s, mix_r, zdev(zz), tp)
    units = gate.shape[2]
    loaded(qw.at[pl.ds(0, (2 * width * units + units * width // 2) // cols)], expert_l)
    arrived(wts.at[pl.ds(0, 3)], wline_r)

    parts = [[g] for g in range(outer)]

    def product(part_groups, t):
        left = jnp.concatenate([
            jnp.concatenate([rows[t * outer + i, :, rows_of(g, z), :].reshape(PLANE * seqs, xq) for g in part_groups],
                            axis=0) for i in range(outer)], axis=1)
        span = pl.ds(t * outer, outer)
        return [jnp.dot(left, w[span].reshape(outer * xq, w.shape[2]), preferred_element_type=f32) for w in (gate, up)]

    def pass_on(part_groups):
        for g in part_groups:
            span, some = pl.ds(tp * outer, outer), rows_of(g, z)
            arrived(rows.at[span, pl.ds(0, 3), some], prow_r + g)
            block_rows = rows.at[span, :, some]
            begin(block_rows, block_rows, crow_s, crow_r + g, me, 1 - tp)

    def start(part_groups):
        k = part_groups[0] % 2
        for i, v in enumerate(product(part_groups, tp)):
            begun[k, i] = v
        return k

    def collect(part_groups, k):
        for g in part_groups:
            arrived(rows.at[pl.ds((1 - tp) * outer, outer), :, rows_of(g, z)], crow_r + g)
        late = product(part_groups, 1 - tp)
        return begun[k, 0] + late[0], begun[k, 1] + late[1]

    act_s, act_r = group(act.at[0]), take("r", outer)

    def span_of(part_groups):
        return pl.ds(part_groups[0], len(part_groups))

    def activate(part_groups, a, u):
        scale = jnp.concatenate([scales[:, rows_of(g, z), :].reshape(PLANE * seqs, 128)[:, :1] for g in part_groups],
                                axis=0)
        a, u = a * scale, u * scale
        made = (a / (1.0 + jnp.exp(-a)) * u).astype(bf16)
        here = act.at[tp, span_of(part_groups)]
        here[...] = made.reshape(len(part_groups), PLANE * seqs, made.shape[1])
        begin(here, here, act_s, act_r + part_groups[0], me, 1 - tp)

    back_s, back_r = group(eout.at[pl.ds(0, 3)]), take("r", outer)
    which = lax.broadcasted_iota(jnp.int32, (PLANE * seqs, 128), 1) == me

    def give(part_groups):
        span = span_of(part_groups)
        arrived(act.at[1 - tp, span], act_r + part_groups[0])
        lefts = [act[t, span].reshape(len(part_groups) * PLANE * seqs, act.shape[3]) for t in range(2)]
        made = (jnp.dot(lefts[0], down[0], preferred_element_type=f32)
                + jnp.dot(lefts[1], down[1], preferred_element_type=f32))
        for j, g in enumerate(part_groups):
            zz = dests[g]
            wt = wts[:, sl(zz, seqs), :].reshape(PLANE * seqs, 128)
            weight = jnp.sum(jnp.where(which, wt, 0.0), axis=-1, keepdims=True)
            scaled = made[j * PLANE * seqs:(j + 1) * PLANE * seqs] * weight
            eout[zz] = scaled.astype(bf16).reshape(PLANE, seqs, made.shape[1])
            for i in (2, 0, 1):
                begin(eout.at[zz, i], back.at[zz, i], back_s, back_r + zz, plane[i], tp)

    pass_on(parts[0])
    arrived(ssq.at[:, pl.ds(0, 3)], psq_r)
    squares = ssq[0]
    for i in range(1, outer):
        squares = squares + ssq[i]
    ssqp[tp] = squares
    begin(ssqp.at[tp], ssqp.at[tp], csq_s, csq_r, me, 1 - tp)
    early = start(parts[0])
    pass_on(parts[1])
    a, u = collect(parts[0], early)
    arrived(ssqp.at[1 - tp], csq_r)
    squares = ssqp[0] + ssqp[1]
    for q in range(PLANE):
        scale = lax.rsqrt(squares[q, :1, :] * (1.0 / width) + epsilon)
        scale = jnp.sum(jnp.where(eye, jnp.broadcast_to(scale, (line, line)), 0.0), axis=1, keepdims=True)
        scales[q] = jnp.broadcast_to(scale, (line, 128))
    activate(parts[0], a, u)
    arrived(down.at[1 - tp], down_r)
    far_s, far_r = group(fsum.at[pl.ds(0, outer - 1)]), take("r")

    def near(g):
        zz = dests[g]
        arrived(back.at[zz], back_r + zz)
        summed = eout[zz, 3].astype(f32)
        for i in range(3):
            summed = summed + back[zz, i].astype(f32)
        if g < outer - 1:
            fsum[zz] = summed.astype(bf16)
            begin(fsum.at[zz], far.at[z], far_s, far_r, zdev(zz), tp)
        return summed

    last = len(parts) - 1
    for k in range(1, len(parts)):
        early = start(parts[k])
        if k == last:
            give(parts[k - 1])
        elif k > 1:
            pass_on(parts[k + 1])
        a, u = collect(parts[k], early)
        activate(parts[k], a, u)
        if k == 1:
            pass_on(parts[2])
        if k < last:
            give(parts[k - 1])
    near(0)
    give(parts[last])
    for g in range(1, outer):
        summed = near(g)
    arrived(mixin.at[pl.ds(0, outer - 1)], mix_r)
    arrived(far.at[pl.ds(0, outer - 1)], far_r)
    for zz in zs:
        summed = summed + far[zz].astype(f32)
    for zc in range(outer):
        here = hid_ref[:, pl.ds(pl.multiple_of(zc * pf + tp * xq, xq), xq)].astype(f32) + mixin[zc].astype(f32)
        upd[tp, :, zc * xq:(zc + 1) * xq] = (here + summed[:, zc * xq:(zc + 1) * xq]).astype(bf16)
    u_s, u_r = group(upd.at[0]), take("r")
    begin(upd.at[tp], upd.at[tp], u_s, u_r, me, 1 - tp)
    arrived(upd.at[1 - tp], u_r)
    for t in range(2):
        for zc in range(outer):
            out_ref[:, zc * pf + t * xq:zc * pf + (t + 1) * xq] = upd[t, :, zc * xq:(zc + 1) * xq]
    assert wholes[0] % (32 * cols) == 0 and wholes[1] % 4096 == 0, wholes
    for s, whole in enumerate((qw.at[pl.ds(0, wholes[0] // (2 * cols))], maxes.at[pl.ds(0, wholes[1] // 512)],
                               ssq.at[0, pl.ds(0, outer - 1)], ssq)):
        copy(whole, whole, s, 0, me, 1 - tp).wait_send()
    assert used["r"] == recv.shape[0] and used["l"] == local.shape[0], used


def step_kernel(hidden, attn_gain, query_weight, key_weight, value_weight, forget_weight, forget_bias,
                cache_keys, cache_values, cache_logsum, lengths, out_weight, ffn_gain, expert_ids, expert_scores,
                gate_weights, up_weights, down_weights):
    n = lax.axis_size("ep")
    seqs, width = hidden.shape
    cols = query_weight.shape[1]
    heads = cols // HD
    cache_len = cache_keys.shape[3]
    feats = out_weight.shape[0]
    units = gate_weights.shape[2]
    outer = n // PLANE
    line = outer * seqs
    xq = PLANE * feats // 2
    half = width // 2
    bf16, f32 = jnp.bfloat16, jnp.float32
    vmem = pl.BlockSpec(memory_space=pltpu.VMEM)
    hbm = pl.BlockSpec(memory_space=pltpu.HBM)
    v = pltpu.VMEM
    results = pl.pallas_call(
        functools.partial(step_body, n),
        out_shape=[v((seqs, width), bf16), v((seqs, HD), bf16), v((seqs, HD), bf16), v((seqs, heads), f32)],
        in_specs=[hbm] * 18,
        out_specs=[vmem] * 4,
        scratch_shapes=[
            pltpu.SMEM((seqs,), jnp.int32), pltpu.SMEM((heads,), f32), v((seqs, width), bf16), v((width,), bf16),
            v((width,), bf16), v((1, width), f32), v((TOP_K, seqs), jnp.int32), v((TOP_K, seqs), f32),
            v((width, cols), bf16), v((HD, width), bf16), v((HD, width), bf16), v((heads, width), bf16),
            v((seqs, HD, cache_len), bf16), v((seqs, HD, cache_len), bf16), v((seqs, heads, cache_len), f32),
            v((seqs * heads, cache_len), f32), v((seqs * heads, 128), f32), v((seqs * heads, 128), f32),
            v((seqs * heads, 128), f32), v((seqs * heads, 2 * HD), f32),
            v((2, line, cols), bf16), v((feats, cols), bf16), v((2, feats, 2 * cols), bf16),
            v((2 * outer, xq, units), bf16), v((2 * outer, xq, units), bf16), v((2, units, half), bf16),
            v((line, xq), bf16), v((2, line, feats), f32), v((line, xq), bf16),
            v((outer, seqs, xq), bf16),
            v((2 * outer, PLANE, line, xq), bf16), v((outer, PLANE, 8, line), f32), v((2, PLANE, 8, line), f32),
            v((PLANE, line, 128), f32), v((PLANE, line, 128), f32),
                        v((2, 2, PLANE * seqs, units), f32), v((2, outer, PLANE * seqs, units), bf16),
            v((outer, PLANE, seqs, half), bf16), v((outer, 3, seqs, half), bf16),
            v((outer, seqs, half), bf16), v((outer, seqs, half), bf16), v((2, seqs, half), bf16),
            pltpu.SemaphoreType.DMA((4,)), pltpu.SemaphoreType.DMA((17 + 6 * outer,)), pltpu.SemaphoreType.DMA((15,)),
        ],
        compiler_params=pltpu.CompilerParams(
            collective_id=0, has_side_effects=True, vmem_limit_bytes=40 * 1024 * 1024),
    )(*[pltpu.with_memory_space_constraint(a, pltpu.HBM) for a in (
        lengths, forget_bias, hidden, attn_gain, ffn_gain, expert_ids.T, expert_scores.T,
        query_weight, key_weight.T, value_weight.T, forget_weight.T, cache_keys, cache_values, cache_logsum,
        out_weight, gate_weights, up_weights, down_weights)])

    def hand_out(*refs):
        for i in range(4):
            refs[4 + i][...] = refs[i][...]

    updated, key_new, value_new, new_logsum = pl.pallas_call(
        hand_out,
        out_shape=[jax.ShapeDtypeStruct(r.shape, r.dtype) for r in results],
        in_specs=[vmem] * 4,
        out_specs=[vmem] * 4,
    )(*[pltpu.with_memory_space_constraint(r, pltpu.VMEM) for r in results])
    return updated, key_new.reshape(seqs, 1, HD), value_new.reshape(seqs, 1, HD), new_logsum


def per_device(hidden, attn_gain, query_weight, key_weight, value_weight, forget_weight, forget_bias,
               cache_keys, cache_values, cache_logsum, lengths, out_weight, ffn_gain, expert_ids, expert_scores,
               gate_weights, up_weights, down_weights):
    n = lax.axis_size("ep")
    seqs, width = hidden.shape
    fits = (
        n % (2 * PLANE) == 0
        and lax.axis_size("tp") == 2
        and gate_weights.shape[0] == 1
        and cache_keys.shape[1] == 1
        and seqs % 16 == 0
        and (query_weight.shape[1] // HD) % 16 == 0
        and out_weight.shape[0] % 128 == 0
        and n >= 4 * PLANE
        and n <= 128
    )
    if fits:
        return step_kernel(
            hidden, attn_gain, query_weight, key_weight, value_weight, forget_weight, forget_bias,
            cache_keys, cache_values, cache_logsum, lengths, out_weight, ffn_gain, expert_ids, expert_scores,
            gate_weights, up_weights, down_weights)
    attended, key_new, value_new, new_logsum = attend(
        hidden, attn_gain, query_weight, key_weight, value_weight, forget_weight, forget_bias,
        cache_keys, cache_values, cache_logsum, lengths)
    updated = rest_general(attended, hidden, out_weight, ffn_gain, expert_ids, expert_scores,
                           gate_weights, up_weights, down_weights)
    return (updated, key_new, value_new, new_logsum)


def solution(mesh):
    in_specs = (
        P("ep", None),
        P(),
        P(None, "tp"),
        P(None, "tp"),
        P(None, "tp"),
        P(None, "tp"),
        P("tp"),
        P("ep", "tp", None, None),
        P("ep", "tp", None, None),
        P("ep", "tp", None),
        P("ep"),
        P("ep", None),
        P(),
        P("ep", None),
        P("ep", None),
        P("ep", None, "tp"),
        P("ep", None, "tp"),
        P("ep", "tp", None),
    )
    out_specs = (P("ep", None), P("ep", "tp", None), P("ep", "tp", None), P("ep", "tp"))
    return jax.shard_map(
        per_device, mesh=mesh, in_specs=in_specs, out_specs=out_specs, check_vma=False
    )
```

```python
import functools
import math

import jax
import jax.numpy as jnp
from jax import lax
from jax.experimental import pallas as pl
from jax.experimental.pallas import tpu as pltpu
from jax.sharding import PartitionSpec as P

HD = 64
TOP_K = 6


epsilon = 1e-06


def root_norm(values_in, gain):
    floats = values_in.astype(jnp.float32)
    inv_root = lax.rsqrt(jnp.mean(floats * floats, axis=-1, keepdims=True) + epsilon)
    return floats * inv_root * gain.astype(jnp.float32)


def attend(hidden, attn_gain, query_weight, key_weight, value_weight, forget_weight, forget_bias,
           cache_keys, cache_values, cache_logsum, lengths):
    rows_here = hidden.shape[0]
    query_heads = query_weight.shape[1] // HD
    key_heads = key_weight.shape[1] // HD
    group_size = query_heads // key_heads
    cache_len = cache_keys.shape[-1]
    score_scale = HD ** (-0.5)
    normed = root_norm(hidden, attn_gain).astype(jnp.bfloat16)
    queries = jnp.dot(normed, query_weight, preferred_element_type=jnp.float32).astype(jnp.bfloat16)
    key_new = (
        jnp.dot(normed, key_weight, preferred_element_type=jnp.float32)
        .astype(jnp.bfloat16)
        .reshape(rows_here, key_heads, HD)
    )
    value_new = (
        jnp.dot(normed, value_weight, preferred_element_type=jnp.float32)
        .astype(jnp.bfloat16)
        .reshape(rows_here, key_heads, HD)
    )
    log_forget = jax.nn.log_sigmoid(
        jnp.dot(normed, forget_weight, preferred_element_type=jnp.float32) + forget_bias
    )
    positions = jnp.arange(cache_len, dtype=jnp.int32)
    is_last = positions[None, :] == (lengths - 1)[:, None]
    new_logsum = jnp.sum(jnp.where(is_last[:, None, :], cache_logsum, 0.0), axis=-1) + log_forget
    grouped = queries.reshape(rows_here, key_heads, group_size, HD)
    scores = jnp.einsum("sgjd,sgdp->sgjp", grouped, cache_keys, preferred_element_type=jnp.float32)
    scores = scores.reshape(rows_here, query_heads, cache_len) * score_scale
    scores = scores + new_logsum[:, :, None] - cache_logsum
    is_live = positions[None, :] < lengths[:, None]
    scores = jnp.where(is_live[:, None, :], scores, -jnp.inf)
    own_score = (
        jnp.einsum("sgjd,sgd->sgj", grouped, key_new, preferred_element_type=jnp.float32).reshape(
            rows_here, query_heads
        )
        * score_scale
    )
    top_score = jnp.maximum(jnp.max(scores, axis=-1), own_score)
    past_exp = jnp.exp(scores - top_score[:, :, None])
    own_exp = jnp.exp(own_score - top_score)
    denominator = jnp.sum(past_exp, axis=-1) + own_exp
    past_weight = (past_exp / denominator[:, :, None]).astype(jnp.bfloat16)
    own_weight = (own_exp / denominator).astype(jnp.bfloat16)
    attended = jnp.einsum(
        "sgjp,sgdp->sgjd",
        past_weight.reshape(rows_here, key_heads, group_size, cache_len),
        cache_values,
        preferred_element_type=jnp.float32,
    )
    attended = (
        attended
        + own_weight.astype(jnp.float32).reshape(rows_here, key_heads, group_size)[:, :, :, None]
        * value_new.astype(jnp.float32)[:, :, None, :]
    )
    attended = attended.reshape(rows_here, query_heads * HD).astype(jnp.bfloat16)
    return attended, key_new, value_new, new_logsum


def rest_general(attended, hidden, out_weight, ffn_gain, expert_ids, expert_scores,
                 gate_weights, up_weights, down_weights):
    rows_here = hidden.shape[0]
    whole_heads = lax.all_gather(attended, "tp", axis=1, tiled=True)
    projected = lax.dot_general(
        lax.all_gather(whole_heads, "ep", axis=0, tiled=True),
        out_weight,
        (((1,), (1,)), ((), ())),
        preferred_element_type=jnp.float32,
    ).astype(jnp.bfloat16)
    mixed = lax.all_to_all(projected, "ep", split_axis=0, concat_axis=1, tiled=True)
    residual = hidden.astype(jnp.float32) + mixed.astype(jnp.float32)
    ffn_in = root_norm(residual, ffn_gain).astype(jnp.bfloat16)
    ep_size = lax.axis_size("ep")
    local_experts = gate_weights.shape[0]
    experts = ep_size * local_experts
    route_count = rows_here * TOP_K
    capacity = 2 * ((route_count + experts - 1) // experts)
    flat_ids = expert_ids.reshape(route_count)
    onehot = (flat_ids[:, None] == jnp.arange(experts, dtype=jnp.int32)[None, :]).astype(jnp.int32)
    running = jnp.cumsum(onehot, axis=0)
    slot_index = jnp.sum(running * onehot, axis=1) - 1
    target = flat_ids * capacity + slot_index
    dispatch_map = (
        target[:, None] == jnp.arange(experts * capacity, dtype=jnp.int32)[None, :]
    ).astype(jnp.bfloat16)
    route_rows = jnp.repeat(ffn_in, TOP_K, axis=0)
    outgoing = lax.dot_general(
        dispatch_map, route_rows, (((0,), (0,)), ((), ())), preferred_element_type=jnp.float32
    )
    outgoing = outgoing.astype(jnp.bfloat16).reshape(
        ep_size, local_experts, capacity, ffn_in.shape[1]
    )
    arrived = lax.all_to_all(outgoing, "ep", split_axis=0, concat_axis=0, tiled=True)
    gate_act = jnp.einsum(
        "sekd,edf->sekf", arrived, gate_weights, preferred_element_type=jnp.float32
    )
    up_act = jnp.einsum("sekd,edf->sekf", arrived, up_weights, preferred_element_type=jnp.float32)
    hidden_act = (jax.nn.silu(gate_act) * up_act).astype(jnp.bfloat16)
    partial_out = jnp.einsum(
        "sekf,efd->sekd", hidden_act, down_weights, preferred_element_type=jnp.float32
    )
    half_sum = lax.psum_scatter(
        partial_out.astype(jnp.bfloat16), "tp", scatter_dimension=3, tiled=True
    )
    sent_back = lax.all_to_all(half_sum, "ep", split_axis=0, concat_axis=0, tiled=True)
    share_width = sent_back.shape[-1]
    picked = jnp.dot(
        dispatch_map,
        sent_back.reshape(experts * capacity, share_width),
        preferred_element_type=jnp.float32,
    )
    route_weight = expert_scores / jnp.sum(expert_scores, axis=-1, keepdims=True)
    expert_mix = jnp.sum(
        picked.reshape(rows_here, TOP_K, share_width) * route_weight[:, :, None], axis=1
    )
    own_part = lax.dynamic_slice_in_dim(
        residual, lax.axis_index("tp") * share_width, share_width, 1
    )
    updated = lax.all_gather((own_part + expert_mix).astype(jnp.bfloat16), "tp", axis=1, tiled=True)
    return updated


MESH = pl.DeviceIdType.MESH
PLANE = 4


def step_body(n, len_hbm, fbias_hbm, hid_hbm, again_hbm, fgain_hbm, ids_hbm, rscore_hbm,
              qw_hbm, kw_hbm, vw_hbm, fw_hbm, keys_hbm, vals_hbm, logs_hbm, ow_hbm, gate_hbm, up_hbm, down_hbm,
              out_ref, key_ref, val_ref, nlog_ref,
              len_ref, fbias_ref, hid_ref, again, fgain, fgain_row, ids_ref, rscore_ref, qw, kw, vw, fw, keys, vals, logs, scores, maxes, lasts, sums, mixed_heads, att, wsend, ow, gate, up, down,
              hidl, part, mixl, mixin, rows, ssq, ssqp, scales, wts, act, eout, back, fsum, far, upd,
              send, recv, local):
    f32, bf16 = jnp.float32, jnp.bfloat16
    me, tp = lax.axis_index("ep"), lax.axis_index("tp")
    seqs, width = hid_ref.shape
    cols = qw.shape[1]
    heads = cols // HD
    cache_len = keys.shape[2]
    outer = n // PLANE
    feats = wsend.shape[0]
    pf = PLANE * feats
    xq = pf // 2
    line = outer * seqs
    z, xy = me // PLANE, lax.rem(me, PLANE)
    x, y = lax.rem(xy, 2), xy // 2
    kept = lax.rem(y + tp, 2)
    spots = [y * 2 + (1 - x), (1 - y) * 2 + x, (1 - y) * 2 + (1 - x)]
    plane = [z * PLANE + s for s in spots]

    def zdev(zz):
        return zz * PLANE + xy

    near_tables = [sorted([j for j in range(outer) if j != i], key=lambda j: (abs(j - i), j)) for i in range(outer)]
    far_tables = [sorted(range(outer), key=lambda j: (-abs(j - i), j)) for i in range(outer)]

    def pick(tables, k, zz):
        value = tables[0][k]
        for i in range(1, outer):
            value = jnp.where(zz == i, tables[i][k], value)
        return value

    zs = [pick(near_tables, k, z) for k in range(outer - 1)]
    dests = [pick(far_tables, k, z) for k in range(outer - 1)] + [z]

    def rows_of(g, zz):
        return sl(zz if g == outer - 1 else pick(far_tables, g, zz), seqs)

    used = {"s": 0, "r": 0, "l": 0}

    def take(kind, count=1):
        base = used[kind]
        used[kind] += count
        return base

    def copy(src, dst, s, r, ep, core):
        return pltpu.make_async_remote_copy(src_ref=src, dst_ref=dst, send_sem=send.at[s], recv_sem=recv.at[r],
                                            device_id=(ep, core), device_id_type=MESH)

    wholes = [0, 0]

    def group(whole):
        size = math.prod(whole.shape) * whole.dtype.itemsize
        kind = 0 if size % (32 * cols) == 0 else 1
        wholes[kind] += size
        return kind

    def begin(src, dst, s, r, ep, core):
        copy(src, dst, s, r, ep, core).start()

    def arrived(dst, r):
        copy(dst, dst, 0, r, me, 1 - tp).wait_recv()

    def load(src, dst, l=None):
        c = pltpu.make_async_copy(src, dst, local.at[take("l") if l is None else l])
        c.start()
        return c

    def sl(i, size):
        return pl.ds(pl.multiple_of(i * size, size), size)

    barrier = pltpu.get_barrier_semaphore()
    for d in range(1, outer):
        for core in range(2):
            pl.semaphore_signal(barrier, inc=1, device_id=(zdev(lax.rem(z + d, outer)), core), device_id_type=MESH)
    for p in plane:
        pl.semaphore_signal(barrier, inc=1, device_id=(p, tp), device_id_type=MESH)
    for p in plane[:2]:
        pl.semaphore_signal(barrier, inc=1, device_id=(p, 1 - tp), device_id_type=MESH)
    pl.semaphore_signal(barrier, inc=1, device_id=(me, 1 - tp), device_id_type=MESH)

    ow_load = load(ow_hbm.at[:, sl(tp, cols)], wsend)
    slot, own_l = lax.rem(xy, 2), take("l")

    first = [load(hid_hbm, hid_ref), load(again_hbm, again), load(ids_hbm, ids_ref), load(rscore_hbm, rscore_ref)]
    scalars = [load(fbias_hbm, fbias_ref), load(len_hbm, len_ref), load(fgain_hbm, fgain)]
    small_l, qw_l, keys_l, logs_l, vals_l = [take("l") for _ in range(5)]
    for src, dst in ((kw_hbm, kw), (vw_hbm, vw), (fw_hbm, fw)):
        load(src, dst, small_l)
    qchunk = width // 4
    for i in range(4):
        load(qw_hbm.at[pl.ds(i * qchunk, qchunk)], qw.at[pl.ds(i * qchunk, qchunk)], qw_l)
    batch = seqs // 4
    for i in range(4):
        some = pl.ds(i * batch, batch)
        load(keys_hbm.at[some, 0], keys.at[some], keys_l)
        load(logs_hbm.at[some], logs.at[some], logs_l)
    for i in range(4):
        some = pl.ds(i * batch, batch)
        load(vals_hbm.at[some, 0], vals.at[some], vals_l)

    def loaded(ref, l):
        pltpu.make_async_copy(ref, ref, local.at[l]).wait()

    pl.semaphore_wait(barrier, 2 * (outer - 1) + 3 + 2 + 1)

    hf = feats // 2
    lo, hi = pl.ds(0, hf), pl.ds(hf, hf)
    ow_load.wait()
    ow_s, ow_r = group(ow.at[0]), take("r", 5)
    quarters = [pl.ds(k * hf // 2, hf // 2) for k in range(4)]
    for i, some, r in ((0, quarters[0], 0), (1, quarters[2], 1), (0, quarters[1], 2), (1, quarters[3], 3),
                       (0, hi, 4), (1, lo, 4)):
        begin(wsend.at[some], ow.at[slot, some, sl(tp, cols)], ow_s, ow_r + r, plane[i], i)

    @pl.when(tp == 0)
    def own_rows():
        load(ow_hbm, ow.at[slot], own_l)

    for c in first:
        c.wait()
    normed = root_norm(hid_ref[...], again[...][None, :]).astype(bf16)
    rscore = rscore_ref[...]
    route = rscore / jnp.sum(rscore, axis=0, keepdims=True)
    ids = ids_ref[...].astype(f32)
    lanes = lax.broadcasted_iota(jnp.int32, (seqs, 128), 1).astype(f32)
    small_eye = (lax.broadcasted_iota(jnp.int32, (seqs, seqs), 0) == lax.broadcasted_iota(jnp.int32, (seqs, seqs), 1))

    def column(row):
        return jnp.sum(jnp.where(small_eye, jnp.broadcast_to(row, (seqs, seqs)), 0.0), axis=1, keepdims=True)

    table = jnp.zeros((seqs, 128), f32)
    for k in range(TOP_K):
        table = table + jnp.where(lanes == column(ids[k:k + 1, :]), column(route[k:k + 1, :]), 0.0)
    wts[3, sl(z, seqs), :] = table

    others = pl.ds(0, (outer - 1) * seqs)
    hid_s, hid_r = group(hidl.at[others]), take("r")
    for zz in zs:
        begin(hid_ref.at[:, pl.ds(pl.multiple_of(zz * pf + kept * xq, xq), xq)], hidl.at[sl(z, seqs)],
              hid_s, hid_r, zdev(zz), tp)
    hidl[sl(z, seqs), :] = hid_ref[:, pl.ds(pl.multiple_of(z * pf + kept * xq, xq), xq)]
    wt_s, wt_r = group(wts.at[0, others]), take("r")
    for zz in zs:
        begin(wts.at[3, sl(z, seqs)], wts.at[3, sl(z, seqs)], wt_s, wt_r, zdev(zz), tp)

    loaded(qw, qw_l)
    acc = jnp.dot(normed, qw[...], preferred_element_type=f32)
    queries = acc.astype(bf16).astype(f32) * (HD ** -0.5)
    loaded(qw.at[pl.ds(0, (2 * HD + heads) * width // cols)], small_l)
    for c in scalars:
        c.wait()
    fgain_row[...] = fgain[...].astype(f32)[None, :]

    def new_token(w):
        return lax.dot_general(normed, w[...], (((1,), (1,)), ((), ())), preferred_element_type=f32)

    key_new = new_token(kw).astype(bf16)
    value_new = new_token(vw).astype(bf16)
    key_ref[...] = key_new
    val_ref[...] = value_new
    hl = lax.broadcasted_iota(jnp.int32, (seqs, heads), 1)
    fb = jnp.zeros((seqs, heads), f32)
    for h in range(heads):
        fb = jnp.where(hl == h, fbias_ref[h], fb)
    pre = new_token(fw) + fb
    log_forget = jnp.minimum(pre, 0.0) - jnp.log1p(jnp.exp(-jnp.abs(pre)))

    expert_l = take("l")
    for t in range(2):
        for zc in range(outer):
            rows_from = pl.ds(zc * pf + t * xq, xq)
            load(gate_hbm.at[0, rows_from], gate.at[t * outer + zc], expert_l)
            load(up_hbm.at[0, rows_from], up.at[t * outer + zc], expert_l)
    down_s, down_r = group(down.at[0]), take("r")
    for zc in range(outer):
        mine = pl.ds(pl.multiple_of(zc * pf + tp * xq, xq), xq)
        other = pl.ds(pl.multiple_of(zc * pf + (1 - tp) * xq, xq), xq)
        load(down_hbm.at[0, :, mine], down.at[tp, :, pl.ds(zc * xq, xq)], expert_l)
        begin(down_hbm.at[0, :, other], down.at[tp, :, pl.ds(zc * xq, xq)], down_s, down_r, me, 1 - tp)

    total = seqs * heads

    def spread(v):
        return jnp.broadcast_to(v[:, None, :], (seqs, heads, v.shape[1])).reshape(total, v.shape[1])

    row_head = lax.rem(lax.broadcasted_iota(jnp.int32, (total, 128), 0), heads)
    picked = jnp.zeros((total, 128), f32)
    for j in range(cols // 128):
        picked = jnp.where(row_head // 2 == j, spread(queries[:, j * 128:(j + 1) * 128]), picked)
    picked = jnp.where(lax.rem(row_head, 2) == 0, picked, pltpu.roll(picked, HD, 1))[:, :HD]
    per_head = picked.astype(bf16)
    own = jnp.sum(picked * spread(key_new.astype(f32)), axis=-1, keepdims=True)

    positions = lax.broadcasted_iota(jnp.int32, (heads, cache_len), 1)
    for s in range(seqs):
        if s == 0:
            loaded(keys, keys_l)
            loaded(logs, logs_l)
        here = pl.ds(s * heads, heads)
        size = len_ref[s]
        level = logs[s]
        dots = jnp.dot(per_head[s * heads:(s + 1) * heads, :], keys[s], preferred_element_type=f32)
        past = jnp.where(positions < size, dots - level, -jnp.inf)
        scores[here, :] = past
        maxes[here, :] = jnp.broadcast_to(jnp.max(past, axis=-1, keepdims=True), (heads, 128))
        last = jnp.sum(jnp.where(positions == size - 1, level, 0.0), axis=-1, keepdims=True)
        lasts[here, :] = jnp.broadcast_to(last, (heads, 128))
    own_lane = lax.broadcasted_iota(jnp.int32, (total, heads), 1)
    own_row = lax.rem(lax.broadcasted_iota(jnp.int32, (total, heads), 0), heads)
    forget_col = jnp.sum(jnp.where(own_lane == own_row, spread(log_forget), 0.0), axis=-1, keepdims=True)
    newlog = lasts[:, :1] + forget_col
    nlog_ref[...] = jnp.sum(jnp.where(own_lane == own_row, jnp.broadcast_to(newlog, (total, heads)), 0.0)
                            .reshape(seqs, heads, heads), axis=1)
    own = own - newlog
    peak = jnp.maximum(maxes[:, :1], own)
    maxes[...] = jnp.broadcast_to(peak, (total, 128))
    for s in range(seqs):
        if s == 0:
            loaded(vals, vals_l)
        here = pl.ds(s * heads, heads)
        weights = jnp.exp(scores[here, :] - maxes[here, :][:, :1])
        sums[here, :] = jnp.broadcast_to(jnp.sum(weights, axis=-1, keepdims=True), (heads, 128))
        mixed_heads[here, :HD] = lax.dot_general(weights.astype(bf16), vals[s], (((1,), (1,)), ((), ())),
                                                 preferred_element_type=f32)
    own_exp = jnp.exp(own - peak)
    inverse = 1.0 / (sums[:, :1] + own_exp)
    outs = (mixed_heads[:, :HD] + own_exp * spread(value_new.astype(f32))) * inverse
    mixed_heads[:, :HD] = outs
    mixed_heads[:, HD:] = outs
    wide = lax.broadcasted_iota(jnp.int32, (seqs, 128), 1)
    for j in range(cols // 128):
        even = mixed_heads[pl.ds(2 * j, seqs, stride=heads), :]
        odd = mixed_heads[pl.ds(2 * j + 1, seqs, stride=heads), :]
        att[tp, sl(z, seqs), j * 128:(j + 1) * 128] = jnp.where(wide < HD, even, odd).astype(bf16)

    att_s, att_r = group(att.at[0, others]), take("r")
    for zz in reversed(zs):
        begin(att.at[tp, sl(z, seqs)], att.at[tp, sl(z, seqs)], att_s, att_r, zdev(zz), tp)
    relay_s, relay_r = group(ow.at[0, lo]), take("r")

    @pl.when(tp == 0)
    def relay_along_y():
        for k in range(2):
            piece = ow.at[1 - slot, quarters[k]]
            arrived(piece, ow_r + 2 * k)
            begin(piece, piece, relay_s, relay_r, plane[1], 1)

    @pl.when(tp == 1)
    def relay_along_x():
        for k in range(2):
            piece = ow.at[slot, quarters[2 + k]]
            arrived(piece, ow_r + 1 + 2 * k)
            begin(piece, piece, relay_s, relay_r, plane[0], 1)

    arrived(wts.at[0, others], wt_r)
    wline_s, wline_r = group(wts.at[pl.ds(0, 3)]), take("r")
    for i in range(3):
        begin(wts.at[3], wts.at[i], wline_s, wline_r, plane[i], tp)
    arrived(hidl.at[others], hid_r)
    arrived(att.at[0, others], att_r)
    both_s, both_r = group(att.at[0]), take("r")
    begin(att.at[tp], att.at[tp], both_s, both_r, me, 1 - tp)
    arrived(ow.at[0, lo], ow_r + 4)

    @pl.when(tp == 0)
    def own_rows_there():
        loaded(ow.at[slot], own_l)

    arrived(att.at[1 - tp], both_r)
    lines = jnp.concatenate([att[0], att[1]], axis=1)

    def project(i):
        part[i] = lax.dot_general(lines, ow[i], (((1,), (1,)), ((), ())), preferred_element_type=f32)

    project(slot)

    @pl.when(tp == 1)
    def last_rows_there():
        arrived(ow.at[1 - slot], relay_r)

    project(1 - slot)
    mixed = jnp.concatenate([part[0], part[1]], axis=1).astype(bf16)
    residual = hidl[...].astype(f32) + mixed.astype(f32)
    gain = fgain_row[:, pl.ds(pl.multiple_of(z * pf + kept * xq, xq), xq)]
    block = kept * outer + z
    rows[block, 3] = (residual * gain).astype(bf16)
    square = jnp.sum(residual * residual, axis=-1, keepdims=True)
    eye = (lax.broadcasted_iota(jnp.int32, (line, line), 0) == lax.broadcasted_iota(jnp.int32, (line, line), 1))
    flat = jnp.sum(jnp.where(eye, jnp.broadcast_to(square, (line, line)), 0.0), axis=0, keepdims=True)
    ssq[z, 3] = jnp.broadcast_to(flat, (8, line))
    mixl[...] = mixed

    zrow_s, zrow_r = group(rows.at[0, pl.ds(0, outer - 1)]), take("r", 2 * outer - 1)
    prow_s, prow_r = group(rows.at[pl.ds(0, 3)]), take("r", outer)
    crow_s, crow_r = group(rows.at[pl.ds(0, outer)]), take("r", outer)
    zsq_s, zsq_r = 2, take("r")
    psq_s, psq_r = 3, take("r")
    csq_s, csq_r = 3, take("r")
    mix_s, mix_r = group(mixl.at[others]), take("r")

    def out_to_plane(g, zz):
        b, some = kept * outer + zz, rows_of(g, z)
        for i in (2, 0, 1):
            begin(rows.at[b, 3, some], rows.at[b, i, some], prow_s, prow_r + g, plane[i], tp)

    for g in range(outer):
        for zz in reversed(zs):
            some = rows_of(g, zz)
            begin(rows.at[block, 3, some], rows.at[block, 3, some], zrow_s, zrow_r + (z if g == 0 else outer - 1 + g), zdev(zz), tp)
        if g == 0:
            for zz in reversed(zs):
                begin(ssq.at[z, 3], ssq.at[z, 3], zsq_s, zsq_r, zdev(zz), tp)
        out_to_plane(g, z)
    swap_s, swap_r = take("s"), take("r")

    @pl.when(y == 0)
    def mixed_stays():
        mixin[z] = mixl[sl(z, seqs), :]

    @pl.when(y == 1)
    def mixed_swaps():
        begin(mixl.at[sl(z, seqs)], mixin.at[z], 4, swap_r, me, 1 - tp)

    for g in range(outer):
        if g:
            arrived(rows.at[pl.ds(0, outer - 1), 3, rows_of(g, z)], zrow_r + outer - 1 + g)
        for zz in zs:
            if g == 0:
                arrived(rows.at[kept * outer + zz, 3, rows_of(g, z)], zrow_r + zz)
            out_to_plane(g, zz)
        if g == 0:
            arrived(ssq.at[0, pl.ds(0, outer - 1)], zsq_r)
            for i in range(3):
                begin(ssq.at[:, 3], ssq.at[:, i], psq_s, psq_r, plane[i], tp)
    for zz in zs:
        begin(mixl.at[sl(zz, seqs)], mixin.at[z], mix_s, mix_r, zdev(zz), kept)
    units = gate.shape[2]
    loaded(qw.at[pl.ds(0, (2 * width * units + units * width // 2) // cols)], expert_l)
    arrived(wts.at[pl.ds(0, 3)], wline_r)

    parts = [[g] for g in range(outer)]

    def pass_on(part_groups):
        for g in part_groups:
            mine, theirs, some = pl.ds(kept * outer, outer), pl.ds((1 - kept) * outer, outer), rows_of(g, z)
            arrived(rows.at[pl.ds(0, outer), pl.ds(0, 3), some], prow_r + g)
            for ref in (rows.at[theirs, pl.ds(1, 2), some], rows.at[mine, 0, some], rows.at[mine, 3, some]):
                begin(ref, ref, crow_s, crow_r + g, me, 1 - tp)

    def collect(part_groups):
        for g in part_groups:
            arrived(rows.at[pl.ds(0, outer), :, rows_of(g, z)], crow_r + g)
        left = jnp.concatenate([
            jnp.concatenate([rows[b, :, rows_of(g, z), :].reshape(PLANE * seqs, xq) for g in part_groups], axis=0)
            for b in range(2 * outer)], axis=1)
        return [jnp.dot(left, w[...].reshape(width, w.shape[2]), preferred_element_type=f32) for w in (gate, up)]

    act_s, act_r = group(act.at[0]), take("r", outer)

    def span_of(part_groups):
        return pl.ds(part_groups[0], len(part_groups))

    def activate(part_groups, a, u):
        scale = jnp.concatenate([scales[:, rows_of(g, z), :].reshape(PLANE * seqs, 128)[:, :1] for g in part_groups],
                                axis=0)
        a, u = a * scale, u * scale
        made = (a / (1.0 + jnp.exp(-a)) * u).astype(bf16)
        here = act.at[tp, span_of(part_groups)]
        here[...] = made.reshape(len(part_groups), PLANE * seqs, made.shape[1])
        begin(here, here, act_s, act_r + part_groups[0], me, 1 - tp)

    back_s, back_r = group(eout.at[pl.ds(0, 3)]), take("r", outer)
    which = lax.broadcasted_iota(jnp.int32, (PLANE * seqs, 128), 1) == me

    def give(part_groups):
        span = span_of(part_groups)
        arrived(act.at[1 - tp, span], act_r + part_groups[0])
        lefts = [act[t, span].reshape(len(part_groups) * PLANE * seqs, act.shape[3]) for t in range(2)]
        made = (jnp.dot(lefts[0], down[0], preferred_element_type=f32)
                + jnp.dot(lefts[1], down[1], preferred_element_type=f32))
        for j, g in enumerate(part_groups):
            zz = dests[g]
            wt = wts[:, sl(zz, seqs), :].reshape(PLANE * seqs, 128)
            weight = jnp.sum(jnp.where(which, wt, 0.0), axis=-1, keepdims=True)
            scaled = made[j * PLANE * seqs:(j + 1) * PLANE * seqs] * weight
            eout[zz] = scaled.astype(bf16).reshape(PLANE, seqs, made.shape[1])
            for i in (2, 0, 1):
                begin(eout.at[zz, i], back.at[zz, i], back_s, back_r + zz, plane[i], tp)

    pass_on(parts[0])
    arrived(ssq.at[:, pl.ds(0, 3)], psq_r)
    squares = ssq[0]
    for i in range(1, outer):
        squares = squares + ssq[i]
    ssqp[tp] = squares
    begin(ssqp.at[tp], ssqp.at[tp], csq_s, csq_r, me, 1 - tp)
    pass_on(parts[1])
    a, u = collect(parts[0])
    arrived(ssqp.at[1 - tp], csq_r)
    squares = ssqp[0] + ssqp[1]
    for q in range(PLANE):
        scale = lax.rsqrt(squares[q, :1, :] * (1.0 / width) + epsilon)
        scale = jnp.sum(jnp.where(eye, jnp.broadcast_to(scale, (line, line)), 0.0), axis=1, keepdims=True)
        scales[q] = jnp.broadcast_to(scale, (line, 128))
    activate(parts[0], a, u)
    arrived(down.at[1 - tp], down_r)
    far_s, far_r = group(fsum.at[pl.ds(0, outer - 1)]), take("r")

    def near(g):
        zz = dests[g]
        arrived(back.at[zz], back_r + zz)
        summed = eout[zz, 3].astype(f32)
        for i in range(3):
            summed = summed + back[zz, i].astype(f32)
        if g < outer - 1:
            fsum[zz] = summed.astype(bf16)
            begin(fsum.at[zz], far.at[z], far_s, far_r, zdev(zz), tp)
        return summed

    last = len(parts) - 1
    for k in range(1, len(parts)):
        if k == last:
            give(parts[k - 1])
        elif k > 1:
            pass_on(parts[k + 1])
        a, u = collect(parts[k])
        activate(parts[k], a, u)
        if k == 1:
            pass_on(parts[2])
        if k < last:
            give(parts[k - 1])
    near(0)
    give(parts[last])
    for g in range(1, outer):
        summed = near(g)
    arrived(mixin.at[pl.ds(0, outer - 1)], mix_r)

    @pl.when(y == 1)
    def mixed_swapped():
        arrived(mixin.at[z], swap_r)
        copy(mixl.at[sl(z, seqs)], mixin.at[z], 4, 0, me, 1 - tp).wait_send()

    arrived(far.at[pl.ds(0, outer - 1)], far_r)
    for zz in zs:
        summed = summed + far[zz].astype(f32)
    for zc in range(outer):
        here = hid_ref[:, pl.ds(pl.multiple_of(zc * pf + tp * xq, xq), xq)].astype(f32) + mixin[zc].astype(f32)
        upd[tp, :, zc * xq:(zc + 1) * xq] = (here + summed[:, zc * xq:(zc + 1) * xq]).astype(bf16)
    u_s, u_r = group(upd.at[0]), take("r")
    begin(upd.at[tp], upd.at[tp], u_s, u_r, me, 1 - tp)
    arrived(upd.at[1 - tp], u_r)
    for t in range(2):
        for zc in range(outer):
            out_ref[:, zc * pf + t * xq:zc * pf + (t + 1) * xq] = upd[t, :, zc * xq:(zc + 1) * xq]
    assert wholes[0] % (32 * cols) == 0 and wholes[1] % 4096 == 0, wholes
    for s, whole in enumerate((qw.at[pl.ds(0, wholes[0] // (2 * cols))], maxes.at[pl.ds(0, wholes[1] // 512)],
                               ssq.at[0, pl.ds(0, outer - 1)], ssq)):
        copy(whole, whole, s, 0, me, 1 - tp).wait_send()
    assert used["r"] == recv.shape[0] and used["l"] == local.shape[0], used


def step_kernel(hidden, attn_gain, query_weight, key_weight, value_weight, forget_weight, forget_bias,
                cache_keys, cache_values, cache_logsum, lengths, out_weight, ffn_gain, expert_ids, expert_scores,
                gate_weights, up_weights, down_weights):
    n = lax.axis_size("ep")
    seqs, width = hidden.shape
    cols = query_weight.shape[1]
    heads = cols // HD
    cache_len = cache_keys.shape[3]
    feats = out_weight.shape[0]
    units = gate_weights.shape[2]
    outer = n // PLANE
    line = outer * seqs
    xq = PLANE * feats // 2
    half = width // 2
    bf16, f32 = jnp.bfloat16, jnp.float32
    vmem = pl.BlockSpec(memory_space=pltpu.VMEM)
    hbm = pl.BlockSpec(memory_space=pltpu.HBM)
    v = pltpu.VMEM
    results = pl.pallas_call(
        functools.partial(step_body, n),
        out_shape=[v((seqs, width), bf16), v((seqs, HD), bf16), v((seqs, HD), bf16), v((seqs, heads), f32)],
        in_specs=[hbm] * 18,
        out_specs=[vmem] * 4,
        scratch_shapes=[
            pltpu.SMEM((seqs,), jnp.int32), pltpu.SMEM((heads,), f32), v((seqs, width), bf16), v((width,), bf16),
            v((width,), bf16), v((1, width), f32), v((TOP_K, seqs), jnp.int32), v((TOP_K, seqs), f32),
            v((width, cols), bf16), v((HD, width), bf16), v((HD, width), bf16), v((heads, width), bf16),
            v((seqs, HD, cache_len), bf16), v((seqs, HD, cache_len), bf16), v((seqs, heads, cache_len), f32),
            v((seqs * heads, cache_len), f32), v((seqs * heads, 128), f32), v((seqs * heads, 128), f32),
            v((seqs * heads, 128), f32), v((seqs * heads, 2 * HD), f32),
            v((2, line, cols), bf16), v((feats, cols), bf16), v((2, feats, 2 * cols), bf16),
            v((2 * outer, xq, units), bf16), v((2 * outer, xq, units), bf16), v((2, units, half), bf16),
            v((line, xq), bf16), v((2, line, feats), f32), v((line, xq), bf16),
            v((outer, seqs, xq), bf16),
            v((2 * outer, PLANE, line, xq), bf16), v((outer, PLANE, 8, line), f32), v((2, PLANE, 8, line), f32),
            v((PLANE, line, 128), f32), v((PLANE, line, 128), f32),
                        v((2, outer, PLANE * seqs, units), bf16),
            v((outer, PLANE, seqs, half), bf16), v((outer, 3, seqs, half), bf16),
            v((outer, seqs, half), bf16), v((outer, seqs, half), bf16), v((2, seqs, half), bf16),
            pltpu.SemaphoreType.DMA((5,)), pltpu.SemaphoreType.DMA((18 + 6 * outer,)), pltpu.SemaphoreType.DMA((15,)),
        ],
        compiler_params=pltpu.CompilerParams(
            collective_id=0, has_side_effects=True, vmem_limit_bytes=40 * 1024 * 1024),
    )(*[pltpu.with_memory_space_constraint(a, pltpu.HBM) for a in (
        lengths, forget_bias, hidden, attn_gain, ffn_gain, expert_ids.T, expert_scores.T,
        query_weight, key_weight.T, value_weight.T, forget_weight.T, cache_keys, cache_values, cache_logsum,
        out_weight, gate_weights, up_weights, down_weights)])

    def hand_out(*refs):
        for i in range(4):
            refs[4 + i][...] = refs[i][...]

    updated, key_new, value_new, new_logsum = pl.pallas_call(
        hand_out,
        out_shape=[jax.ShapeDtypeStruct(r.shape, r.dtype) for r in results],
        in_specs=[vmem] * 4,
        out_specs=[vmem] * 4,
    )(*[pltpu.with_memory_space_constraint(r, pltpu.VMEM) for r in results])
    return updated, key_new.reshape(seqs, 1, HD), value_new.reshape(seqs, 1, HD), new_logsum


def per_device(hidden, attn_gain, query_weight, key_weight, value_weight, forget_weight, forget_bias,
               cache_keys, cache_values, cache_logsum, lengths, out_weight, ffn_gain, expert_ids, expert_scores,
               gate_weights, up_weights, down_weights):
    n = lax.axis_size("ep")
    seqs, width = hidden.shape
    fits = (
        n % (2 * PLANE) == 0
        and lax.axis_size("tp") == 2
        and gate_weights.shape[0] == 1
        and cache_keys.shape[1] == 1
        and seqs % 16 == 0
        and (query_weight.shape[1] // HD) % 16 == 0
        and out_weight.shape[0] % 128 == 0
        and n >= 4 * PLANE
        and n <= 128
    )
    if fits:
        return step_kernel(
            hidden, attn_gain, query_weight, key_weight, value_weight, forget_weight, forget_bias,
            cache_keys, cache_values, cache_logsum, lengths, out_weight, ffn_gain, expert_ids, expert_scores,
            gate_weights, up_weights, down_weights)
    attended, key_new, value_new, new_logsum = attend(
        hidden, attn_gain, query_weight, key_weight, value_weight, forget_weight, forget_bias,
        cache_keys, cache_values, cache_logsum, lengths)
    updated = rest_general(attended, hidden, out_weight, ffn_gain, expert_ids, expert_scores,
                           gate_weights, up_weights, down_weights)
    return (updated, key_new, value_new, new_logsum)


def solution(mesh):
    in_specs = (
        P("ep", None),
        P(),
        P(None, "tp"),
        P(None, "tp"),
        P(None, "tp"),
        P(None, "tp"),
        P("tp"),
        P("ep", "tp", None, None),
        P("ep", "tp", None, None),
        P("ep", "tp", None),
        P("ep"),
        P("ep", None),
        P(),
        P("ep", None),
        P("ep", None),
        P("ep", None, "tp"),
        P("ep", None, "tp"),
        P("ep", "tp", None),
    )
    out_specs = (P("ep", None), P("ep", "tp", None), P("ep", "tp", None), P("ep", "tp"))
    return jax.shard_map(
        per_device, mesh=mesh, in_specs=in_specs, out_specs=out_specs, check_vma=False
    )
```
